512 devices in a mesh: grp: 2 (over y), dp: 8 (over x), kv: 16 (over z), tp: 2 (over core).
Axes of the slice: x: 8, y: 2, z: 16, core: 2. Of those that a mesh axis runs over, the one named last changes fastest.
The devices are a block of a 8x8x16 slice.
Arguments:
- tokens: bfloat16 [2048, 2048], P(('grp', 'dp'), ('kv', 'tp')), parts along dimension 0, may hold values from -6 to 6
- norm_gain: float32 [2048], P('kv'), may hold values from 0.1 to 1.9
- w_query: bfloat16 [2048, 512], P('kv', 'tp'), may hold values from -0.125 to 0.125
- w_key: bfloat16 [2048, 512], P('kv', 'tp'), may hold values from -0.125 to 0.125
- w_value: bfloat16 [2048, 1024], P('kv', 'tp'), may hold values from -0.125 to 0.125
- w_outgate: bfloat16 [2048, 1024], P('kv', 'tp'), may hold values from -0.125 to 0.125
- w_ingate: bfloat16 [2048, 8], P('kv'), may hold values from -0.125 to 0.125
- w_forget: bfloat16 [2048, 8], P('kv'), may hold values from -0.125 to 0.125
- in_bias: float32 [8], replicated, may hold values from -1.5 to 0.5
- forget_bias: float32 [8], replicated, may hold values from -1 to 4
- memory: float32 [2048, 8, 64, 128], P(('grp', 'dp', 'kv'), 'tp'), parts along dimension 0, may hold values from -4 to 4
- normalizer: float32 [2048, 512], P(('grp', 'dp', 'kv'), 'tp'), parts along dimension 0, may hold values from -4 to 4
- stabilizer: float32 [2048, 8], P(('grp', 'dp', 'kv'), 'tp'), parts along dimension 0, may hold values from -1 to 1
- w_out: bfloat16 [1024, 2048], P('tp', 'kv'), may hold values from -0.1875 to 0.1875
- mlp_gain: float32 [2048], replicated, may hold values from 0.1 to 1.9
- w_up: bfloat16 [2048, 8192], P(None, ('kv', 'tp')), may hold values from -0.125 to 0.125
- w_down: bfloat16 [8192, 2048], P(('kv', 'tp')), may hold values from -0.125 to 0.125
Outputs:
- mixed_out: bfloat16 [2048, 2048], P(('grp', 'dp'), ('kv', 'tp')), parts along dimension 0
- memory_new: float32 [2048, 8, 64, 128], P(('grp', 'dp', 'kv'), 'tp'), parts along dimension 0
- normalizer_new: float32 [2048, 512], P(('grp', 'dp', 'kv'), 'tp'), parts along dimension 0
- stabilizer_new: float32 [2048, 8], P(('grp', 'dp', 'kv'), 'tp'), parts along dimension 0
The draws below stay inside these ranges and needn't reach their ends.
There are 2 independent parts, one for each index of `grp`. The reference program is written for one: setup_inputs(seed, part) draws one part's arguments, and reference() takes and returns one part's arrays. A program takes and returns all parts, laid end to end along the dimension named above; an argument that names none is the same for every part. Nothing has to cross between parts.
All inputs are finite; a program needn't handle non-finite values.
Results may differ from the reference program's by a relative error of at most 0.03.
Values may be sent and summed in bfloat16 or wider, within the bound.
A program may use at most 64 MiB of HBM per device.

```python
import jax
import jax.numpy as jnp
from jax import lax

D = 2048
HEADS = 8
QK_DIM = 64
VD_DIM = 128
FF = 8192
BATCH = 1024
N_KV = 16
N_TP = 2


def with_spikes(drawn, stream_key, source, target, blocks, factor):
    owner, partner = [(jnp.arange(drawn.shape[dim]) // (drawn.shape[dim] // blocks)).reshape([-1 if axis == dim else 1 for axis in range(drawn.ndim)]) for dim in (source, target)]
    chosen = jax.random.permutation(stream_key, blocks)[partner]
    strong = (owner == chosen) | (owner == (partner + blocks // 2) % blocks)
    return jnp.where(strong, factor * drawn, drawn)


def block_levels(key, dims, cuts, smallest, largest):
    def one(dim, shards_of):
        heights = jax.random.uniform(jax.random.fold_in(jax.random.fold_in(key, 6), dim), (shards_of,), jnp.float32, smallest / len(cuts), largest / len(cuts))
        return jnp.repeat(jnp.exp(heights), dims[dim] // shards_of).reshape((-1,) + (1,) * (len(dims) - dim - 1))

    loudness = one(*cuts[0])
    for cut in cuts[1:]:
        loudness = loudness * one(*cut)
    return loudness


def bell_draw(own_key, shape, scale, most, split=(), held_as=jnp.bfloat16):
    gain = block_levels(own_key, shape, split, -0.22, 0.18) if split else 1.0
    result = jax.random.normal(own_key, shape, jnp.float32) * scale * gain
    return jnp.minimum(jnp.maximum(result, -most), most).astype(held_as)


def noise_with(key, dims, scale, most, cuts, heavy, dtype=jnp.bfloat16):
    values = scale * jax.random.normal(key, dims, jnp.float32)
    if cuts:
        values = values * block_levels(key, dims, cuts, -0.22, 0.18)
    return jnp.clip(with_spikes(values, jax.random.fold_in(key, 3), *heavy), -most, most).astype(dtype)


def setup_inputs(seed: int = 0, part: int = 0) -> dict:
    key_of = jax.random.split(jax.random.key(seed), 18)
    part_splits = jax.random.split(jax.random.fold_in(key_of[17], part), 18)
    tokens = noise_with(part_splits[0], (BATCH, D), 1.0, 6.0, ((0, 8), (1, 32)), (1, 0, 32, 2.75))
    norm_gain = jnp.clip(1.0 + 0.18 * jax.random.normal(key_of[1], (D,), jnp.float32), 0.1, 1.9)
    w_query = bell_draw(key_of[2], (D, HEADS * QK_DIM), D ** -0.5, 0.125, ((0, 16), (1, 2)))
    w_key = bell_draw(key_of[3], (D, HEADS * QK_DIM), D ** -0.5, 0.125, ((0, 16), (1, 2)))
    w_value = bell_draw(key_of[4], (D, HEADS * VD_DIM), D ** -0.5, 0.125, ((0, 16), (1, 2)))
    w_outgate = bell_draw(key_of[5], (D, HEADS * VD_DIM), D ** -0.5, 0.125, ((0, 16), (1, 2)))
    w_ingate = bell_draw(key_of[6], (D, HEADS), D ** -0.5, 0.125, ((0, 16),))
    w_forget = bell_draw(key_of[7], (D, HEADS), D ** -0.5, 0.125, ((0, 16),))
    in_bias = jnp.clip(jax.random.uniform(key_of[8], (HEADS,), jnp.float32, -1.5, 0.5), -1.5, 0.5)
    forget_bias = jnp.clip(jax.random.uniform(key_of[9], (HEADS,), jnp.float32, -1.0, 4.0), -1.0, 4.0)
    memory = bell_draw(part_splits[10], (BATCH, HEADS, QK_DIM, VD_DIM), 0.5, 4.0, ((0, 128), (1, 2)), jnp.float32)
    normalizer = bell_draw(part_splits[11], (BATCH, HEADS * QK_DIM), 0.5, 4.0, ((0, 128), (1, 2)), jnp.float32)
    stabilizer = jnp.clip(jax.random.uniform(part_splits[12], (BATCH, HEADS), jnp.float32, -1.0, 1.0) * block_levels(part_splits[12], (BATCH, HEADS), ((0, 128), (1, 2)), -0.4, 0.0), -1.0, 1.0)
    w_out = bell_draw(key_of[13], (HEADS * VD_DIM, D), (HEADS * VD_DIM) ** -0.5, 0.1875, ((0, 2), (1, 16)))
    mlp_gain = jnp.clip(1.0 + 0.18 * jax.random.normal(key_of[14], (D,), jnp.float32), 0.1, 1.9)
    w_up = bell_draw(key_of[15], (D, FF), D ** -0.5, 0.125, ((1, 32),))
    w_down = noise_with(key_of[16], (FF, D), FF ** -0.5, 0.125, ((0, 32),), (0, 1, 32, 2.75))
    return dict(tokens=tokens, norm_gain=norm_gain, w_query=w_query, w_key=w_key, w_value=w_value, w_outgate=w_outgate, w_ingate=w_ingate, w_forget=w_forget, in_bias=in_bias, forget_bias=forget_bias, memory=memory, normalizer=normalizer, stabilizer=stabilizer, w_out=w_out, mlp_gain=mlp_gain, w_up=w_up, w_down=w_down)


EPSILON = 1e-06

def block_sum(left, weight, parts):
    rows = left.shape[0]
    width = weight.shape[0] // parts
    left_blocks = jnp.transpose(left.reshape(rows, parts, width), (1, 0, 2))
    weight_blocks = weight.reshape(parts, width, weight.shape[1])

    def step(total, pair):
        term = jnp.dot(pair[0], pair[1], preferred_element_type=jnp.float32).astype(jnp.bfloat16)
        term = lax.optimization_barrier(term)
        return (total + term.astype(jnp.float32), None)
    start = jnp.zeros((rows, weight.shape[1]), jnp.float32)
    total, unused = lax.scan(step, start, (left_blocks, weight_blocks))
    return total

def reference(tokens, norm_gain, w_query, w_key, w_value, w_outgate, w_ingate, w_forget, in_bias, forget_bias, memory, normalizer, stabilizer, w_out, mlp_gain, w_up, w_down):
    batch_rows = tokens.shape[0]
    tokens_f = tokens.astype(jnp.float32)
    rscale = lax.rsqrt(lax.optimization_barrier(jnp.mean(tokens_f * tokens_f, axis=1, keepdims=True)) + EPSILON)
    scaled = (tokens_f * norm_gain).astype(jnp.bfloat16)

    def product(weight):
        return block_sum(scaled, weight, N_KV) * rscale
    queries = product(w_query).reshape(batch_rows, HEADS, QK_DIM)
    keys_in = (product(w_key) * QK_DIM ** (-0.5)).reshape(batch_rows, HEADS, QK_DIM)
    values_in = product(w_value).reshape(batch_rows, HEADS, VD_DIM)
    out_pre = product(w_outgate).reshape(batch_rows, HEADS, VD_DIM)
    log_in = product(w_ingate) + in_bias
    log_forget = jax.nn.log_sigmoid(product(w_forget) + forget_bias)
    carried = log_forget + stabilizer
    stab_new = jnp.maximum(carried, log_in)
    take_new = jnp.exp(log_in - stab_new)
    keep_old = jnp.exp(carried - stab_new)
    norm_old = normalizer.reshape(batch_rows, HEADS, QK_DIM)
    score = lax.optimization_barrier(jnp.sum(queries * keys_in, axis=2))
    readout = jnp.einsum('shkv,shk->shv', memory, queries, precision=lax.Precision.HIGHEST)
    numer = (take_new * score)[..., None] * values_in + keep_old[..., None] * readout
    denom = take_new * score + keep_old * lax.optimization_barrier(jnp.sum(norm_old * queries, axis=2))
    cell = numer / jnp.maximum(jnp.abs(denom), 1.0)[..., None]
    hidden = (jax.nn.sigmoid(out_pre) * cell).reshape(batch_rows, HEADS * VD_DIM).astype(jnp.bfloat16)
    middle = (tokens_f + jnp.dot(hidden, w_out, preferred_element_type=jnp.float32)).astype(jnp.bfloat16)
    middle_f = middle.astype(jnp.float32)
    rscale_mid = lax.rsqrt(lax.optimization_barrier(jnp.mean(middle_f * middle_f, axis=1, keepdims=True)) + EPSILON)
    normed = (middle_f * rscale_mid * mlp_gain).astype(jnp.bfloat16)
    upward = jnp.dot(normed, w_up, preferred_element_type=jnp.float32)
    squared = jnp.square(jax.nn.relu(upward)).astype(jnp.bfloat16)
    mixed_out = (middle_f + block_sum(squared, w_down, N_KV * N_TP)).astype(jnp.bfloat16)
    memory_new = keep_old[..., None, None] * memory + take_new[..., None, None] * keys_in[..., :, None] * values_in[..., None, :]
    normalizer_new = (keep_old[..., None] * norm_old + take_new[..., None] * keys_in).reshape(batch_rows, HEADS * QK_DIM)
    return (mixed_out, memory_new, normalizer_new, stab_new)
```

```python
import functools

import jax
import jax.numpy as jnp
from jax import lax
from jax.experimental import pallas as pl
from jax.experimental.pallas import tpu as pltpu
from jax.sharding import PartitionSpec as P

EPSILON = 1e-06
MESH = pl.DeviceIdType.MESH
F32 = jnp.float32
BF16 = jnp.bfloat16

TWO_LEVEL = {1: 0, 2: 0, 3: 0, 4: 0, 5: 4, 6: 4, 7: 4, 8: 4}
PROJ_TREE = TWO_LEVEL
HID_TREE = TWO_LEVEL
MID_TREE = TWO_LEVEL
DOWN_TREE = TWO_LEVEL
REACH = 4


def messages(tree, n):
    half = n // 2
    out = []
    for side, last in ((1, half), (-1, n - 1 - half)):
        for k in range(1, last + 1):
            out.append((len(out), side, k, tree[k]))
    return out


def children_of(msgs, side, k):
    return [m for m in msgs if m[1] == side and m[3] == k]


def depth_below(msgs, m):
    below = children_of(msgs, m[1], m[2])
    return 1 + max(depth_below(msgs, c) for c in below) if below else 0


def level_of(tree, k):
    return 0 if k == 0 else 1 + level_of(tree, tree[k])


def kernel(
    n,
    tok,
    ngain,
    wq,
    wk,
    wv,
    wg,
    wi,
    wf,
    ib,
    fb,
    mem,
    nrm,
    stab,
    wo,
    mgain,
    wup,
    wdn,
    out,
    mem_new,
    nrm_new,
    stab_new,
    tokb,
    ngv,
    wp,
    wib,
    wfb,
    ibb,
    fbb,
    memb,
    memo,
    nrmb,
    stabb,
    wob,
    mgb,
    wupb,
    wdnb,
    pf,
    ps,
    pr,
    sf,
    ro,
    tokrow,
    hidg,
    opown,
    opsend,
    oprecv,
    midg,
    down_own,
    ds,
    dr,
    fxs,
    fxr,
    lsem,
    xs,
    xr,
    ps_s,
    ps_r,
    hid_s,
    hid_r,
    mid_s,
    mid_r,
    dn_s,
    dn_r,
):
    me = lax.axis_index("kv")
    tp = lax.axis_index("tp")
    other = 1 - tp
    rows = tokb.shape[1]
    half_ch = tokb.shape[2]
    seqs, heads, qk, vd = memb.shape
    hw = heads * qk
    vw = heads * vd
    proj = wp.shape[1]
    width = mgb.shape[0] * mgb.shape[1]
    half_rows = rows // 2

    def at(z):
        return lax.rem(z + 2 * n, n)

    barrier = pltpu.get_barrier_semaphore()
    for step in range(1, REACH + 1):
        for side in (1, -1):
            pl.semaphore_signal(barrier, inc=1, device_id={"kv": at(me + side * step)}, device_id_type=MESH)
    pl.semaphore_signal(barrier, inc=1, device_id={"tp": other}, device_id_type=MESH)

    loads = {}

    def load(name, src, dst):
        c = pltpu.make_async_copy(src, dst, lsem.at[len(loads)])
        c.start()
        loads[name] = c

    load("tok", tok, tokb.at[tp])
    load("ngain", ngain, ngv)
    load("wq", wq, wp.at[:, 0:hw])
    load("wk", wk, wp.at[:, hw : 2 * hw])
    load("wv", wv, wp.at[:, 2 * hw : 2 * hw + vw])
    load("wg", wg, wp.at[:, 2 * hw + vw : proj])
    load("wi", wi, wib)
    load("wf", wf, wfb)
    load("ib", ib, ibb)
    load("fb", fb, fbb)
    load("stab", stab, stabb)
    load("nrm", nrm, nrmb)
    load("mem", mem, memb)
    load("wo", wo, wob)
    load("mgain", mgain, mgb)
    load("wup", wup, wupb.at[tp])
    load("wdn", wdn, wdnb.at[tp])

    pl.semaphore_wait(barrier, 2 * REACH + 1)

    def to_partner(src, dst, i):
        return pltpu.make_async_remote_copy(
            src_ref=src, dst_ref=dst, send_sem=xs.at[i], recv_sem=xr.at[i], device_id={"tp": other}, device_id_type=MESH
        )

    loads["tok"].wait()
    tok_x = to_partner(tokb.at[tp], tokb.at[tp], 0)
    tok_x.start()
    sends = [tok_x]

    for name in ("ngain", "wq", "wk", "wv", "wg", "wi", "wf"):
        loads[name].wait()

    lane128 = lax.broadcasted_iota(jnp.int32, (rows, 128), 1)

    def project(which):
        t = tokb[which].astype(F32)
        gain = jnp.where(which == 0, ngv[:, 0:half_ch], ngv[:, half_ch : 2 * half_ch])
        scaled = (t * gain).astype(BF16)
        chans = pl.ds(pl.multiple_of(which * half_ch, half_ch), half_ch)
        main = jnp.dot(scaled, wp[chans, :], preferred_element_type=F32)
        gi = jnp.dot(scaled, wib[chans, :], preferred_element_type=F32)
        gf = jnp.dot(scaled, wfb[chans, :], preferred_element_type=F32)
        sq = jnp.sum(t * t, axis=1, keepdims=True)
        zeros = jnp.zeros((rows, 128 - 2 * gi.shape[1]), F32)
        gates = jnp.concatenate([gi, gf, zeros], axis=1)
        gates = jnp.where(lane128 == 2 * gi.shape[1], sq, gates)
        return main, gates

    gate_lanes = 2 * wib.shape[1]
    main, gates = project(tp)
    pf[:, :, 0:proj] = main.reshape(n, seqs, proj)
    pf[:, :, proj:] = gates.reshape(n, seqs, 128)
    tok_x.wait_recv()
    main, gates = project(other)
    pf[:, :, 0:proj] += main.reshape(n, seqs, proj)
    pf[:, :, proj:] += gates.reshape(n, seqs, 128)

    lane8 = lax.broadcasted_iota(jnp.int32, (seqs, 128), 1)

    def pack_gates(g):
        total = g[:, gate_lanes : gate_lanes + 1] + g[:, gate_lanes + 1 : gate_lanes + 2]
        upper = total.astype(BF16).astype(F32)
        return jnp.where(lane8 == gate_lanes, upper, jnp.where(lane8 == gate_lanes + 1, total - upper, g))

    def reduce_scatter(tree, own, recv, emit, send_sem, recv_sem, send_buf):
        msgs = messages(tree, n)

        def copy_of(m):
            slot, side, k, parent = m
            return pltpu.make_async_remote_copy(
                src_ref=send_buf.at[slot],
                dst_ref=recv.at[slot],
                send_sem=send_sem.at[slot],
                recv_sem=recv_sem.at[slot],
                device_id={"kv": at(me - side * (k - parent))},
                device_id_type=MESH,
            )

        order = sorted(msgs, key=lambda m: (depth_below(msgs, m), -level_of(tree, m[2]), -m[2]))
        for m in order:
            slot, side, k, parent = m
            mine = own(at(me - side * k))
            kids = children_of(msgs, side, k)
            for c in kids:
                copy_of(c).wait_recv()
            emit(slot, mine, [c[0] for c in kids])
            c = copy_of(m)
            c.start()
            sends.append(c)
        last = [m for m in msgs if m[3] == 0]

        def finish():
            for c in last:
                copy_of(c).wait_recv()
            return [c[0] for c in last]

        return finish

    def all_gather(tree, buf, send_sem, recv_sem):
        msgs = messages(tree, n)

        def copy_of(m):
            slot, side, k, parent = m
            origin = at(me - side * parent)
            return pltpu.make_async_remote_copy(
                src_ref=buf.at[origin],
                dst_ref=buf.at[origin],
                send_sem=send_sem.at[slot],
                recv_sem=recv_sem.at[slot],
                device_id={"kv": at(me + side * (k - parent))},
                device_id_type=MESH,
            )

        def arrival(m):
            slot, side, k, parent = m
            origin = at(me - side * k)
            return pltpu.make_async_remote_copy(
                src_ref=buf.at[origin],
                dst_ref=buf.at[origin],
                send_sem=send_sem.at[slot],
                recv_sem=recv_sem.at[slot],
                device_id={"kv": at(me - side * k)},
                device_id_type=MESH,
            )

        def send(m):
            c = copy_of(m)
            c.start()
            sends.append(c)

        waited = set()
        firsts = [m for m in msgs if m[3] == 0]
        for m in sorted(firsts, key=lambda m: (-depth_below(msgs, m), -m[2])):
            send(m)

        def finish():
            todo = sorted([m for m in msgs if children_of(msgs, m[1], m[2])], key=lambda m: (level_of(tree, m[2]), m[2]))
            for m in todo:
                arrival(m).wait_recv()
                waited.add(m[0])
                for c in sorted(children_of(msgs, m[1], m[2]), key=lambda c: (-depth_below(msgs, c), -c[2])):
                    send(c)
            for m in msgs:
                if m[0] not in waited:
                    arrival(m).wait_recv()

        return finish

    def own_proj(d):
        return pf[d, :, 0:proj], pf[d, :, proj:]

    def sum_proj(mine, slots):
        a, g = mine
        for s in slots:
            a = a + pr[s, :, 0:proj].astype(F32)
            g = g + pr[s, :, proj:].astype(F32)
        return a, g

    def emit_proj(slot, mine, slots):
        a, g = sum_proj(mine, slots)
        ps[slot, :, 0:proj] = a.astype(BF16)
        ps[slot, :, proj:] = pack_gates(g).astype(BF16)

    finish = reduce_scatter(PROJ_TREE, own_proj, pr, emit_proj, ps_s, ps_r, ps)

    loads["wup"].wait()
    loads["wdn"].wait()
    up_x = to_partner(wupb.at[tp], wupb.at[tp], 1)
    up_x.start()
    dn_x = to_partner(wdnb.at[tp], wdnb.at[tp], 2)
    dn_x.start()
    sends += [up_x, dn_x]
    my_rows = pl.ds(pl.multiple_of(tp * half_rows, half_rows), half_rows)
    their_rows = pl.ds(pl.multiple_of(other * half_rows, half_rows), half_rows)
    tokrow[...] = jnp.concatenate([tokb[0, my_rows, :], tokb[1, my_rows, :]], axis=1).astype(F32)
    for name in ("ib", "fb", "stab", "nrm", "mem", "wo", "mgain"):
        loads[name].wait()

    slots = finish()
    total, gate = sum_proj(own_proj(me), slots)
    sf[:, 0:proj] = total
    squares = gate[:, gate_lanes : gate_lanes + 1] + gate[:, gate_lanes + 1 : gate_lanes + 2]
    rscale = lax.rsqrt(squares / width + EPSILON)
    q = sf[:, 0:hw] * rscale
    k = sf[:, hw : 2 * hw] * rscale * qk ** (-0.5)
    v = sf[:, 2 * hw : 2 * hw + vw] * rscale
    all_heads = wib.shape[1]

    def mine_of(x, first):
        return jnp.where(tp == 0, x[:, first : first + heads], x[:, first + heads : first + 2 * heads])

    log_in = mine_of(gate, 0) * rscale + mine_of(ibb[...], 0)
    fpre = mine_of(gate, all_heads) * rscale + mine_of(fbb[...], 0)
    log_forget = jnp.minimum(fpre, 0.0) - jnp.log(1.0 + jnp.exp(-jnp.abs(fpre)))
    carried = log_forget + stabb[...]
    snew = jnp.maximum(carried, log_in)
    take = jnp.exp(log_in - snew)
    keep = jnp.exp(carried - snew)
    stab_new[...] = snew

    hlane = lax.broadcasted_iota(jnp.int32, (seqs, hw), 1) // qk

    def spread(x):
        r = jnp.broadcast_to(x[:, 0:1], (seqs, hw))
        for h in range(1, heads):
            r = jnp.where(hlane == h, x[:, h : h + 1], r)
        return r

    def per_head(x):
        return [jnp.sum(jnp.where(hlane == h, x, 0.0), axis=1, keepdims=True) for h in range(heads)]

    tk = spread(take) * k
    nrm_new[...] = spread(keep) * nrmb[...] + tk
    scores = per_head(q * k)
    nqs = per_head(nrmb[...] * q)
    qt = q.T
    for s in range(seqs):
        for h in range(heads):
            col = qt[h * qk : (h + 1) * qk, s : s + 1]
            ro[s : s + 1, h * vd : (h + 1) * vd] = jnp.sum(memb[s, h] * col, axis=0, keepdims=True)
    hidden = []
    for h in range(heads):
        ts = take[:, h : h + 1] * scores[h]
        kp = keep[:, h : h + 1]
        numer = ts * v[:, h * vd : (h + 1) * vd] + kp * ro[:, h * vd : (h + 1) * vd]
        denom = ts + kp * nqs[h]
        cell = numer / jnp.maximum(jnp.abs(denom), 1.0)
        og = sf[:, 2 * hw + vw + h * vd : 2 * hw + vw + (h + 1) * vd] * rscale
        hidg[me, :, h * vd : (h + 1) * vd] = ((1.0 / (1.0 + jnp.exp(-og))) * cell).astype(BF16)
    finish = all_gather(HID_TREE, hidg, hid_s, hid_r)

    kt = tk.T
    for s in range(seqs):
        for h in range(heads):
            col = kt[h * qk : (h + 1) * qk, s : s + 1]
            memo[s, h] = keep[s : s + 1, h : h + 1] * memb[s, h] + col * v[s : s + 1, h * vd : (h + 1) * vd]
    mem_out = pltpu.make_async_copy(memo, mem_new, lsem.at[len(loads)])
    mem_out.start()

    finish()
    gathered = hidg[...].astype(F32).reshape(rows, vw).astype(BF16)
    opown[...] = jnp.dot(gathered, wob[...], preferred_element_type=F32)
    opsend[...] = opown[their_rows, :]
    op_x = to_partner(opsend, oprecv, 3)
    op_x.start()
    sends.append(op_x)
    op_x.wait_recv()
    middle = (tokrow[...] + opown[my_rows, :] + oprecv[...]).astype(BF16)
    midg[me] = middle
    all_gather(MID_TREE, midg, mid_s, mid_r)()

    up_x.wait_recv()
    dn_x.wait_recv()
    sq_sum = jnp.zeros((half_rows, 128), F32)
    acc = [None, None]
    for j in range(n // 2):
        pair = []
        for z in (2 * j, 2 * j + 1):
            m = midg[z].astype(F32)
            sq_sum = sq_sum + m * m
            pair.append((m * mgb[z : z + 1, :]).astype(BF16))
        x = jnp.concatenate(pair, axis=1)
        for u in range(2):
            d = jnp.dot(x, wupb[u, j * 256 : (j + 1) * 256, :], preferred_element_type=F32)
            acc[u] = d if acc[u] is None else acc[u] + d
    rmid = lax.rsqrt(jnp.sum(sq_sum, axis=1, keepdims=True) / width + EPSILON)
    sqd = [jnp.square(jnp.maximum(a * rmid, 0.0)).astype(BF16) for a in acc]

    def own_down(d):
        cols = pl.ds(pl.multiple_of(d * 128, 128), 128)
        return jnp.dot(sqd[0], wdnb[0, :, cols], preferred_element_type=F32) + jnp.dot(
            sqd[1], wdnb[1, :, cols], preferred_element_type=F32
        )

    def sum_down(a, slots):
        for s in slots:
            a = a + dr[s].astype(F32)
        return a

    def emit_down(slot, mine, slots):
        ds[slot] = sum_down(mine, slots).astype(BF16)

    finish = reduce_scatter(DOWN_TREE, own_down, dr, emit_down, dn_s, dn_r, ds)
    mine = own_down(me) + midg[me].astype(F32)
    mixed = sum_down(mine, finish()).astype(F32)
    left, right = mixed[:, 0:half_ch], mixed[:, half_ch : 2 * half_ch]
    fxs[...] = jnp.where(tp == 0, right, left).astype(BF16)
    fin_x = to_partner(fxs, fxr, 4)
    fin_x.start()
    sends.append(fin_x)
    out[my_rows, :] = jnp.where(tp == 0, left, right).astype(BF16)
    fin_x.wait_recv()
    out[their_rows, :] = fxr[...]
    mem_out.wait()
    for c in sends:
        c.wait_send()


def shards(n, *args):
    (tok, ngain, wq, wk, wv, wg, wi, wf, ib, fb, mem, nrm, stab, wo, mgain, wup, wdn) = args
    rows, half_ch = tok.shape
    chans = ngain.shape[0]
    seqs, heads, qk, vd = mem.shape
    hw, vw = heads * qk, heads * vd
    proj = 2 * hw + 2 * vw
    wide = proj + 128
    width = mgain.shape[0]
    hid = wup.shape[1]
    msgs = n - 1
    any_space = pl.BlockSpec(memory_space=pl.ANY)
    vmem = pl.BlockSpec(memory_space=pltpu.VMEM)
    dma = pltpu.SemaphoreType.DMA
    out = pl.pallas_call(
        functools.partial(kernel, n),
        out_shape=(
            jax.ShapeDtypeStruct(tok.shape, BF16),
            jax.ShapeDtypeStruct(mem.shape, F32),
            jax.ShapeDtypeStruct(nrm.shape, F32),
            jax.ShapeDtypeStruct(stab.shape, F32),
        ),
        in_specs=[any_space] * 17,
        out_specs=(vmem, any_space, vmem, vmem),
        scratch_shapes=[
            pltpu.VMEM((2, rows, half_ch), BF16),
            pltpu.VMEM((1, chans), F32),
            pltpu.VMEM((chans, proj), BF16),
            pltpu.VMEM(wi.shape, BF16),
            pltpu.VMEM(wf.shape, BF16),
            pltpu.VMEM((1, ib.shape[0]), F32),
            pltpu.VMEM((1, fb.shape[0]), F32),
            pltpu.VMEM(mem.shape, F32),
            pltpu.VMEM(mem.shape, F32),
            pltpu.VMEM(nrm.shape, F32),
            pltpu.VMEM(stab.shape, F32),
            pltpu.VMEM(wo.shape, BF16),
            pltpu.VMEM((width // 128, 128), F32),
            pltpu.VMEM((2, *wup.shape), BF16),
            pltpu.VMEM((2, *wdn.shape), BF16),
            pltpu.VMEM((n, seqs, wide), F32),
            pltpu.VMEM((msgs, seqs, wide), BF16),
            pltpu.VMEM((msgs, seqs, wide), BF16),
            pltpu.VMEM((seqs, proj), F32),
            pltpu.VMEM((seqs, vw), F32),
            pltpu.VMEM((rows // 2, 128), F32),
            pltpu.VMEM((n, seqs, vw), BF16),
            pltpu.VMEM((rows, 128), F32),
            pltpu.VMEM((rows // 2, 128), F32),
            pltpu.VMEM((rows // 2, 128), F32),
            pltpu.VMEM((n, rows // 2, 128), BF16),
            pltpu.VMEM((rows // 2, 128), F32),
            pltpu.VMEM((msgs, rows // 2, 128), BF16),
            pltpu.VMEM((msgs, rows // 2, 128), BF16),
            pltpu.VMEM((rows // 2, half_ch), BF16),
            pltpu.VMEM((rows // 2, half_ch), BF16),
            dma((20,)),
            dma((5,)),
            dma((5,)),
            dma((msgs,)),
            dma((msgs,)),
            dma((msgs,)),
            dma((msgs,)),
            dma((msgs,)),
            dma((msgs,)),
            dma((msgs,)),
            dma((msgs,)),
        ],
        compiler_params=pltpu.CompilerParams(collective_id=0, has_side_effects=True, vmem_limit_bytes=40 * 2**20),
        name="cell_step",
    )(
        tok,
        ngain.reshape(1, -1),
        wq,
        wk,
        wv,
        wg,
        wi,
        wf,
        ib.reshape(1, -1),
        fb.reshape(1, -1),
        mem,
        nrm,
        stab,
        wo,
        mgain.reshape(-1, 128),
        wup,
        wdn,
    )
    return tuple(out)


def solution(mesh):
    placed = (
        P(("grp", "dp"), ("kv", "tp")),
        P("kv"),
        P("kv", "tp"),
        P("kv", "tp"),
        P("kv", "tp"),
        P("kv", "tp"),
        P("kv", None),
        P("kv", None),
        P(),
        P(),
        P(("grp", "dp", "kv"), "tp", None, None),
        P(("grp", "dp", "kv"), "tp"),
        P(("grp", "dp", "kv"), "tp"),
        P("tp", "kv"),
        P(),
        P(None, ("kv", "tp")),
        P(("kv", "tp"), None),
    )
    return jax.shard_map(
        functools.partial(shards, mesh.shape["kv"]),
        mesh=mesh,
        in_specs=placed,
        out_specs=(
            P(("grp", "dp"), ("kv", "tp")),
            P(("grp", "dp", "kv"), "tp", None, None),
            P(("grp", "dp", "kv"), "tp"),
            P(("grp", "dp", "kv"), "tp"),
        ),
        check_vma=False,
    )
```

```python
import functools

import jax
import jax.numpy as jnp
from jax import lax
from jax.experimental import pallas as pl
from jax.experimental.pallas import tpu as pltpu
from jax.sharding import PartitionSpec as P

EPSILON = 1e-06
MESH = pl.DeviceIdType.MESH
F32 = jnp.float32
BF16 = jnp.bfloat16

TWO_LEVEL = {1: 0, 2: 0, 3: 0, 4: 0, 5: 4, 6: 4, 7: 4, 8: 4}
PROJ_TREE = TWO_LEVEL
HID_TREE = TWO_LEVEL
MID_TREE = TWO_LEVEL
DOWN_TREE = TWO_LEVEL
REACH = 4


def messages(tree, n):
    half = n // 2
    out = []
    for side, last in ((1, half), (-1, n - 1 - half)):
        for k in range(1, last + 1):
            out.append((len(out), side, k, tree[k]))
    return out


def children_of(msgs, side, k):
    return [m for m in msgs if m[1] == side and m[3] == k]


def depth_below(msgs, m):
    below = children_of(msgs, m[1], m[2])
    return 1 + max(depth_below(msgs, c) for c in below) if below else 0


def level_of(tree, k):
    return 0 if k == 0 else 1 + level_of(tree, tree[k])


def kernel(
    n,
    tok,
    ngain,
    wq,
    wk,
    wv,
    wg,
    wi,
    wf,
    ib,
    fb,
    mem,
    nrm,
    stab,
    wo,
    mgain,
    wup,
    wdn,
    out,
    mem_new,
    nrm_new,
    stab_new,
    tokb,
    ngv,
    wp,
    wib,
    ibb,
    fbb,
    memb,
    nrmb,
    stabb,
    wob,
    mgb,
    wupb,
    wdnb,
    pf,
    ps,
    pr,
    sf,
    ro,
    tokrow,
    hidg,
    opown,
    opsend,
    oprecv,
    midg,
    down_own,
    ds,
    dr,
    mixt,
    fxs,
    fxr,
    lsem,
    xs,
    xr,
    ps_s,
    ps_r,
    hid_s,
    hid_r,
    mid_s,
    mid_r,
    dn_s,
    dn_r,
):
    me = lax.axis_index("kv")
    tp = lax.axis_index("tp")
    other = 1 - tp
    half_ch, rows = tokb.shape[1:]
    seqs, heads, qk, vd = memb.shape
    hw = heads * qk
    vw = heads * vd
    proj = wp.shape[1]
    width = mgb.shape[0] * mgb.shape[1]
    half_rows = rows // 2

    def at(z):
        return lax.rem(z + 2 * n, n)

    barrier = pltpu.get_barrier_semaphore()
    for step in range(1, REACH + 1):
        for side in (1, -1):
            pl.semaphore_signal(barrier, inc=1, device_id={"kv": at(me + side * step)}, device_id_type=MESH)
    pl.semaphore_signal(barrier, inc=1, device_id={"tp": other}, device_id_type=MESH)

    loads = {}

    def load(name, src, dst):
        c = pltpu.make_async_copy(src, dst, lsem.at[len(loads)])
        c.start()
        loads[name] = c

    load("tok", tok, tokb.at[tp])
    load("ngain", ngain, ngv)
    load("wq", wq, wp.at[:, 0:hw])
    load("wk", wk, wp.at[:, hw : 2 * hw])
    load("wv", wv, wp.at[:, 2 * hw : 2 * hw + vw])
    load("wg", wg, wp.at[:, 2 * hw + vw : proj])
    load("wi", wi, wib.at[0])
    load("wf", wf, wib.at[1])
    load("ib", ib, ibb)
    load("fb", fb, fbb)
    load("stab", stab, stabb)
    load("nrm", nrm, nrmb)
    load("mem", mem, memb)
    load("wo", wo, wob)
    load("mgain", mgain, mgb)
    load("wup", wup, wupb.at[tp])
    load("wdn", wdn, wdnb.at[tp])

    pl.semaphore_wait(barrier, 2 * REACH + 1)

    def to_partner(src, dst, i):
        return pltpu.make_async_remote_copy(
            src_ref=src, dst_ref=dst, send_sem=xs.at[i], recv_sem=xr.at[i], device_id={"tp": other}, device_id_type=MESH
        )

    loads["tok"].wait()
    tok_x = to_partner(tokb.at[tp], tokb.at[tp], 0)
    tok_x.start()
    sends = [tok_x]

    for name in ("ngain", "wq", "wk", "wv", "wg", "wi", "wf"):
        loads[name].wait()

    gate_lanes = 2 * wib.shape[1]
    lane128 = lax.broadcasted_iota(jnp.int32, (rows, 128), 1)
    gw = jnp.concatenate(
        [wib[0].astype(F32), wib[1].astype(F32), jnp.zeros((128 - gate_lanes, 2 * half_ch), F32)], axis=0
    ).astype(BF16)
    tok_x.wait_recv()
    t = jnp.concatenate([tokb[0], tokb[1]], axis=0).astype(F32).T
    scaled = (t * ngv[...]).astype(BF16)
    main = jnp.dot(scaled, wp[...], preferred_element_type=F32)
    gates = lax.dot_general(scaled, gw, (((1,), (1,)), ((), ())), preferred_element_type=F32)
    pf[:, :, 0:proj] = main.reshape(n, seqs, proj)
    pf[:, :, proj:] = jnp.where(lane128 == gate_lanes, jnp.sum(t * t, axis=1, keepdims=True), gates).reshape(n, seqs, 128)
    tokrow[...] = t

    lane8 = lax.broadcasted_iota(jnp.int32, (seqs, 128), 1)

    def pack_gates(g):
        total = g[:, gate_lanes : gate_lanes + 1] + g[:, gate_lanes + 1 : gate_lanes + 2]
        upper = total.astype(BF16).astype(F32)
        return jnp.where(lane8 == gate_lanes, upper, jnp.where(lane8 == gate_lanes + 1, total - upper, g))

    def reduce_scatter(tree, own, recv, emit, send_sem, recv_sem, send_buf):
        msgs = messages(tree, n)

        def copy_of(m):
            slot, side, k, parent = m
            return pltpu.make_async_remote_copy(
                src_ref=send_buf.at[slot],
                dst_ref=recv.at[slot],
                send_sem=send_sem.at[slot],
                recv_sem=recv_sem.at[slot],
                device_id={"kv": at(me - side * (k - parent))},
                device_id_type=MESH,
            )

        order = sorted(msgs, key=lambda m: (depth_below(msgs, m), -level_of(tree, m[2]), -m[2]))
        for m in order:
            slot, side, k, parent = m
            mine = own(at(me - side * k))
            kids = children_of(msgs, side, k)
            for c in kids:
                copy_of(c).wait_recv()
            emit(slot, mine, [c[0] for c in kids])
            c = copy_of(m)
            c.start()
            sends.append(c)
        last = [m for m in msgs if m[3] == 0]

        def finish():
            for c in last:
                copy_of(c).wait_recv()
            return [c[0] for c in last]

        return finish

    def all_gather(tree, buf, send_sem, recv_sem):
        msgs = messages(tree, n)

        def copy_of(m):
            slot, side, k, parent = m
            origin = at(me - side * parent)
            return pltpu.make_async_remote_copy(
                src_ref=buf.at[origin],
                dst_ref=buf.at[origin],
                send_sem=send_sem.at[slot],
                recv_sem=recv_sem.at[slot],
                device_id={"kv": at(me + side * (k - parent))},
                device_id_type=MESH,
            )

        def arrival(m):
            slot, side, k, parent = m
            origin = at(me - side * k)
            return pltpu.make_async_remote_copy(
                src_ref=buf.at[origin],
                dst_ref=buf.at[origin],
                send_sem=send_sem.at[slot],
                recv_sem=recv_sem.at[slot],
                device_id={"kv": at(me - side * k)},
                device_id_type=MESH,
            )

        def send(m):
            c = copy_of(m)
            c.start()
            sends.append(c)

        waited = set()
        firsts = [m for m in msgs if m[3] == 0]
        for m in sorted(firsts, key=lambda m: (-depth_below(msgs, m), -m[2])):
            send(m)

        def finish():
            todo = sorted([m for m in msgs if children_of(msgs, m[1], m[2])], key=lambda m: (level_of(tree, m[2]), m[2]))
            for m in todo:
                arrival(m).wait_recv()
                waited.add(m[0])
                for c in sorted(children_of(msgs, m[1], m[2]), key=lambda c: (-depth_below(msgs, c), -c[2])):
                    send(c)
            for m in msgs:
                if m[0] not in waited:
                    arrival(m).wait_recv()

        return finish

    def own_proj(d):
        return pf[d, :, 0:proj], pf[d, :, proj:]

    def sum_proj(mine, slots):
        a, g = mine
        for s in slots:
            a = a + pr[s, :, 0:proj].astype(F32)
            g = g + pr[s, :, proj:].astype(F32)
        return a, g

    def emit_proj(slot, mine, slots):
        a, g = sum_proj(mine, slots)
        ps[slot, :, 0:proj] = a.astype(BF16)
        ps[slot, :, proj:] = pack_gates(g).astype(BF16)

    finish = reduce_scatter(PROJ_TREE, own_proj, pr, emit_proj, ps_s, ps_r, ps)

    loads["wup"].wait()
    loads["wdn"].wait()
    up_x = to_partner(wupb.at[tp], wupb.at[tp], 1)
    up_x.start()
    dn_x = to_partner(wdnb.at[tp], wdnb.at[tp], 2)
    dn_x.start()
    sends += [up_x, dn_x]
    my_rows = pl.ds(pl.multiple_of(tp * half_rows, half_rows), half_rows)
    their_rows = pl.ds(pl.multiple_of(other * half_rows, half_rows), half_rows)
    for name in ("ib", "fb", "stab", "nrm", "mem", "wo", "mgain"):
        loads[name].wait()

    slots = finish()
    total, gate = sum_proj(own_proj(me), slots)
    sf[:, 0:proj] = total
    squares = gate[:, gate_lanes : gate_lanes + 1] + gate[:, gate_lanes + 1 : gate_lanes + 2]
    rscale = lax.rsqrt(squares / width + EPSILON)
    q = sf[:, 0:hw] * rscale
    k = sf[:, hw : 2 * hw] * rscale * qk ** (-0.5)
    v = sf[:, 2 * hw : 2 * hw + vw] * rscale
    all_heads = wib.shape[1]

    def mine_of(x, first):
        return jnp.where(tp == 0, x[:, first : first + heads], x[:, first + heads : first + 2 * heads])

    log_in = mine_of(gate, 0) * rscale + mine_of(ibb[...], 0)
    fpre = mine_of(gate, all_heads) * rscale + mine_of(fbb[...], 0)
    log_forget = jnp.minimum(fpre, 0.0) - jnp.log(1.0 + jnp.exp(-jnp.abs(fpre)))
    carried = log_forget + stabb[...].T
    snew = jnp.maximum(carried, log_in)
    take = jnp.exp(log_in - snew)
    keep = jnp.exp(carried - snew)
    stab_new[...] = snew.T

    hlane = lax.broadcasted_iota(jnp.int32, (seqs, hw), 1) // qk

    def spread(x):
        r = jnp.broadcast_to(x[:, 0:1], (seqs, hw))
        for h in range(1, heads):
            r = jnp.where(hlane == h, x[:, h : h + 1], r)
        return r

    def per_head(x):
        return [jnp.sum(jnp.where(hlane == h, x, 0.0), axis=1, keepdims=True) for h in range(heads)]

    tk = spread(take) * k
    nrm_new[...] = spread(keep) * nrmb[...] + tk
    scores = per_head(q * k)
    nqs = per_head(nrmb[...] * q)
    qt = q.T
    for s in range(seqs):
        for h in range(heads):
            col = qt[h * qk : (h + 1) * qk, s : s + 1]
            ro[s : s + 1, h * vd : (h + 1) * vd] = jnp.sum(memb[s, h] * col, axis=0, keepdims=True)
    hidden = []
    for h in range(heads):
        ts = take[:, h : h + 1] * scores[h]
        kp = keep[:, h : h + 1]
        numer = ts * v[:, h * vd : (h + 1) * vd] + kp * ro[:, h * vd : (h + 1) * vd]
        denom = ts + kp * nqs[h]
        cell = numer / jnp.maximum(jnp.abs(denom), 1.0)
        og = sf[:, 2 * hw + vw + h * vd : 2 * hw + vw + (h + 1) * vd] * rscale
        hidg[me, :, h * vd : (h + 1) * vd] = ((1.0 / (1.0 + jnp.exp(-og))) * cell).astype(BF16)
    finish = all_gather(HID_TREE, hidg, hid_s, hid_r)

    kt = tk.T
    for s in range(seqs):
        for h in range(heads):
            col = kt[h * qk : (h + 1) * qk, s : s + 1]
            mem_new[s, h] = keep[s : s + 1, h : h + 1] * memb[s, h] + col * v[s : s + 1, h * vd : (h + 1) * vd]

    finish()
    gathered = hidg[...].astype(F32).reshape(rows, vw).astype(BF16)
    opown[...] = jnp.dot(gathered, wob[...], preferred_element_type=F32)
    opsend[...] = opown[their_rows, :]
    op_x = to_partner(opsend, oprecv, 3)
    op_x.start()
    sends.append(op_x)
    op_x.wait_recv()
    middle = (tokrow[my_rows, :] + opown[my_rows, :] + oprecv[...]).astype(BF16)
    midg[me] = middle
    all_gather(MID_TREE, midg, mid_s, mid_r)()

    up_x.wait_recv()
    dn_x.wait_recv()
    sq_sum = jnp.zeros((half_rows, 128), F32)
    acc = [None, None]
    for j in range(n // 2):
        pair = []
        for z in (2 * j, 2 * j + 1):
            m = midg[z].astype(F32)
            sq_sum = sq_sum + m * m
            pair.append((m * mgb[z : z + 1, :]).astype(BF16))
        x = jnp.concatenate(pair, axis=1)
        for u in range(2):
            d = jnp.dot(x, wupb[u, j * 256 : (j + 1) * 256, :], preferred_element_type=F32)
            acc[u] = d if acc[u] is None else acc[u] + d
    rmid = lax.rsqrt(jnp.sum(sq_sum, axis=1, keepdims=True) / width + EPSILON)
    sqd = [jnp.square(jnp.maximum(a * rmid, 0.0)).astype(BF16) for a in acc]

    def own_down(d):
        cols = pl.ds(pl.multiple_of(d * 128, 128), 128)
        return jnp.dot(sqd[0], wdnb[0, :, cols], preferred_element_type=F32) + jnp.dot(
            sqd[1], wdnb[1, :, cols], preferred_element_type=F32
        )

    def sum_down(a, slots):
        for s in slots:
            a = a + dr[s].astype(F32)
        return a

    def emit_down(slot, mine, slots):
        ds[slot] = sum_down(mine, slots).astype(BF16)

    finish = reduce_scatter(DOWN_TREE, own_down, dr, emit_down, dn_s, dn_r, ds)
    mine = own_down(me) + midg[me].astype(F32)
    mixed = sum_down(mine, finish()).astype(F32)
    mixt[...] = mixed.T
    mine = pl.ds(pl.multiple_of(tp * half_ch, half_ch), half_ch)
    theirs = pl.ds(pl.multiple_of(other * half_ch, half_ch), half_ch)
    fxs[...] = mixt[theirs, :].astype(BF16)
    fin_x = to_partner(fxs, fxr, 4)
    fin_x.start()
    sends.append(fin_x)
    kept = mixt[mine, :]
    fin_x.wait_recv()
    got = fxr[...].astype(F32)
    out[...] = jnp.where(tp == 0, jnp.concatenate([kept, got], axis=1), jnp.concatenate([got, kept], axis=1)).astype(BF16)
    for c in sends:
        c.wait_send()


def hand_over(*refs):
    count = (len(refs) - 1) // 2
    sems = refs[-1]
    copies = [pltpu.make_async_copy(refs[i], refs[count + i], sems.at[i]) for i in range(count)]
    for c in copies:
        c.start()
    for c in copies:
        c.wait()


def shards(n, *args):
    (tok, ngain, wq, wk, wv, wg, wi, wf, ib, fb, mem, nrm, stab, wo, mgain, wup, wdn) = args
    rows, half_ch = tok.shape
    chans = ngain.shape[0]
    seqs, heads, qk, vd = mem.shape
    hw, vw = heads * qk, heads * vd
    proj = 2 * hw + 2 * vw
    wide = proj + 128
    width = mgain.shape[0]
    hid = wup.shape[1]
    msgs = n - 1
    any_space = pl.BlockSpec(memory_space=pl.ANY)
    vmem = pl.BlockSpec(memory_space=pltpu.VMEM)
    dma = pltpu.SemaphoreType.DMA
    out = pl.pallas_call(
        functools.partial(kernel, n),
        out_shape=(
            pltpu.VMEM((half_ch, rows), BF16),
            pltpu.VMEM(mem.shape, F32),
            pltpu.VMEM(nrm.shape, F32),
            pltpu.VMEM((heads, seqs), F32),
        ),
        in_specs=[any_space] * 17,
        out_specs=(vmem,) * 4,
        scratch_shapes=[
            pltpu.VMEM((2, half_ch, rows), BF16),
            pltpu.VMEM((1, chans), F32),
            pltpu.VMEM((chans, proj), BF16),
            pltpu.VMEM((2, wi.shape[1], chans), BF16),
            pltpu.VMEM((1, ib.shape[0]), F32),
            pltpu.VMEM((1, fb.shape[0]), F32),
            pltpu.VMEM(mem.shape, F32),
            pltpu.VMEM(nrm.shape, F32),
            pltpu.VMEM((heads, seqs), F32),
            pltpu.VMEM(wo.shape, BF16),
            pltpu.VMEM((width // 128, 128), F32),
            pltpu.VMEM((2, *wup.shape), BF16),
            pltpu.VMEM((2, *wdn.shape), BF16),
            pltpu.VMEM((n, seqs, wide), F32),
            pltpu.VMEM((msgs, seqs, wide), BF16),
            pltpu.VMEM((msgs, seqs, wide), BF16),
            pltpu.VMEM((seqs, proj), F32),
            pltpu.VMEM((seqs, vw), F32),
            pltpu.VMEM((rows, 128), F32),
            pltpu.VMEM((n, seqs, vw), BF16),
            pltpu.VMEM((rows, 128), F32),
            pltpu.VMEM((rows // 2, 128), F32),
            pltpu.VMEM((rows // 2, 128), F32),
            pltpu.VMEM((n, rows // 2, 128), BF16),
            pltpu.VMEM((rows // 2, 128), F32),
            pltpu.VMEM((msgs, rows // 2, 128), BF16),
            pltpu.VMEM((msgs, rows // 2, 128), BF16),
            pltpu.VMEM((2 * half_ch, rows // 2), F32),
            pltpu.VMEM((half_ch, rows // 2), BF16),
            pltpu.VMEM((half_ch, rows // 2), BF16),
            dma((20,)),
            dma((5,)),
            dma((5,)),
            dma((msgs,)),
            dma((msgs,)),
            dma((msgs,)),
            dma((msgs,)),
            dma((msgs,)),
            dma((msgs,)),
            dma((msgs,)),
            dma((msgs,)),
        ],
        compiler_params=pltpu.CompilerParams(collective_id=0, has_side_effects=True, vmem_limit_bytes=40 * 2**20),
        name="cell_step",
    )(*[pltpu.with_memory_space_constraint(x, pltpu.HBM) for x in (
        tok.T,
        ngain.reshape(1, -1),
        wq,
        wk,
        wv,
        wg,
        wi.T,
        wf.T,
        ib.reshape(1, -1),
        fb.reshape(1, -1),
        mem,
        nrm,
        stab.T,
        wo,
        mgain.reshape(-1, 128),
        wup,
        wdn,
    )])
    out = pl.pallas_call(
        hand_over,
        out_shape=tuple(jax.ShapeDtypeStruct(o.shape, o.dtype) for o in out),
        in_specs=[vmem] * 4,
        out_specs=(any_space,) * 4,
        scratch_shapes=[dma((4,))],
        name="hand_over",
    )(*[pltpu.with_memory_space_constraint(o, pltpu.VMEM) for o in out])
    return out[0].T, out[1], out[2], out[3].T


def solution(mesh):
    placed = (
        P(("grp", "dp"), ("kv", "tp")),
        P("kv"),
        P("kv", "tp"),
        P("kv", "tp"),
        P("kv", "tp"),
        P("kv", "tp"),
        P("kv", None),
        P("kv", None),
        P(),
        P(),
        P(("grp", "dp", "kv"), "tp", None, None),
        P(("grp", "dp", "kv"), "tp"),
        P(("grp", "dp", "kv"), "tp"),
        P("tp", "kv"),
        P(),
        P(None, ("kv", "tp")),
        P(("kv", "tp"), None),
    )
    return jax.shard_map(
        functools.partial(shards, mesh.shape["kv"]),
        mesh=mesh,
        in_specs=placed,
        out_specs=(
            P(("grp", "dp"), ("kv", "tp")),
            P(("grp", "dp", "kv"), "tp", None, None),
            P(("grp", "dp", "kv"), "tp"),
            P(("grp", "dp", "kv"), "tp"),
        ),
        check_vma=False,
    )
```

```python
import functools

import jax
import jax.numpy as jnp
from jax import lax
from jax.experimental import pallas as pl
from jax.experimental.pallas import tpu as pltpu
from jax.sharding import PartitionSpec as P

EPSILON = 1e-06
MESH = pl.DeviceIdType.MESH
F32 = jnp.float32
BF16 = jnp.bfloat16

TWO_LEVEL = {1: 0, 2: 0, 3: 0, 4: 0, 5: 4, 6: 4, 7: 4, 8: 4}
PROJ_TREE = TWO_LEVEL
HID_TREE = TWO_LEVEL
MID_TREE = TWO_LEVEL
DOWN_TREE = TWO_LEVEL


def messages(tree, n):
    half = n // 2
    out = []
    for side, last in ((1, half), (-1, n - 1 - half)):
        for k in range(1, last + 1):
            out.append((len(out), side, k, tree[k]))
    return out


def children_of(msgs, side, k):
    return [m for m in msgs if m[1] == side and m[3] == k]


def depth_below(msgs, m):
    below = children_of(msgs, m[1], m[2])
    return 1 + max(depth_below(msgs, c) for c in below) if below else 0


def level_of(tree, k):
    return 0 if k == 0 else 1 + level_of(tree, tree[k])


def kernel(
    n,
    tok,
    ngain,
    wq,
    wk,
    wv,
    wg,
    wi,
    wf,
    ib,
    fb,
    mem,
    nrm,
    stab,
    wo,
    mgain,
    wup,
    wdn,
    out,
    mem_new,
    nrm_new,
    stab_new,
    tokb,
    ngv,
    wp,
    wib,
    ibb,
    fbb,
    memb,
    nrmb,
    stabb,
    wob,
    mgb,
    wupb,
    wdnb,
    pf,
    ps,
    pr,
    sf,
    ro,
    tokrow,
    hidg,
    opown,
    opsend,
    oprecv,
    midg,
    ds,
    dr,
    fs,
    fr,
    fxs,
    fxr,
    lsem,
    xs,
    xr,
    ps_s,
    ps_r,
    hid_s,
    hid_r,
    mid_s,
    mid_r,
    dn_s,
    dn_r,
    fs_s,
    fr_r,
    near,
):
    me = lax.axis_index("kv")
    tp = lax.axis_index("tp")
    other = 1 - tp
    half_ch, rows = tokb.shape[1:]
    seqs, heads, qk, vd = memb.shape
    hw = heads * qk
    vw = heads * vd
    proj = wp.shape[1]
    width = mgb.shape[0] * mgb.shape[1]
    half_rows = rows // 2

    def at(z):
        return lax.rem(z + 2 * n, n)

    barrier = pltpu.get_barrier_semaphore()
    for side in (1, -1):
        pl.semaphore_signal(barrier, inc=1, device_id={"kv": at(me + side)}, device_id_type=MESH)
    pl.semaphore_signal(barrier, inc=1, device_id={"tp": other}, device_id_type=MESH)

    def tell(i, step):
        for side in (1, -1):
            pl.semaphore_signal(near.at[i], inc=1, device_id={"kv": at(me + side * step)}, device_id_type=MESH)

    def hear(i):
        pl.semaphore_wait(near.at[i], 2)

    loads = {}

    def load(name, src, dst):
        c = pltpu.make_async_copy(src, dst, lsem.at[len(loads)])
        c.start()
        loads[name] = c

    load("tok", tok, tokb.at[tp])
    load("ngain", ngain, ngv)
    load("wq", wq, wp.at[:, 0:hw])
    load("wk", wk, wp.at[:, hw : 2 * hw])
    load("wv", wv, wp.at[:, 2 * hw : 2 * hw + vw])
    load("wg", wg, wp.at[:, 2 * hw + vw : proj])
    load("wi", wi, wib.at[0])
    load("wf", wf, wib.at[1])
    load("ib", ib, ibb)
    load("fb", fb, fbb)
    load("stab", stab, stabb)
    load("nrm", nrm, nrmb)
    load("mem", mem, memb)
    load("wo", wo, wob)
    load("mgain", mgain, mgb)
    load("wup", wup, wupb.at[tp])
    load("wdn", wdn, wdnb.at[tp])

    pl.semaphore_wait(barrier, 3)
    tell(0, 1)

    def to_partner(src, dst, i):
        return pltpu.make_async_remote_copy(
            src_ref=src, dst_ref=dst, send_sem=xs.at[i], recv_sem=xr.at[i], device_id={"tp": other}, device_id_type=MESH
        )

    loads["tok"].wait()
    tok_x = to_partner(tokb.at[tp], tokb.at[tp], 0)
    tok_x.start()
    sends = [tok_x]

    for name in ("ngain", "wq", "wk", "wv", "wg", "wi", "wf"):
        loads[name].wait()

    gate_lanes = 2 * wib.shape[1]
    lane128 = lax.broadcasted_iota(jnp.int32, (rows, 128), 1)
    gw = jnp.concatenate(
        [wib[0].astype(F32), wib[1].astype(F32), jnp.zeros((128 - gate_lanes, 2 * half_ch), F32)], axis=0
    ).astype(BF16)
    hear(0)
    tell(1, 2)
    tok_x.wait_recv()
    t = jnp.concatenate([tokb[0], tokb[1]], axis=0).astype(F32).T
    scaled = (t * ngv[...]).astype(BF16)
    main = jnp.dot(scaled, wp[...], preferred_element_type=F32)
    gates = lax.dot_general(scaled, gw, (((1,), (1,)), ((), ())), preferred_element_type=F32)
    pf[:, :, 0:proj] = main.reshape(n, seqs, proj)
    pf[:, :, proj:] = jnp.where(lane128 == gate_lanes, jnp.sum(t * t, axis=1, keepdims=True), gates).reshape(n, seqs, 128)
    tokrow[...] = t

    lane8 = lax.broadcasted_iota(jnp.int32, (seqs, 128), 1)

    def pack_gates(g):
        total = g[:, gate_lanes : gate_lanes + 1] + g[:, gate_lanes + 1 : gate_lanes + 2]
        upper = total.astype(BF16).astype(F32)
        return jnp.where(lane8 == gate_lanes, upper, jnp.where(lane8 == gate_lanes + 1, total - upper, g))

    def reduce_scatter(tree, own, emit, copies_of):
        msgs = messages(tree, n)
        order = sorted(msgs, key=lambda m: (depth_below(msgs, m), -level_of(tree, m[2]), -m[2]))
        for m in order:
            slot, side, k, parent = m
            mine = own(at(me - side * k))
            kids = children_of(msgs, side, k)
            for c in kids:
                copies_of(c)[0].wait_recv()
            emit(m, mine, [c[0] for c in kids])
            for c in copies_of(m):
                c.start()
                sends.append(c)
        return [m for m in msgs if m[3] == 0]

    def along(m, src, dst, send_sem, recv_sem, core=None):
        slot, side, k, parent = m
        where = {"kv": at(me - side * (k - parent))}
        if core is not None:
            where["tp"] = core
        return pltpu.make_async_remote_copy(
            src_ref=src, dst_ref=dst, send_sem=send_sem, recv_sem=recv_sem, device_id=where, device_id_type=MESH
        )

    def all_gather(tree, buf, send_sem, recv_sem):
        msgs = messages(tree, n)

        def copy_of(m):
            slot, side, k, parent = m
            origin = at(me - side * parent)
            return pltpu.make_async_remote_copy(
                src_ref=buf.at[origin],
                dst_ref=buf.at[origin],
                send_sem=send_sem.at[slot],
                recv_sem=recv_sem.at[slot],
                device_id={"kv": at(me + side * (k - parent))},
                device_id_type=MESH,
            )

        def arrival(m):
            slot, side, k, parent = m
            origin = at(me - side * k)
            return pltpu.make_async_remote_copy(
                src_ref=buf.at[origin],
                dst_ref=buf.at[origin],
                send_sem=send_sem.at[slot],
                recv_sem=recv_sem.at[slot],
                device_id={"kv": at(me - side * k)},
                device_id_type=MESH,
            )

        def send(m):
            c = copy_of(m)
            c.start()
            sends.append(c)

        waited = set()
        firsts = [m for m in msgs if m[3] == 0]
        for m in sorted(firsts, key=lambda m: (-depth_below(msgs, m), -m[2])):
            send(m)

        def finish():
            todo = sorted([m for m in msgs if children_of(msgs, m[1], m[2])], key=lambda m: (level_of(tree, m[2]), m[2]))
            for m in todo:
                arrival(m).wait_recv()
                waited.add(m[0])
                for c in sorted(children_of(msgs, m[1], m[2]), key=lambda c: (-depth_below(msgs, c), -c[2])):
                    send(c)
            for m in msgs:
                if m[0] not in waited:
                    arrival(m).wait_recv()

        return finish

    hear(1)

    def own_proj(d):
        return pf[d, :, 0:proj], pf[d, :, proj:]

    def sum_proj(mine, slots):
        a, g = mine
        for s in slots:
            a = a + pr[s, :, 0:proj].astype(F32)
            g = g + pr[s, :, proj:].astype(F32)
        return a, g

    def emit_proj(m, mine, slots):
        slot = m[0]
        a, g = sum_proj(mine, slots)
        ps[slot, :, 0:proj] = a.astype(BF16)
        ps[slot, :, proj:] = pack_gates(g).astype(BF16)

    def proj_copies(m):
        i = m[0]
        return [along(m, ps.at[i], pr.at[i], ps_s.at[i], ps_r.at[i])]

    last = reduce_scatter(PROJ_TREE, own_proj, emit_proj, proj_copies)

    loads["wup"].wait()
    loads["wdn"].wait()
    up_x = to_partner(wupb.at[tp], wupb.at[tp], 1)
    up_x.start()
    dn_x = to_partner(wdnb.at[tp], wdnb.at[tp], 2)
    dn_x.start()
    sends += [up_x, dn_x]
    my_rows = pl.ds(pl.multiple_of(tp * half_rows, half_rows), half_rows)
    their_rows = pl.ds(pl.multiple_of(other * half_rows, half_rows), half_rows)
    for name in ("ib", "fb", "stab", "nrm", "mem", "wo", "mgain"):
        loads[name].wait()

    for m in last:
        proj_copies(m)[0].wait_recv()
    slots = [m[0] for m in last]
    total, gate = sum_proj(own_proj(me), slots)
    sf[:, 0:proj] = total
    squares = gate[:, gate_lanes : gate_lanes + 1] + gate[:, gate_lanes + 1 : gate_lanes + 2]
    rscale = lax.rsqrt(squares / width + EPSILON)
    q = sf[:, 0:hw] * rscale
    k = sf[:, hw : 2 * hw] * rscale * qk ** (-0.5)
    v = sf[:, 2 * hw : 2 * hw + vw] * rscale
    all_heads = wib.shape[1]

    def mine_of(x, first):
        return jnp.where(tp == 0, x[:, first : first + heads], x[:, first + heads : first + 2 * heads])

    log_in = mine_of(gate, 0) * rscale + mine_of(ibb[...], 0)
    fpre = mine_of(gate, all_heads) * rscale + mine_of(fbb[...], 0)
    log_forget = jnp.minimum(fpre, 0.0) - jnp.log(1.0 + jnp.exp(-jnp.abs(fpre)))
    carried = log_forget + stabb[...].T
    snew = jnp.maximum(carried, log_in)
    take = jnp.exp(log_in - snew)
    keep = jnp.exp(carried - snew)
    stab_new[...] = snew.T

    hlane = lax.broadcasted_iota(jnp.int32, (seqs, hw), 1) // qk

    def spread(x):
        r = jnp.broadcast_to(x[:, 0:1], (seqs, hw))
        for h in range(1, heads):
            r = jnp.where(hlane == h, x[:, h : h + 1], r)
        return r

    def per_head(x):
        return [jnp.sum(jnp.where(hlane == h, x, 0.0), axis=1, keepdims=True) for h in range(heads)]

    tk = spread(take) * k
    nrm_new[...] = spread(keep) * nrmb[...] + tk
    scores = per_head(q * k)
    nqs = per_head(nrmb[...] * q)
    qt = q.T
    for s in range(seqs):
        for h in range(heads):
            col = qt[h * qk : (h + 1) * qk, s : s + 1]
            ro[s : s + 1, h * vd : (h + 1) * vd] = jnp.sum(memb[s, h] * col, axis=0, keepdims=True)
    hidden = []
    for h in range(heads):
        ts = take[:, h : h + 1] * scores[h]
        kp = keep[:, h : h + 1]
        numer = ts * v[:, h * vd : (h + 1) * vd] + kp * ro[:, h * vd : (h + 1) * vd]
        denom = ts + kp * nqs[h]
        cell = numer / jnp.maximum(jnp.abs(denom), 1.0)
        og = sf[:, 2 * hw + vw + h * vd : 2 * hw + vw + (h + 1) * vd] * rscale
        hidg[me, :, h * vd : (h + 1) * vd] = ((1.0 / (1.0 + jnp.exp(-og))) * cell).astype(BF16)
    finish = all_gather(HID_TREE, hidg, hid_s, hid_r)

    kt = tk.T
    for s in range(seqs):
        for h in range(heads):
            col = kt[h * qk : (h + 1) * qk, s : s + 1]
            mem_new[s, h] = keep[s : s + 1, h : h + 1] * memb[s, h] + col * v[s : s + 1, h * vd : (h + 1) * vd]

    finish()
    gathered = hidg[...].astype(F32).reshape(rows, vw).astype(BF16)
    opown[...] = jnp.dot(gathered, wob[...], preferred_element_type=F32)
    opsend[...] = opown[their_rows, :]
    op_x = to_partner(opsend, oprecv, 3)
    op_x.start()
    sends.append(op_x)
    op_x.wait_recv()
    middle = (tokrow[my_rows, :] + opown[my_rows, :] + oprecv[...]).astype(BF16)
    midg[me] = middle
    all_gather(MID_TREE, midg, mid_s, mid_r)()

    up_x.wait_recv()
    dn_x.wait_recv()
    sq_sum = jnp.zeros((half_rows, 128), F32)
    acc = [None, None]
    for j in range(n // 2):
        pair = []
        for z in (2 * j, 2 * j + 1):
            m = midg[z].astype(F32)
            sq_sum = sq_sum + m * m
            pair.append((m * mgb[z : z + 1, :]).astype(BF16))
        x = jnp.concatenate(pair, axis=1)
        for u in range(2):
            d = jnp.dot(x, wupb[u, j * 256 : (j + 1) * 256, :], preferred_element_type=F32)
            acc[u] = d if acc[u] is None else acc[u] + d
    rmid = lax.rsqrt(jnp.sum(sq_sum, axis=1, keepdims=True) / width + EPSILON)
    sqd = [jnp.square(jnp.maximum(a * rmid, 0.0)).astype(BF16) for a in acc]

    def own_down(d):
        cols = pl.ds(pl.multiple_of(d * 128, 128), 128)
        return jnp.dot(sqd[0], wdnb[0, :, cols], preferred_element_type=F32) + jnp.dot(
            sqd[1], wdnb[1, :, cols], preferred_element_type=F32
        )

    def sum_down(a, slots):
        for s in slots:
            a = a + dr[s].astype(F32)
        return a

    def halves(a):
        return [
            jnp.concatenate([a[0:quarter, h : h + half_ch], a[quarter : 2 * quarter, h : h + half_ch]], axis=1)
            for h in (0, half_ch)
        ]

    quarter = half_rows // 2
    msgs_n = n - 1

    def emit_down(m, mine, slots):
        a = sum_down(mine, slots)
        if m[3] == 0:
            fs[m[0], 0], fs[m[0], 1] = [x.astype(BF16) for x in halves(a)]
        else:
            ds[m[0]] = a.astype(BF16)

    def down_copies(m):
        i = m[0]
        if m[3] == 0:
            return [
                along(m, fs.at[i, c], fr.at[tp, i], fs_s.at[2 * i + c], fr_r.at[tp * msgs_n + i], c) for c in range(2)
            ]
        return [along(m, ds.at[i], dr.at[i], dn_s.at[i], dn_r.at[i])]

    last = reduce_scatter(DOWN_TREE, own_down, emit_down, down_copies)
    left, right = halves(own_down(me) + midg[me].astype(F32))
    fxs[...] = jnp.where(tp == 0, right, left)
    fin_x = to_partner(fxs, fxr, 4)
    fin_x.start()
    sends.append(fin_x)
    fin_x.wait_recv()
    sums = [jnp.where(tp == 0, left, right), fxr[...]]
    sums = [jnp.where(tp == 0, sums[0], sums[1]), jnp.where(tp == 0, sums[1], sums[0])]
    for m in last:
        for r in range(2):
            i = m[0]
            along(m, fs.at[i, r], fr.at[r, i], fs_s.at[2 * i + r], fr_r.at[r * msgs_n + i], r).wait_recv()
            sums[r] = sums[r] + fr[r, i].astype(F32)
    flat = jnp.concatenate(sums, axis=0).T
    out[...] = jnp.concatenate(
        [flat[h : h + half_ch, r : r + quarter] for r in (0, quarter) for h in (0, half_ch)], axis=1
    ).astype(BF16)
    for c in sends:
        c.wait_send()


def hand_over(*refs):
    count = (len(refs) - 1) // 2
    sems = refs[-1]
    copies = [pltpu.make_async_copy(refs[i], refs[count + i], sems.at[i]) for i in range(count)]
    for c in copies:
        c.start()
    for c in copies:
        c.wait()


def shards(n, *args):
    (tok, ngain, wq, wk, wv, wg, wi, wf, ib, fb, mem, nrm, stab, wo, mgain, wup, wdn) = args
    rows, half_ch = tok.shape
    chans = ngain.shape[0]
    seqs, heads, qk, vd = mem.shape
    hw, vw = heads * qk, heads * vd
    proj = 2 * hw + 2 * vw
    wide = proj + 128
    width = mgain.shape[0]
    hid = wup.shape[1]
    msgs = n - 1
    any_space = pl.BlockSpec(memory_space=pl.ANY)
    vmem = pl.BlockSpec(memory_space=pltpu.VMEM)
    dma = pltpu.SemaphoreType.DMA
    out = pl.pallas_call(
        functools.partial(kernel, n),
        out_shape=(
            pltpu.VMEM((half_ch, rows), BF16),
            pltpu.VMEM(mem.shape, F32),
            pltpu.VMEM(nrm.shape, F32),
            pltpu.VMEM((heads, seqs), F32),
        ),
        in_specs=[any_space] * 17,
        out_specs=(vmem,) * 4,
        scratch_shapes=[
            pltpu.VMEM((2, half_ch, rows), BF16),
            pltpu.VMEM((1, chans), F32),
            pltpu.VMEM((chans, proj), BF16),
            pltpu.VMEM((2, wi.shape[1], chans), BF16),
            pltpu.VMEM((1, ib.shape[0]), F32),
            pltpu.VMEM((1, fb.shape[0]), F32),
            pltpu.VMEM(mem.shape, F32),
            pltpu.VMEM(nrm.shape, F32),
            pltpu.VMEM((heads, seqs), F32),
            pltpu.VMEM(wo.shape, BF16),
            pltpu.VMEM((width // 128, 128), F32),
            pltpu.VMEM((2, *wup.shape), BF16),
            pltpu.VMEM((2, *wdn.shape), BF16),
            pltpu.VMEM((n, seqs, wide), F32),
            pltpu.VMEM((msgs, seqs, wide), BF16),
            pltpu.VMEM((msgs, seqs, wide), BF16),
            pltpu.VMEM((seqs, proj), F32),
            pltpu.VMEM((seqs, vw), F32),
            pltpu.VMEM((rows, 128), F32),
            pltpu.VMEM((n, seqs, vw), BF16),
            pltpu.VMEM((rows, 128), F32),
            pltpu.VMEM((rows // 2, 128), F32),
            pltpu.VMEM((rows // 2, 128), F32),
            pltpu.VMEM((n, rows // 2, 128), BF16),
            pltpu.VMEM((msgs, rows // 2, 128), BF16),
            pltpu.VMEM((msgs, rows // 2, 128), BF16),
            pltpu.VMEM((msgs, 2, rows // 4, 128), BF16),
            pltpu.VMEM((2, msgs, rows // 4, 128), BF16),
            pltpu.VMEM((rows // 4, 128), F32),
            pltpu.VMEM((rows // 4, 128), F32),
            dma((20,)),
            dma((5,)),
            dma((5,)),
            dma((msgs,)),
            dma((msgs,)),
            dma((msgs,)),
            dma((msgs,)),
            dma((msgs,)),
            dma((msgs,)),
            dma((msgs,)),
            dma((msgs,)),
            dma((2 * msgs,)),
            dma((2 * msgs,)),
            pltpu.SemaphoreType.REGULAR((2,)),
        ],
        compiler_params=pltpu.CompilerParams(collective_id=0, has_side_effects=True, vmem_limit_bytes=40 * 2**20),
        name="cell_step",
    )(*[pltpu.with_memory_space_constraint(x, pltpu.HBM) for x in (
        tok.T,
        ngain.reshape(1, -1),
        wq,
        wk,
        wv,
        wg,
        wi.T,
        wf.T,
        ib.reshape(1, -1),
        fb.reshape(1, -1),
        mem,
        nrm,
        stab.T,
        wo,
        mgain.reshape(-1, 128),
        wup,
        wdn,
    )])
    out = pl.pallas_call(
        hand_over,
        out_shape=tuple(jax.ShapeDtypeStruct(o.shape, o.dtype) for o in out),
        in_specs=[vmem] * 4,
        out_specs=(any_space,) * 4,
        scratch_shapes=[dma((4,))],
        name="hand_over",
    )(*[pltpu.with_memory_space_constraint(o, pltpu.VMEM) for o in out])
    return out[0].T, out[1], out[2], out[3].T


def solution(mesh):
    placed = (
        P(("grp", "dp"), ("kv", "tp")),
        P("kv"),
        P("kv", "tp"),
        P("kv", "tp"),
        P("kv", "tp"),
        P("kv", "tp"),
        P("kv", None),
        P("kv", None),
        P(),
        P(),
        P(("grp", "dp", "kv"), "tp", None, None),
        P(("grp", "dp", "kv"), "tp"),
        P(("grp", "dp", "kv"), "tp"),
        P("tp", "kv"),
        P(),
        P(None, ("kv", "tp")),
        P(("kv", "tp"), None),
    )
    return jax.shard_map(
        functools.partial(shards, mesh.shape["kv"]),
        mesh=mesh,
        in_specs=placed,
        out_specs=(
            P(("grp", "dp"), ("kv", "tp")),
            P(("grp", "dp", "kv"), "tp", None, None),
            P(("grp", "dp", "kv"), "tp"),
            P(("grp", "dp", "kv"), "tp"),
        ),
        check_vma=False,
    )
```

```python
import functools

import jax
import jax.numpy as jnp
from jax import lax
from jax.experimental import pallas as pl
from jax.experimental.pallas import tpu as pltpu
from jax.sharding import PartitionSpec as P

EPSILON = 1e-06
MESH = pl.DeviceIdType.MESH
F32 = jnp.float32
BF16 = jnp.bfloat16

TWO_LEVEL = {1: 0, 2: 0, 3: 0, 4: 0, 5: 4, 6: 4, 7: 4, 8: 4}
PROJ_TREE = TWO_LEVEL
REACH = 4
MID_TREE = TWO_LEVEL
DOWN_TREE = TWO_LEVEL


def messages(tree, n):
    half = n // 2
    out = []
    for side, last in ((1, half), (-1, n - 1 - half)):
        for k in range(1, last + 1):
            out.append((len(out), side, k, tree[k]))
    return out


def children_of(msgs, side, k):
    return [m for m in msgs if m[1] == side and m[3] == k]


def depth_below(msgs, m):
    below = children_of(msgs, m[1], m[2])
    return 1 + max(depth_below(msgs, c) for c in below) if below else 0


def level_of(tree, k):
    return 0 if k == 0 else 1 + level_of(tree, tree[k])


def kernel(
    n,
    columns,
    tok,
    ngain,
    wq,
    wk,
    wv,
    wg,
    wi,
    wf,
    ib,
    fb,
    mem,
    nrm,
    stab,
    wo,
    mgain,
    wup,
    wdn,
    out,
    mem_new,
    nrm_new,
    stab_new,
    tokb,
    ngv,
    wp,
    wib,
    ibb,
    fbb,
    memb,
    nrmb,
    stabb,
    wob,
    mgb,
    wupb,
    wdnb,
    pf,
    ps,
    pr,
    sf,
    ro,
    tokrow,
    tst,
    tokx,
    tfwd,
    hid_own,
    hidg,
    midg,
    ds,
    dr,
    fs,
    fr,
    fxs,
    fxr,
    lsem,
    xs,
    xr,
    ps_s,
    ps_r,
    hid_s,
    hid_r,
    mid_s,
    mid_r,
    dn_s,
    dn_r,
    fs_s,
    fr_r,
    pre_s,
    pre_r,
):
    me = lax.axis_index("kv")
    tp = lax.axis_index("tp")
    column = lax.axis_index("dp")
    other = 1 - tp
    half_ch, rows = tokb.shape[1:]
    seqs, heads, qk, vd = memb.shape
    hw = heads * qk
    vw = heads * vd
    proj = wp.shape[1]
    width = mgb.shape[0] * mgb.shape[1]
    half_rows = rows // 2
    wo_rows = wob.shape[1]

    def at(z):
        return lax.rem(z + 2 * n, n)

    barrier = pltpu.get_barrier_semaphore()
    for step in range(1, REACH + 1):
        for side in (1, -1):
            pl.semaphore_signal(barrier, inc=1, device_id={"kv": at(me + side * step)}, device_id_type=MESH)
    pl.semaphore_signal(barrier, inc=1, device_id={"tp": other}, device_id_type=MESH)
    for step in range(1, columns):
        pl.semaphore_signal(barrier, inc=1, device_id={"dp": lax.rem(column + step, columns)}, device_id_type=MESH)

    loads = {}

    def load(name, src, dst):
        c = pltpu.make_async_copy(src, dst, lsem.at[len(loads)])
        c.start()
        loads[name] = c

    load("tok", tok, tokb.at[tp])
    load("ngain", ngain, ngv)
    load("wq", wq, wp.at[:, 0:hw])
    load("wk", wk, wp.at[:, hw : 2 * hw])
    load("wv", wv, wp.at[:, 2 * hw : 2 * hw + vw])
    load("wg", wg, wp.at[:, 2 * hw + vw : proj])
    load("wi", wi, wib.at[0])
    load("wf", wf, wib.at[1])
    load("ib", ib, ibb)
    load("fb", fb, fbb)
    load("stab", stab, stabb)
    load("nrm", nrm, nrmb)
    load("mem", mem, memb)
    load("wo", wo, wob.at[tp, :, 0:128])
    load("mgain", mgain, mgb)
    load("wup", wup, wupb.at[tp])
    load("wdn", wdn, wdnb.at[tp])

    pl.semaphore_wait(barrier, 2 * REACH + columns)

    def to_partner(src, dst, i):
        return pltpu.make_async_remote_copy(
            src_ref=src, dst_ref=dst, send_sem=xs.at[i], recv_sem=xr.at[i], device_id={"tp": other}, device_id_type=MESH
        )

    loads["tok"].wait()
    tok_x = to_partner(tokb.at[tp], tokb.at[tp], 0)
    tok_x.start()
    sends = [tok_x]

    for name in ("ngain", "wq", "wk", "wv", "wg", "wi", "wf"):
        loads[name].wait()

    gate_lanes = 2 * wib.shape[1]
    lane128 = lax.broadcasted_iota(jnp.int32, (rows, 128), 1)
    gw = jnp.concatenate(
        [wib[0].astype(F32), wib[1].astype(F32), jnp.zeros((128 - gate_lanes, 2 * half_ch), F32)], axis=0
    ).astype(BF16)
    tok_x.wait_recv()
    t = jnp.concatenate([tokb[0], tokb[1]], axis=0).astype(F32).T
    scaled = (t * ngv[...]).astype(BF16)
    main = jnp.dot(scaled, wp[...], preferred_element_type=F32)
    gates = lax.dot_general(scaled, gw, (((1,), (1,)), ((), ())), preferred_element_type=F32)
    pf[:, :, 0:proj] = main.reshape(n, seqs, proj)
    pf[:, :, proj:] = jnp.where(lane128 == gate_lanes, jnp.sum(t * t, axis=1, keepdims=True), gates).reshape(n, seqs, 128)
    tokrow[...] = t.reshape(n, seqs, 2 * half_ch)

    lane8 = lax.broadcasted_iota(jnp.int32, (seqs, 128), 1)

    def pack_gates(g):
        total = g[:, gate_lanes : gate_lanes + 1] + g[:, gate_lanes + 1 : gate_lanes + 2]
        upper = total.astype(BF16).astype(F32)
        return jnp.where(lane8 == gate_lanes, upper, jnp.where(lane8 == gate_lanes + 1, total - upper, g))

    def reduce_scatter(tree, own, emit, copies_of, before_relays=None):
        msgs = messages(tree, n)
        order = sorted(msgs, key=lambda m: (depth_below(msgs, m), -level_of(tree, m[2]), -m[2]))
        for m in order:
            slot, side, k, parent = m
            mine = own(at(me - side * k))
            kids = children_of(msgs, side, k)
            if kids and before_relays is not None:
                before_relays()
                before_relays = None
            for c in kids:
                copies_of(c)[0].wait_recv()
            emit(m, mine, [c[0] for c in kids])
            for c in copies_of(m):
                c.start()
                sends.append(c)
        return [m for m in msgs if m[3] == 0]

    def along(m, src, dst, send_sem, recv_sem, core=None):
        slot, side, k, parent = m
        where = {"kv": at(me - side * (k - parent))}
        if core is not None:
            where["tp"] = core
        return pltpu.make_async_remote_copy(
            src_ref=src, dst_ref=dst, send_sem=send_sem, recv_sem=recv_sem, device_id=where, device_id_type=MESH
        )

    def all_gather(tree, buf, send_sem, recv_sem):
        msgs = messages(tree, n)

        def copy_of(m):
            slot, side, k, parent = m
            origin = at(me - side * parent)
            return pltpu.make_async_remote_copy(
                src_ref=buf.at[origin],
                dst_ref=buf.at[origin],
                send_sem=send_sem.at[slot],
                recv_sem=recv_sem.at[slot],
                device_id={"kv": at(me + side * (k - parent))},
                device_id_type=MESH,
            )

        def arrival(m):
            slot, side, k, parent = m
            origin = at(me - side * k)
            return pltpu.make_async_remote_copy(
                src_ref=buf.at[origin],
                dst_ref=buf.at[origin],
                send_sem=send_sem.at[slot],
                recv_sem=recv_sem.at[slot],
                device_id={"kv": at(me - side * k)},
                device_id_type=MESH,
            )

        def send(m):
            c = copy_of(m)
            c.start()
            sends.append(c)

        waited = set()
        firsts = [m for m in msgs if m[3] == 0]
        for m in sorted(firsts, key=lambda m: (-depth_below(msgs, m), -m[2])):
            send(m)

        def finish():
            todo = sorted([m for m in msgs if children_of(msgs, m[1], m[2])], key=lambda m: (level_of(tree, m[2]), m[2]))
            for m in todo:
                arrival(m).wait_recv()
                waited.add(m[0])
                for c in sorted(children_of(msgs, m[1], m[2]), key=lambda c: (-depth_below(msgs, c), -c[2])):
                    send(c)
            for m in msgs:
                if m[0] not in waited:
                    arrival(m).wait_recv()

        return finish

    stride = n // 4
    piece = pl.ds(pl.multiple_of(column * (wo_rows // columns), wo_rows // columns), wo_rows // columns)
    parity = lax.rem(me, 2)
    mine_offset = jnp.where(tp == parity, 0, -1)

    def lanes(slot):
        return pl.ds(slot * 128, 128)

    def hop(src, dst, i, step, side="kv"):
        where = at(me + step) if side == "kv" else lax.rem(column + step, columns)
        return pltpu.make_async_remote_copy(
            src_ref=src, dst_ref=dst, send_sem=pre_s.at[i], recv_sem=pre_r.at[i], device_id={side: where}, device_id_type=MESH
        )

    def piece_hop(source, slot, i, step):
        return hop(wob.at[tp, piece, lanes(source)], wob.at[tp, piece, lanes(slot)], i, step)

    for i, step in enumerate((stride, -stride, 2 * stride)):
        for b in range(2):
            tst[i, b] = tokrow[at(me + step + mine_offset + 2 * b)]
    loads["wo"].wait()
    pre = {
        "w_up": piece_hop(0, 3, 0, stride),
        "w_dn": piece_hop(0, 1, 1, -stride),
        "t_up": hop(tst.at[0], tokx.at[3], 2, stride),
        "t_dn": hop(tst.at[1], tokx.at[1], 3, -stride),
        "t_on": hop(tst.at[2], tfwd, 4, stride),
        "w_fw": piece_hop(3, 2, 5, stride),
        "t_fw": hop(tfwd, tokx.at[2], 6, stride),
    }

    def begin(c):
        c.start()
        sends.append(c)

    for name in ("w_up", "w_dn", "t_up", "t_dn", "t_on"):
        begin(pre[name])
    wo_x = to_partner(wob.at[tp, :, lanes(0)], wob.at[tp, :, lanes(0)], 3)
    begin(wo_x)

    def forward_on():
        pre["w_up"].wait_recv()
        pre["t_on"].wait_recv()
        begin(pre["w_fw"])
        begin(pre["t_fw"])

    def to_columns():
        pre["w_dn"].wait_recv()
        pre["w_fw"].wait_recv()
        for step in range(1, columns):
            begin(column_copy(step))

    def column_copy(step):
        part = wob.at[tp, piece, 128:512]
        return hop(part, part, 7 + step, step, "dp")

    def column_arrival(step):
        rows_there = wo_rows // columns
        theirs = pl.ds(pl.multiple_of(lax.rem(column - step + columns, columns) * rows_there, rows_there), rows_there)
        part = wob.at[tp, theirs, 128:512]
        return hop(part, part, 7 + step, step, "dp")

    def own_proj(d):
        return pf[d, :, 0:proj], pf[d, :, proj:]

    def sum_proj(mine, slots):
        a, g = mine
        for s in slots:
            a = a + pr[s, :, 0:proj].astype(F32)
            g = g + pr[s, :, proj:].astype(F32)
        return a, g

    def emit_proj(m, mine, slots):
        slot = m[0]
        a, g = sum_proj(mine, slots)
        ps[slot, :, 0:proj] = a.astype(BF16)
        ps[slot, :, proj:] = pack_gates(g).astype(BF16)

    def proj_copies(m):
        i = m[0]
        return [along(m, ps.at[i], pr.at[i], ps_s.at[i], ps_r.at[i])]

    last = reduce_scatter(PROJ_TREE, own_proj, emit_proj, proj_copies, forward_on)
    to_columns()

    loads["wup"].wait()
    loads["wdn"].wait()
    up_x = to_partner(wupb.at[tp], wupb.at[tp], 1)
    up_x.start()
    dn_x = to_partner(wdnb.at[tp], wdnb.at[tp], 2)
    dn_x.start()
    sends += [up_x, dn_x]
    for name in ("ib", "fb", "stab", "nrm", "mem", "mgain"):
        loads[name].wait()

    for m in last:
        proj_copies(m)[0].wait_recv()
    slots = [m[0] for m in last]
    total, gate = sum_proj(own_proj(me), slots)
    sf[:, 0:proj] = total
    squares = gate[:, gate_lanes : gate_lanes + 1] + gate[:, gate_lanes + 1 : gate_lanes + 2]
    rscale = lax.rsqrt(squares / width + EPSILON)
    q = sf[:, 0:hw] * rscale
    k = sf[:, hw : 2 * hw] * rscale * qk ** (-0.5)
    v = sf[:, 2 * hw : 2 * hw + vw] * rscale
    all_heads = wib.shape[1]

    def mine_of(x, first):
        return jnp.where(tp == 0, x[:, first : first + heads], x[:, first + heads : first + 2 * heads])

    log_in = mine_of(gate, 0) * rscale + mine_of(ibb[...], 0)
    fpre = mine_of(gate, all_heads) * rscale + mine_of(fbb[...], 0)
    log_forget = jnp.minimum(fpre, 0.0) - jnp.log(1.0 + jnp.exp(-jnp.abs(fpre)))
    carried = log_forget + stabb[...].T
    snew = jnp.maximum(carried, log_in)
    take = jnp.exp(log_in - snew)
    keep = jnp.exp(carried - snew)
    stab_new[...] = snew.T

    hlane = lax.broadcasted_iota(jnp.int32, (seqs, hw), 1) // qk

    def spread(x):
        r = jnp.broadcast_to(x[:, 0:1], (seqs, hw))
        for h in range(1, heads):
            r = jnp.where(hlane == h, x[:, h : h + 1], r)
        return r

    def per_head(x):
        return [jnp.sum(jnp.where(hlane == h, x, 0.0), axis=1, keepdims=True) for h in range(heads)]

    tk = spread(take) * k
    nrm_new[...] = spread(keep) * nrmb[...] + tk
    scores = per_head(q * k)
    nqs = per_head(nrmb[...] * q)
    qt = q.T
    for s in range(seqs):
        for h in range(heads):
            col = qt[h * qk : (h + 1) * qk, s : s + 1]
            ro[s : s + 1, h * vd : (h + 1) * vd] = jnp.sum(memb[s, h] * col, axis=0, keepdims=True)
    hidden = []
    for h in range(heads):
        ts = take[:, h : h + 1] * scores[h]
        kp = keep[:, h : h + 1]
        numer = ts * v[:, h * vd : (h + 1) * vd] + kp * ro[:, h * vd : (h + 1) * vd]
        denom = ts + kp * nqs[h]
        cell = numer / jnp.maximum(jnp.abs(denom), 1.0)
        og = sf[:, 2 * hw + vw + h * vd : 2 * hw + vw + (h + 1) * vd] * rscale
        hid_own[:, h * vd : (h + 1) * vd] = ((1.0 / (1.0 + jnp.exp(-og))) * cell).astype(BF16)

    def hid_hop(i, slot, step):
        return pltpu.make_async_remote_copy(
            src_ref=hid_own,
            dst_ref=hidg.at[slot, tp],
            send_sem=hid_s.at[i],
            recv_sem=hid_r.at[2 * slot + tp],
            device_id={"kv": at(me + step), "tp": parity},
            device_id_type=MESH,
        )

    for i, (slot, step) in enumerate(((1, -2), (0, 1), (1, -1))):
        begin(hid_hop(i, slot, step))
    own_hid = pltpu.make_async_remote_copy(
        src_ref=hid_own,
        dst_ref=hidg.at[0, tp],
        send_sem=hid_s.at[3],
        recv_sem=hid_r.at[tp],
        device_id={"tp": other},
        device_id_type=MESH,
    )

    @pl.when(tp != parity)
    def _():
        own_hid.start()

    @pl.when(tp == parity)
    def _():
        hidg[0, tp] = hid_own[...]

    kt = tk.T
    for s in range(seqs):
        for h in range(heads):
            col = kt[h * qk : (h + 1) * qk, s : s + 1]
            mem_new[s, h] = keep[s : s + 1, h : h + 1] * memb[s, h] + col * v[s : s + 1, h * vd : (h + 1) * vd]

    for step in range(1, columns):
        column_arrival(step).wait_recv()
    far = wob.at[tp, :, 128:512]
    far_x = to_partner(far, far, 4)
    begin(far_x)
    wo_x.wait_recv()
    for name in ("t_up", "t_dn", "t_fw"):
        pre[name].wait_recv()

    def hid_arrival(slot, core):
        pltpu.make_async_remote_copy(
            src_ref=hid_own,
            dst_ref=hidg.at[slot, core],
            send_sem=hid_s.at[0],
            recv_sem=hid_r.at[2 * slot + core],
            device_id={"tp": other},
            device_id_type=MESH,
        ).wait_recv()

    for i in range(2):
        tokx[0, i] = tokrow[at(me + mine_offset + 2 * i)]
    far_x.wait_recv()

    @pl.when(tp != parity)
    def _():
        own_hid.wait_send()
        hid_arrival(0, tp)

    hid_arrival(0, other)
    for core in range(2):
        hid_arrival(1, core)
    left_rows = jnp.concatenate(
        [jnp.concatenate([hidg[i, h].astype(F32) for h in range(2)], axis=1) for i in range(2)], axis=0
    ).astype(BF16)
    added = jnp.dot(left_rows[:, 0:vw], wob[0], preferred_element_type=F32) + jnp.dot(
        left_rows[:, vw : 2 * vw], wob[1], preferred_element_type=F32
    )
    for slot in range(4):
        cols = lax.rem(me // 4 + slot, 4)
        block = added[:, slot * 128 : (slot + 1) * 128].reshape(2, seqs, 128) + tokx[slot]
        midg[me, :, :, pl.ds(pl.multiple_of(cols * 128, 128), 128)] = block.astype(BF16)
    all_gather(MID_TREE, midg, mid_s, mid_r)()

    up_x.wait_recv()
    dn_x.wait_recv()
    blocks = half_rows // seqs

    def place(group, m):
        z = tp + 2 * m
        offset = lax.rem(z - group + 1 + n, 4) - 1
        return at(z - offset), lax.div(offset + 1, 2)

    sq_sum = jnp.zeros((half_rows, 512), F32)
    acc = [None, None]
    for group in range(4):
        parts = []
        for m in range(blocks):
            z, half = place(group, m)
            parts.append(midg[z, half].astype(F32))
        x = jnp.concatenate(parts, axis=0)
        sq_sum = sq_sum + x * x
        for j in range(0, 4, 2):
            chans = [group + 4 * (j + i) for i in range(2)]
            xs_in = jnp.concatenate(
                [x[:, (j + i) * 128 : (j + i + 1) * 128] * mgb[c : c + 1, :] for i, c in enumerate(chans)], axis=1
            ).astype(BF16)
            for u in range(2):
                w = jnp.concatenate([wupb[u, c * 128 : (c + 1) * 128, :] for c in chans], axis=0)
                d = jnp.dot(xs_in, w, preferred_element_type=F32)
                acc[u] = d if acc[u] is None else acc[u] + d
    rmid = lax.rsqrt(jnp.sum(sq_sum, axis=1, keepdims=True) / width + EPSILON)
    sqd = [jnp.square(jnp.maximum(a * rmid, 0.0)).astype(BF16) for a in acc]

    def own_down(d):
        cols = pl.ds(pl.multiple_of(d * 128, 128), 128)
        return jnp.dot(sqd[0], wdnb[0, :, cols], preferred_element_type=F32) + jnp.dot(
            sqd[1], wdnb[1, :, cols], preferred_element_type=F32
        )

    def sum_down(a, slots):
        for s in slots:
            a = a + dr[s].astype(F32)
        return a

    def halves(a):
        return [
            jnp.concatenate([a[0:quarter, h : h + half_ch], a[quarter : 2 * quarter, h : h + half_ch]], axis=1)
            for h in (0, half_ch)
        ]

    quarter = half_rows // 2
    msgs_n = n - 1

    def emit_down(m, mine, slots):
        a = sum_down(mine, slots)
        if m[3] == 0:
            fs[m[0], 0], fs[m[0], 1] = [x.astype(BF16) for x in halves(a)]
        else:
            ds[m[0]] = a.astype(BF16)

    def down_copies(m):
        i = m[0]
        if m[3] == 0:
            return [
                along(m, fs.at[i, c], fr.at[tp, i], fs_s.at[2 * i + c], fr_r.at[tp * msgs_n + i], c) for c in range(2)
            ]
        return [along(m, ds.at[i], dr.at[i], dn_s.at[i], dn_r.at[i])]

    last = reduce_scatter(DOWN_TREE, own_down, emit_down, down_copies)
    own_mid = []
    for m in range(blocks):
        z, half = place(lax.rem(me, 4), m)
        own_mid.append(midg[z, half, :, pl.ds(pl.multiple_of(me // 4 * 128, 128), 128)].astype(F32))
    left, right = halves(own_down(me) + jnp.concatenate(own_mid, axis=0))
    fxs[...] = jnp.where(tp == 0, right, left)
    fin_x = to_partner(fxs, fxr, 5)
    fin_x.start()
    sends.append(fin_x)
    fin_x.wait_recv()
    sums = [jnp.where(tp == 0, left, right), fxr[...]]
    sums = [jnp.where(tp == 0, sums[0], sums[1]), jnp.where(tp == 0, sums[1], sums[0])]
    for m in last:
        for r in range(2):
            i = m[0]
            along(m, fs.at[i, r], fr.at[r, i], fs_s.at[2 * i + r], fr_r.at[r * msgs_n + i], r).wait_recv()
            sums[r] = sums[r] + fr[r, i].astype(F32)
    flat = jnp.concatenate(
        [sums[r][m * seqs : (m + 1) * seqs] for m in range(blocks // 2) for r in range(2)], axis=0
    ).T
    out[...] = jnp.concatenate([flat[0:half_ch], flat[half_ch : 2 * half_ch]], axis=1).astype(BF16)
    for c in sends:
        c.wait_send()


def hand_over(*refs):
    count = (len(refs) - 1) // 2
    sems = refs[-1]
    copies = [pltpu.make_async_copy(refs[i], refs[count + i], sems.at[i]) for i in range(count)]
    for c in copies:
        c.start()
    for c in copies:
        c.wait()


def shards(n, columns, *args):
    (tok, ngain, wq, wk, wv, wg, wi, wf, ib, fb, mem, nrm, stab, wo, mgain, wup, wdn) = args
    rows, half_ch = tok.shape
    chans = ngain.shape[0]
    seqs, heads, qk, vd = mem.shape
    hw, vw = heads * qk, heads * vd
    proj = 2 * hw + 2 * vw
    wide = proj + 128
    width = mgain.shape[0]
    hid = wup.shape[1]
    msgs = n - 1
    any_space = pl.BlockSpec(memory_space=pl.ANY)
    vmem = pl.BlockSpec(memory_space=pltpu.VMEM)
    dma = pltpu.SemaphoreType.DMA
    out = pl.pallas_call(
        functools.partial(kernel, n, columns),
        out_shape=(
            pltpu.VMEM((half_ch, rows), BF16),
            pltpu.VMEM(mem.shape, F32),
            pltpu.VMEM(nrm.shape, F32),
            pltpu.VMEM((heads, seqs), F32),
        ),
        in_specs=[any_space] * 17,
        out_specs=(vmem,) * 4,
        scratch_shapes=[
            pltpu.VMEM((2, half_ch, rows), BF16),
            pltpu.VMEM((1, chans), F32),
            pltpu.VMEM((chans, proj), BF16),
            pltpu.VMEM((2, wi.shape[1], chans), BF16),
            pltpu.VMEM((1, ib.shape[0]), F32),
            pltpu.VMEM((1, fb.shape[0]), F32),
            pltpu.VMEM(mem.shape, F32),
            pltpu.VMEM(nrm.shape, F32),
            pltpu.VMEM((heads, seqs), F32),
            pltpu.VMEM((2, wo.shape[0], 512), BF16),
            pltpu.VMEM((width // 128, 128), F32),
            pltpu.VMEM((2, *wup.shape), BF16),
            pltpu.VMEM((2, *wdn.shape), BF16),
            pltpu.VMEM((n, seqs, wide), F32),
            pltpu.VMEM((msgs, seqs, wide), BF16),
            pltpu.VMEM((msgs, seqs, wide), BF16),
            pltpu.VMEM((seqs, proj), F32),
            pltpu.VMEM((seqs, vw), F32),
            pltpu.VMEM((n, seqs, 128), F32),
            pltpu.VMEM((3, 2, seqs, 128), F32),
            pltpu.VMEM((4, 2, seqs, 128), F32),
            pltpu.VMEM((2, seqs, 128), F32),
            pltpu.VMEM((seqs, vw), BF16),
            pltpu.VMEM((2, 2, seqs, vw), BF16),
            pltpu.VMEM((n, 2, seqs, 512), BF16),
            pltpu.VMEM((msgs, rows // 2, 128), BF16),
            pltpu.VMEM((msgs, rows // 2, 128), BF16),
            pltpu.VMEM((msgs, 2, rows // 4, 128), BF16),
            pltpu.VMEM((2, msgs, rows // 4, 128), BF16),
            pltpu.VMEM((rows // 4, 128), F32),
            pltpu.VMEM((rows // 4, 128), F32),
            dma((20,)),
            dma((6,)),
            dma((6,)),
            dma((msgs,)),
            dma((msgs,)),
            dma((msgs,)),
            dma((msgs,)),
            dma((msgs,)),
            dma((msgs,)),
            dma((msgs,)),
            dma((msgs,)),
            dma((2 * msgs,)),
            dma((2 * msgs,)),
            dma((7 + columns,)),
            dma((7 + columns,)),
        ],
        compiler_params=pltpu.CompilerParams(collective_id=0, has_side_effects=True, vmem_limit_bytes=40 * 2**20),
        name="cell_step",
    )(*[pltpu.with_memory_space_constraint(x, pltpu.HBM) for x in (
        tok.T,
        ngain.reshape(1, -1),
        wq,
        wk,
        wv,
        wg,
        wi.T,
        wf.T,
        ib.reshape(1, -1),
        fb.reshape(1, -1),
        mem,
        nrm,
        stab.T,
        wo,
        mgain.reshape(-1, 128),
        wup,
        wdn,
    )])
    out = pl.pallas_call(
        hand_over,
        out_shape=tuple(jax.ShapeDtypeStruct(o.shape, o.dtype) for o in out),
        in_specs=[vmem] * 4,
        out_specs=(any_space,) * 4,
        scratch_shapes=[dma((4,))],
        name="hand_over",
    )(*[pltpu.with_memory_space_constraint(o, pltpu.VMEM) for o in out])
    return out[0].T, out[1], out[2], out[3].T


def solution(mesh):
    placed = (
        P(("grp", "dp"), ("kv", "tp")),
        P("kv"),
        P("kv", "tp"),
        P("kv", "tp"),
        P("kv", "tp"),
        P("kv", "tp"),
        P("kv", None),
        P("kv", None),
        P(),
        P(),
        P(("grp", "dp", "kv"), "tp", None, None),
        P(("grp", "dp", "kv"), "tp"),
        P(("grp", "dp", "kv"), "tp"),
        P("tp", "kv"),
        P(),
        P(None, ("kv", "tp")),
        P(("kv", "tp"), None),
    )
    return jax.shard_map(
        functools.partial(shards, mesh.shape["kv"], mesh.shape["dp"]),
        mesh=mesh,
        in_specs=placed,
        out_specs=(
            P(("grp", "dp"), ("kv", "tp")),
            P(("grp", "dp", "kv"), "tp", None, None),
            P(("grp", "dp", "kv"), "tp"),
            P(("grp", "dp", "kv"), "tp"),
        ),
        check_vma=False,
    )
```

```python
import functools

import jax
import jax.numpy as jnp
from jax import lax
from jax.experimental import pallas as pl
from jax.experimental.pallas import tpu as pltpu
from jax.sharding import PartitionSpec as P

EPSILON = 1e-06
MESH = pl.DeviceIdType.MESH
F32 = jnp.float32
BF16 = jnp.bfloat16

TWO_LEVEL = {1: 0, 2: 0, 3: 0, 4: 0, 5: 4, 6: 4, 7: 4, 8: 4}
PROJ_TREE = TWO_LEVEL
REACH = 4
MID_TREE = TWO_LEVEL
DOWN_TREE = TWO_LEVEL


def messages(tree, n):
    half = n // 2
    out = []
    for side, last in ((1, half), (-1, n - 1 - half)):
        for k in range(1, last + 1):
            out.append((len(out), side, k, tree[k]))
    return out


def children_of(msgs, side, k):
    return [m for m in msgs if m[1] == side and m[3] == k]


def depth_below(msgs, m):
    below = children_of(msgs, m[1], m[2])
    return 1 + max(depth_below(msgs, c) for c in below) if below else 0


def level_of(tree, k):
    return 0 if k == 0 else 1 + level_of(tree, tree[k])


def kernel(
    n,
    columns,
    tok,
    ngain,
    wq,
    wk,
    wv,
    wg,
    wi,
    wf,
    ib,
    fb,
    mem,
    nrm,
    stab,
    wo,
    mgain,
    wup,
    wdn,
    out,
    mem_new,
    nrm_new,
    stab_new,
    tokb,
    ngv,
    wp,
    wib,
    ibb,
    fbb,
    memb,
    nrmb,
    stabb,
    wob,
    mgb,
    wupb,
    wdnb,
    pf,
    ps,
    pr,
    sf,
    ro,
    tokrow,
    tst,
    tokx,
    tfwd,
    hid_own,
    hidg,
    midg,
    ds,
    dr,
    fs,
    fr,
    fxs,
    fxr,
    lsem,
    xs,
    xr,
    ps_s,
    ps_r,
    hid_s,
    hid_r,
    mid_s,
    mid_r,
    dn_s,
    dn_r,
    fs_s,
    fr_r,
    pre_s,
    pre_r,
):
    me = lax.axis_index("kv")
    tp = lax.axis_index("tp")
    column = lax.axis_index("dp")
    other = 1 - tp
    half_ch, rows = tokb.shape[1:]
    seqs, heads, qk, vd = memb.shape
    hw = heads * qk
    vw = heads * vd
    proj = wp.shape[1]
    width = mgb.shape[0] * mgb.shape[1]
    half_rows = rows // 2
    wo_rows = wob.shape[1]

    def at(z):
        return lax.rem(z + 2 * n, n)

    barrier = pltpu.get_barrier_semaphore()
    for step in range(1, REACH + 1):
        for side in (1, -1):
            pl.semaphore_signal(barrier, inc=1, device_id={"kv": at(me + side * step)}, device_id_type=MESH)
    pl.semaphore_signal(barrier, inc=1, device_id={"tp": other}, device_id_type=MESH)
    for step in range(1, columns):
        pl.semaphore_signal(barrier, inc=1, device_id={"dp": lax.rem(column + step, columns)}, device_id_type=MESH)

    loads = {}

    def load(name, src, dst):
        c = pltpu.make_async_copy(src, dst, lsem.at[len(loads)])
        c.start()
        loads[name] = c

    load("tok", tok, tokb.at[tp])
    load("wo", wo, wob.at[tp, :, 0:128])
    load("ngain", ngain, ngv)
    load("wq", wq, wp.at[:, 0:hw])
    load("wk", wk, wp.at[:, hw : 2 * hw])
    load("wv", wv, wp.at[:, 2 * hw : 2 * hw + vw])
    load("wg", wg, wp.at[:, 2 * hw + vw : proj])
    load("wi", wi, wib.at[0])
    load("wf", wf, wib.at[1])
    load("ib", ib, ibb)
    load("fb", fb, fbb)
    load("stab", stab, stabb)
    load("nrm", nrm, nrmb)
    load("mem", mem, memb)
    load("mgain", mgain, mgb)
    load("wup", wup, wupb.at[tp])
    load("wdn", wdn, wdnb.at[tp])

    pl.semaphore_wait(barrier, 2 * REACH + columns)

    def to_partner(src, dst, i):
        return pltpu.make_async_remote_copy(
            src_ref=src, dst_ref=dst, send_sem=xs.at[i], recv_sem=xr.at[i], device_id={"tp": other}, device_id_type=MESH
        )

    loads["tok"].wait()
    tok_x = to_partner(tokb.at[tp], tokb.at[tp], 0)
    tok_x.start()
    sends = [tok_x]

    stride = n // 4
    piece_rows = wo_rows // columns
    parity = lax.rem(me, 2)
    mine_offset = jnp.where(tp == parity, 0, -1)

    def piece(x):
        return pl.ds(pl.multiple_of(x * piece_rows, piece_rows), piece_rows)

    def lanes(slot):
        return pl.ds(slot * 128, 128)

    def hop(src, dst, i, step, side="kv"):
        where = at(me + step) if side == "kv" else lax.rem(column + step, columns)
        return pltpu.make_async_remote_copy(
            src_ref=src, dst_ref=dst, send_sem=pre_s.at[i], recv_sem=pre_r.at[i], device_id={side: where}, device_id_type=MESH
        )

    def piece_hop(source, slot, i, step):
        return hop(wob.at[tp, piece(column), lanes(source)], wob.at[tp, piece(column), lanes(slot)], i, step)

    pre = {
        "w_up": piece_hop(0, 3, 0, stride),
        "w_dn": piece_hop(0, 1, 1, -stride),
        "t_up": hop(tst.at[0], tokx.at[3], 2, stride),
        "t_dn": hop(tst.at[1], tokx.at[1], 3, -stride),
        "t_on": hop(tst.at[2], tfwd, 4, stride),
        "w_fw": piece_hop(3, 2, 5, stride),
        "t_fw": hop(tfwd, tokx.at[2], 6, stride),
    }

    def begin(c):
        c.start()
        sends.append(c)

    def column_copy(slot, step):
        part = wob.at[tp, piece(column), lanes(slot)]
        return hop(part, part, 7 + (slot - 1) * (columns - 1) + step - 1, step, "dp")

    def column_arrival(slot, step):
        part = wob.at[tp, piece(lax.rem(column - step + columns, columns)), lanes(slot)]
        return hop(part, part, 7 + (slot - 1) * (columns - 1) + step - 1, step, "dp")

    by_distance = sorted(range(1, columns), key=lambda step: -min(step, columns - step))

    def to_columns(slot):
        for step in by_distance:
            begin(column_copy(slot, step))

    def from_columns(slot):
        for step in range(1, columns):
            column_arrival(slot, step).wait_recv()

    def share_slot(slot):
        part = wob.at[tp, :, lanes(slot)]
        return to_partner(part, part, 6 + slot)

    def forward_on():
        pre["w_up"].wait_recv()
        begin(pre["w_fw"])
        to_columns(3)
        pre["t_on"].wait_recv()
        begin(pre["t_fw"])
        pre["w_dn"].wait_recv()
        to_columns(1)

    def complete_near():
        pre["w_fw"].wait_recv()
        to_columns(2)
        for slot in (3, 1):
            from_columns(slot)
            begin(share_slot(slot))

    loads["wo"].wait()
    begin(pre["w_up"])
    begin(pre["w_dn"])
    begin(share_slot(0))

    for name in ("ngain", "wq", "wk", "wv", "wg", "wi", "wf"):
        loads[name].wait()

    gate_lanes = 2 * wib.shape[1]
    lane128 = lax.broadcasted_iota(jnp.int32, (rows, 128), 1)
    gw = jnp.concatenate(
        [wib[0].astype(F32), wib[1].astype(F32), jnp.zeros((128 - gate_lanes, 2 * half_ch), F32)], axis=0
    ).astype(BF16)
    tok_x.wait_recv()
    t = jnp.concatenate([tokb[0], tokb[1]], axis=0).astype(F32).T
    scaled = (t * ngv[...]).astype(BF16)
    main = jnp.dot(scaled, wp[...], preferred_element_type=F32)
    gates = lax.dot_general(scaled, gw, (((1,), (1,)), ((), ())), preferred_element_type=F32)
    pf[:, :, 0:proj] = main.reshape(n, seqs, proj)
    pf[:, :, proj:] = jnp.where(lane128 == gate_lanes, jnp.sum(t * t, axis=1, keepdims=True), gates).reshape(n, seqs, 128)
    tokrow[...] = t.reshape(n, seqs, 2 * half_ch)

    lane8 = lax.broadcasted_iota(jnp.int32, (seqs, 128), 1)

    def pack_gates(g):
        total = g[:, gate_lanes : gate_lanes + 1] + g[:, gate_lanes + 1 : gate_lanes + 2]
        upper = total.astype(BF16).astype(F32)
        return jnp.where(lane8 == gate_lanes, upper, jnp.where(lane8 == gate_lanes + 1, total - upper, g))

    def reduce_scatter(tree, own, emit, copies_of, before_relays=None):
        msgs = messages(tree, n)
        order = sorted(msgs, key=lambda m: (depth_below(msgs, m), -level_of(tree, m[2]), -m[2]))
        for m in order:
            slot, side, k, parent = m
            mine = own(at(me - side * k))
            kids = children_of(msgs, side, k)
            if kids and before_relays is not None:
                before_relays()
                before_relays = None
            for c in kids:
                copies_of(c)[0].wait_recv()
            emit(m, mine, [c[0] for c in kids])
            for c in copies_of(m):
                c.start()
                sends.append(c)
        return [m for m in msgs if m[3] == 0]

    def along(m, src, dst, send_sem, recv_sem, core=None):
        slot, side, k, parent = m
        where = {"kv": at(me - side * (k - parent))}
        if core is not None:
            where["tp"] = core
        return pltpu.make_async_remote_copy(
            src_ref=src, dst_ref=dst, send_sem=send_sem, recv_sem=recv_sem, device_id=where, device_id_type=MESH
        )

    def all_gather(tree, buf, send_sem, recv_sem):
        msgs = messages(tree, n)

        def copy_of(m):
            slot, side, k, parent = m
            origin = at(me - side * parent)
            return pltpu.make_async_remote_copy(
                src_ref=buf.at[origin],
                dst_ref=buf.at[origin],
                send_sem=send_sem.at[slot],
                recv_sem=recv_sem.at[slot],
                device_id={"kv": at(me + side * (k - parent))},
                device_id_type=MESH,
            )

        def arrival(m):
            slot, side, k, parent = m
            origin = at(me - side * k)
            return pltpu.make_async_remote_copy(
                src_ref=buf.at[origin],
                dst_ref=buf.at[origin],
                send_sem=send_sem.at[slot],
                recv_sem=recv_sem.at[slot],
                device_id={"kv": at(me - side * k)},
                device_id_type=MESH,
            )

        def send(m):
            c = copy_of(m)
            c.start()
            sends.append(c)

        waited = set()
        firsts = [m for m in msgs if m[3] == 0]
        for m in sorted(firsts, key=lambda m: (-depth_below(msgs, m), -m[2])):
            send(m)

        def finish():
            todo = sorted([m for m in msgs if children_of(msgs, m[1], m[2])], key=lambda m: (level_of(tree, m[2]), m[2]))
            for m in todo:
                arrival(m).wait_recv()
                waited.add(m[0])
                for c in sorted(children_of(msgs, m[1], m[2]), key=lambda c: (-depth_below(msgs, c), -c[2])):
                    send(c)
            for m in msgs:
                if m[0] not in waited:
                    arrival(m).wait_recv()

        return finish

    for i, step in enumerate((stride, -stride, 2 * stride)):
        for b in range(2):
            tst[i, b] = tokrow[at(me + step + mine_offset + 2 * b)].astype(BF16)

    def own_proj(d):
        return pf[d, :, 0:proj], pf[d, :, proj:]

    def sum_proj(mine, slots):
        a, g = mine
        for s in slots:
            a = a + pr[s, :, 0:proj].astype(F32)
            g = g + pr[s, :, proj:].astype(F32)
        return a, g

    def emit_proj(m, mine, slots):
        slot = m[0]
        a, g = sum_proj(mine, slots)
        ps[slot, :, 0:proj] = a.astype(BF16)
        ps[slot, :, proj:] = pack_gates(g).astype(BF16)

    def proj_copies(m):
        i = m[0]
        return [along(m, ps.at[i], pr.at[i], ps_s.at[i], ps_r.at[i])]

    for name in ("t_on", "t_up", "t_dn"):
        begin(pre[name])
    last = reduce_scatter(PROJ_TREE, own_proj, emit_proj, proj_copies, forward_on)
    complete_near()

    loads["wup"].wait()
    loads["wdn"].wait()
    up_x = to_partner(wupb.at[tp], wupb.at[tp], 1)
    up_x.start()
    dn_x = to_partner(wdnb.at[tp], wdnb.at[tp], 2)
    dn_x.start()
    sends += [up_x, dn_x]
    for name in ("ib", "fb", "stab", "nrm", "mem", "mgain"):
        loads[name].wait()

    for m in last:
        proj_copies(m)[0].wait_recv()
    slots = [m[0] for m in last]
    total, gate = sum_proj(own_proj(me), slots)
    sf[:, 0:proj] = total
    squares = gate[:, gate_lanes : gate_lanes + 1] + gate[:, gate_lanes + 1 : gate_lanes + 2]
    rscale = lax.rsqrt(squares / width + EPSILON)
    q = sf[:, 0:hw] * rscale
    k = sf[:, hw : 2 * hw] * rscale * qk ** (-0.5)
    v = sf[:, 2 * hw : 2 * hw + vw] * rscale
    all_heads = wib.shape[1]

    def mine_of(x, first):
        return jnp.where(tp == 0, x[:, first : first + heads], x[:, first + heads : first + 2 * heads])

    log_in = mine_of(gate, 0) * rscale + mine_of(ibb[...], 0)
    fpre = mine_of(gate, all_heads) * rscale + mine_of(fbb[...], 0)
    log_forget = jnp.minimum(fpre, 0.0) - jnp.log(1.0 + jnp.exp(-jnp.abs(fpre)))
    carried = log_forget + stabb[...].T
    snew = jnp.maximum(carried, log_in)
    take = jnp.exp(log_in - snew)
    keep = jnp.exp(carried - snew)
    stab_new[...] = snew.T

    hlane = lax.broadcasted_iota(jnp.int32, (seqs, hw), 1) // qk

    def spread(x):
        r = jnp.broadcast_to(x[:, 0:1], (seqs, hw))
        for h in range(1, heads):
            r = jnp.where(hlane == h, x[:, h : h + 1], r)
        return r

    def per_head(x):
        return [jnp.sum(jnp.where(hlane == h, x, 0.0), axis=1, keepdims=True) for h in range(heads)]

    tk = spread(take) * k
    nrm_new[...] = spread(keep) * nrmb[...] + tk
    scores = per_head(q * k)
    nqs = per_head(nrmb[...] * q)
    qt = q.T
    for s in range(seqs):
        for h in range(heads):
            col = qt[h * qk : (h + 1) * qk, s : s + 1]
            ro[s : s + 1, h * vd : (h + 1) * vd] = jnp.sum(memb[s, h] * col, axis=0, keepdims=True)
    hidden = []
    for h in range(heads):
        ts = take[:, h : h + 1] * scores[h]
        kp = keep[:, h : h + 1]
        numer = ts * v[:, h * vd : (h + 1) * vd] + kp * ro[:, h * vd : (h + 1) * vd]
        denom = ts + kp * nqs[h]
        cell = numer / jnp.maximum(jnp.abs(denom), 1.0)
        og = sf[:, 2 * hw + vw + h * vd : 2 * hw + vw + (h + 1) * vd] * rscale
        hid_own[:, h * vd : (h + 1) * vd] = ((1.0 / (1.0 + jnp.exp(-og))) * cell).astype(BF16)

    def hid_hop(i, slot, step):
        return pltpu.make_async_remote_copy(
            src_ref=hid_own,
            dst_ref=hidg.at[slot, tp],
            send_sem=hid_s.at[i],
            recv_sem=hid_r.at[2 * slot + tp],
            device_id={"kv": at(me + step), "tp": parity},
            device_id_type=MESH,
        )

    for i, (slot, step) in enumerate(((1, -2), (0, 1), (1, -1))):
        begin(hid_hop(i, slot, step))
    own_hid = pltpu.make_async_remote_copy(
        src_ref=hid_own,
        dst_ref=hidg.at[0, tp],
        send_sem=hid_s.at[3],
        recv_sem=hid_r.at[tp],
        device_id={"tp": other},
        device_id_type=MESH,
    )

    @pl.when(tp != parity)
    def _():
        own_hid.start()

    @pl.when(tp == parity)
    def _():
        hidg[0, tp] = hid_own[...]

    kt = tk.T
    for s in range(seqs):
        for h in range(heads):
            col = kt[h * qk : (h + 1) * qk, s : s + 1]
            mem_new[s, h] = keep[s : s + 1, h : h + 1] * memb[s, h] + col * v[s : s + 1, h * vd : (h + 1) * vd]

    from_columns(2)
    begin(share_slot(2))
    for name in ("t_up", "t_dn", "t_fw"):
        pre[name].wait_recv()

    def hid_arrival(slot, core):
        pltpu.make_async_remote_copy(
            src_ref=hid_own,
            dst_ref=hidg.at[slot, core],
            send_sem=hid_s.at[0],
            recv_sem=hid_r.at[2 * slot + core],
            device_id={"tp": other},
            device_id_type=MESH,
        ).wait_recv()

    for i in range(2):
        tokx[0, i] = tokrow[at(me + mine_offset + 2 * i)].astype(BF16)

    @pl.when(tp != parity)
    def _():
        own_hid.wait_send()
        hid_arrival(0, tp)

    hid_arrival(0, other)
    for core in range(2):
        hid_arrival(1, core)
    for slot in range(4):
        share_slot(slot).wait_recv()
    left_rows = jnp.concatenate(
        [jnp.concatenate([hidg[i, h].astype(F32) for h in range(2)], axis=1) for i in range(2)], axis=0
    ).astype(BF16)
    added = jnp.dot(left_rows[:, 0:vw], wob[0], preferred_element_type=F32) + jnp.dot(
        left_rows[:, vw : 2 * vw], wob[1], preferred_element_type=F32
    )
    for slot in range(4):
        cols = lax.rem(me // 4 + slot, 4)
        block = added[:, slot * 128 : (slot + 1) * 128].reshape(2, seqs, 128) + tokx[slot].astype(F32)
        midg[me, :, :, pl.ds(pl.multiple_of(cols * 128, 128), 128)] = block.astype(BF16)
    all_gather(MID_TREE, midg, mid_s, mid_r)()

    up_x.wait_recv()
    dn_x.wait_recv()
    blocks = half_rows // seqs

    def place(group, m):
        z = tp + 2 * m
        offset = lax.rem(z - group + 1 + n, 4) - 1
        return at(z - offset), lax.div(offset + 1, 2)

    sq_sum = jnp.zeros((half_rows, 512), F32)
    acc = [None, None]
    for group in range(4):
        parts = []
        for m in range(blocks):
            z, half = place(group, m)
            parts.append(midg[z, half].astype(F32))
        x = jnp.concatenate(parts, axis=0)
        sq_sum = sq_sum + x * x
        for j in range(0, 4, 2):
            chans = [group + 4 * (j + i) for i in range(2)]
            xs_in = jnp.concatenate(
                [x[:, (j + i) * 128 : (j + i + 1) * 128] * mgb[c : c + 1, :] for i, c in enumerate(chans)], axis=1
            ).astype(BF16)
            for u in range(2):
                w = jnp.concatenate([wupb[u, c * 128 : (c + 1) * 128, :] for c in chans], axis=0)
                d = jnp.dot(xs_in, w, preferred_element_type=F32)
                acc[u] = d if acc[u] is None else acc[u] + d
    rmid = lax.rsqrt(jnp.sum(sq_sum, axis=1, keepdims=True) / width + EPSILON)
    sqd = [jnp.square(jnp.maximum(a * rmid, 0.0)).astype(BF16) for a in acc]

    def own_down(d):
        cols = pl.ds(pl.multiple_of(d * 128, 128), 128)
        return jnp.dot(sqd[0], wdnb[0, :, cols], preferred_element_type=F32) + jnp.dot(
            sqd[1], wdnb[1, :, cols], preferred_element_type=F32
        )

    def sum_down(a, slots):
        for s in slots:
            a = a + dr[s].astype(F32)
        return a

    def halves(a):
        return [
            jnp.concatenate([a[0:quarter, h : h + half_ch], a[quarter : 2 * quarter, h : h + half_ch]], axis=1)
            for h in (0, half_ch)
        ]

    quarter = half_rows // 2
    msgs_n = n - 1

    def emit_down(m, mine, slots):
        a = sum_down(mine, slots)
        if m[3] == 0:
            fs[m[0], 0], fs[m[0], 1] = [x.astype(BF16) for x in halves(a)]
        else:
            ds[m[0]] = a.astype(BF16)

    def down_copies(m):
        i = m[0]
        if m[3] == 0:
            return [
                along(m, fs.at[i, c], fr.at[tp, i], fs_s.at[2 * i + c], fr_r.at[tp * msgs_n + i], c) for c in range(2)
            ]
        return [along(m, ds.at[i], dr.at[i], dn_s.at[i], dn_r.at[i])]

    last = reduce_scatter(DOWN_TREE, own_down, emit_down, down_copies)
    own_mid = []
    for m in range(blocks):
        z, half = place(lax.rem(me, 4), m)
        own_mid.append(midg[z, half, :, pl.ds(pl.multiple_of(me // 4 * 128, 128), 128)].astype(F32))
    left, right = halves(own_down(me) + jnp.concatenate(own_mid, axis=0))
    fxs[...] = jnp.where(tp == 0, right, left)
    fin_x = to_partner(fxs, fxr, 5)
    fin_x.start()
    sends.append(fin_x)
    fin_x.wait_recv()
    sums = [jnp.where(tp == 0, left, right), fxr[...]]
    sums = [jnp.where(tp == 0, sums[0], sums[1]), jnp.where(tp == 0, sums[1], sums[0])]
    for m in last:
        for r in range(2):
            i = m[0]
            along(m, fs.at[i, r], fr.at[r, i], fs_s.at[2 * i + r], fr_r.at[r * msgs_n + i], r).wait_recv()
            sums[r] = sums[r] + fr[r, i].astype(F32)
    flat = jnp.concatenate(
        [sums[r][m * seqs : (m + 1) * seqs] for m in range(blocks // 2) for r in range(2)], axis=0
    ).T
    out[...] = jnp.concatenate([flat[0:half_ch], flat[half_ch : 2 * half_ch]], axis=1).astype(BF16)
    for c in sends:
        c.wait_send()


def hand_over(*refs):
    count = (len(refs) - 1) // 2
    sems = refs[-1]
    copies = [pltpu.make_async_copy(refs[i], refs[count + i], sems.at[i]) for i in range(count)]
    for c in copies:
        c.start()
    for c in copies:
        c.wait()


def shards(n, columns, *args):
    (tok, ngain, wq, wk, wv, wg, wi, wf, ib, fb, mem, nrm, stab, wo, mgain, wup, wdn) = args
    rows, half_ch = tok.shape
    chans = ngain.shape[0]
    seqs, heads, qk, vd = mem.shape
    hw, vw = heads * qk, heads * vd
    proj = 2 * hw + 2 * vw
    wide = proj + 128
    width = mgain.shape[0]
    hid = wup.shape[1]
    msgs = n - 1
    any_space = pl.BlockSpec(memory_space=pl.ANY)
    vmem = pl.BlockSpec(memory_space=pltpu.VMEM)
    dma = pltpu.SemaphoreType.DMA
    out = pl.pallas_call(
        functools.partial(kernel, n, columns),
        out_shape=(
            pltpu.VMEM((half_ch, rows), BF16),
            pltpu.VMEM(mem.shape, F32),
            pltpu.VMEM(nrm.shape, F32),
            pltpu.VMEM((heads, seqs), F32),
        ),
        in_specs=[any_space] * 17,
        out_specs=(vmem,) * 4,
        scratch_shapes=[
            pltpu.VMEM((2, half_ch, rows), BF16),
            pltpu.VMEM((1, chans), F32),
            pltpu.VMEM((chans, proj), BF16),
            pltpu.VMEM((2, wi.shape[1], chans), BF16),
            pltpu.VMEM((1, ib.shape[0]), F32),
            pltpu.VMEM((1, fb.shape[0]), F32),
            pltpu.VMEM(mem.shape, F32),
            pltpu.VMEM(nrm.shape, F32),
            pltpu.VMEM((heads, seqs), F32),
            pltpu.VMEM((2, wo.shape[0], 512), BF16),
            pltpu.VMEM((width // 128, 128), F32),
            pltpu.VMEM((2, *wup.shape), BF16),
            pltpu.VMEM((2, *wdn.shape), BF16),
            pltpu.VMEM((n, seqs, wide), F32),
            pltpu.VMEM((msgs, seqs, wide), BF16),
            pltpu.VMEM((msgs, seqs, wide), BF16),
            pltpu.VMEM((seqs, proj), F32),
            pltpu.VMEM((seqs, vw), F32),
            pltpu.VMEM((n, seqs, 128), F32),
            pltpu.VMEM((3, 2, seqs, 128), BF16),
            pltpu.VMEM((4, 2, seqs, 128), BF16),
            pltpu.VMEM((2, seqs, 128), BF16),
            pltpu.VMEM((seqs, vw), BF16),
            pltpu.VMEM((2, 2, seqs, vw), BF16),
            pltpu.VMEM((n, 2, seqs, 512), BF16),
            pltpu.VMEM((msgs, rows // 2, 128), BF16),
            pltpu.VMEM((msgs, rows // 2, 128), BF16),
            pltpu.VMEM((msgs, 2, rows // 4, 128), BF16),
            pltpu.VMEM((2, msgs, rows // 4, 128), BF16),
            pltpu.VMEM((rows // 4, 128), F32),
            pltpu.VMEM((rows // 4, 128), F32),
            dma((20,)),
            dma((10,)),
            dma((10,)),
            dma((msgs,)),
            dma((msgs,)),
            dma((msgs,)),
            dma((msgs,)),
            dma((msgs,)),
            dma((msgs,)),
            dma((msgs,)),
            dma((msgs,)),
            dma((2 * msgs,)),
            dma((2 * msgs,)),
            dma((7 + 3 * (columns - 1),)),
            dma((7 + 3 * (columns - 1),)),
        ],
        compiler_params=pltpu.CompilerParams(collective_id=0, has_side_effects=True, vmem_limit_bytes=40 * 2**20),
        name="cell_step",
    )(*[pltpu.with_memory_space_constraint(x, pltpu.HBM) for x in (
        tok.T,
        ngain.reshape(1, -1),
        wq,
        wk,
        wv,
        wg,
        wi.T,
        wf.T,
        ib.reshape(1, -1),
        fb.reshape(1, -1),
        mem,
        nrm,
        stab.T,
        wo,
        mgain.reshape(-1, 128),
        wup,
        wdn,
    )])
    out = pl.pallas_call(
        hand_over,
        out_shape=tuple(jax.ShapeDtypeStruct(o.shape, o.dtype) for o in out),
        in_specs=[vmem] * 4,
        out_specs=(any_space,) * 4,
        scratch_shapes=[dma((4,))],
        name="hand_over",
    )(*[pltpu.with_memory_space_constraint(o, pltpu.VMEM) for o in out])
    return out[0].T, out[1], out[2], out[3].T


def solution(mesh):
    placed = (
        P(("grp", "dp"), ("kv", "tp")),
        P("kv"),
        P("kv", "tp"),
        P("kv", "tp"),
        P("kv", "tp"),
        P("kv", "tp"),
        P("kv", None),
        P("kv", None),
        P(),
        P(),
        P(("grp", "dp", "kv"), "tp", None, None),
        P(("grp", "dp", "kv"), "tp"),
        P(("grp", "dp", "kv"), "tp"),
        P("tp", "kv"),
        P(),
        P(None, ("kv", "tp")),
        P(("kv", "tp"), None),
    )
    return jax.shard_map(
        functools.partial(shards, mesh.shape["kv"], mesh.shape["dp"]),
        mesh=mesh,
        in_specs=placed,
        out_specs=(
            P(("grp", "dp"), ("kv", "tp")),
            P(("grp", "dp", "kv"), "tp", None, None),
            P(("grp", "dp", "kv"), "tp"),
            P(("grp", "dp", "kv"), "tp"),
        ),
        check_vma=False,
    )
```

```python
import functools

import jax
import jax.numpy as jnp
from jax import lax
from jax.experimental import pallas as pl
from jax.experimental.pallas import tpu as pltpu
from jax.sharding import PartitionSpec as P

EPSILON = 1e-06
MESH = pl.DeviceIdType.MESH
F32 = jnp.float32
BF16 = jnp.bfloat16

TWO_LEVEL = {1: 0, 2: 0, 3: 0, 4: 0, 5: 4, 6: 4, 7: 4, 8: 4}
PROJ_TREE = TWO_LEVEL
REACH = 4
MID_TREE = TWO_LEVEL
DOWN_TREE = TWO_LEVEL


def messages(tree, n):
    out = []
    for side in (1, -1):
        for k in range(1, n // 2):
            out.append((len(out), side, k, tree[k]))
    out.append((len(out), 0, n // 2, tree[n // 2]))
    return out


def children_of(msgs, side, k):
    return [m for m in msgs if m[1] in (side, 0) and m[3] == k and k > 0]


def depth_below(msgs, m):
    below = children_of(msgs, m[1], m[2])
    return 1 + max(depth_below(msgs, c) for c in below) if below else 0


def level_of(tree, k):
    return 0 if k == 0 else 1 + level_of(tree, tree[k])


def kernel(
    n,
    columns,
    tok,
    ngain,
    wq,
    wk,
    wv,
    wg,
    wi,
    wf,
    ib,
    fb,
    mem,
    nrm,
    stab,
    wo,
    mgain,
    wup,
    wdn,
    out,
    mem_new,
    nrm_new,
    stab_new,
    tokb,
    ngv,
    wp,
    wib,
    ibb,
    fbb,
    memb,
    nrmb,
    stabb,
    wob,
    mgb,
    wupb,
    wdnb,
    pf,
    ps,
    pr,
    sf,
    ro,
    tokrow,
    tst,
    tokx,
    tfwd,
    hid_own,
    hidg,
    midg,
    ds,
    dr,
    fs,
    fr,
    fxs,
    fxr,
    lsem,
    xs,
    xr,
    ps_s,
    ps_r,
    hid_s,
    hid_r,
    mid_s,
    mid_r,
    dn_s,
    dn_r,
    fs_s,
    fr_r,
    pre_s,
    pre_r,
):
    me = lax.axis_index("kv")
    tp = lax.axis_index("tp")
    column = lax.axis_index("dp")
    other = 1 - tp
    half_ch, rows = tokb.shape[1:]
    seqs, heads, qk, vd = memb.shape
    hw = heads * qk
    vw = heads * vd
    proj = wp.shape[1]
    width = mgb.shape[0] * mgb.shape[1]
    half_rows = rows // 2
    wo_rows = wob.shape[1]

    def at(z):
        return lax.rem(z + 2 * n, n)

    far_side = 1 - 2 * lax.rem(me, 2)

    def way(side):
        return far_side if side == 0 else side

    barrier = pltpu.get_barrier_semaphore()
    for step in range(1, REACH + 1):
        for side in (1, -1):
            pl.semaphore_signal(barrier, inc=1, device_id={"kv": at(me + side * step)}, device_id_type=MESH)
    pl.semaphore_signal(barrier, inc=1, device_id={"tp": other}, device_id_type=MESH)
    for step in range(1, columns):
        pl.semaphore_signal(barrier, inc=1, device_id={"dp": lax.rem(column + step, columns)}, device_id_type=MESH)

    loads = {}

    def load(name, src, dst):
        c = pltpu.make_async_copy(src, dst, lsem.at[len(loads)])
        c.start()
        loads[name] = c

    load("tok", tok, tokb.at[tp])
    load("wo", wo, wob.at[tp, :, 0:128])
    load("ngain", ngain, ngv)
    load("wq", wq, wp.at[:, 0:hw])
    load("wk", wk, wp.at[:, hw : 2 * hw])
    load("wv", wv, wp.at[:, 2 * hw : 2 * hw + vw])
    load("wg", wg, wp.at[:, 2 * hw + vw : proj])
    load("wi", wi, wib.at[0])
    load("wf", wf, wib.at[1])
    load("ib", ib, ibb)
    load("fb", fb, fbb)
    load("stab", stab, stabb)
    load("nrm", nrm, nrmb)
    load("mem", mem, memb)
    load("mgain", mgain, mgb)
    load("wup", wup, wupb.at[tp])
    load("wdn", wdn, wdnb.at[tp])

    pl.semaphore_wait(barrier, 2 * REACH + columns)

    def to_partner(src, dst, i):
        return pltpu.make_async_remote_copy(
            src_ref=src, dst_ref=dst, send_sem=xs.at[i], recv_sem=xr.at[i], device_id={"tp": other}, device_id_type=MESH
        )

    loads["tok"].wait()
    tok_x = to_partner(tokb.at[tp], tokb.at[tp], 0)
    tok_x.start()
    sends = [tok_x]

    stride = n // 4
    piece_rows = wo_rows // columns
    parity = lax.rem(me, 2)
    mine_offset = jnp.where(tp == parity, 0, -1)

    def piece(x):
        return pl.ds(pl.multiple_of(x * piece_rows, piece_rows), piece_rows)

    def lanes(slot):
        return pl.ds(slot * 128 if isinstance(slot, int) else pl.multiple_of(slot * 128, 128), 128)

    def hop(src, dst, i, step, side="kv"):
        where = at(me + step) if side == "kv" else lax.rem(column + step, columns)
        return pltpu.make_async_remote_copy(
            src_ref=src, dst_ref=dst, send_sem=pre_s.at[i], recv_sem=pre_r.at[i], device_id={side: where}, device_id_type=MESH
        )

    def piece_hop(source, slot, i, step):
        return hop(wob.at[tp, piece(column), lanes(source)], wob.at[tp, piece(column), lanes(slot)], i, step)

    pre = {
        "w_up": piece_hop(0, 3, 0, stride),
        "w_dn": piece_hop(0, 1, 1, -stride),
        "t_up": hop(tst.at[0], tokx.at[3], 2, stride),
        "t_dn": hop(tst.at[1], tokx.at[1], 3, -stride),
        "t_on": hop(tst.at[2], tfwd, 4, far_side * stride),
        "w_fw": piece_hop(2 + far_side, 2, 5, far_side * stride),
        "t_fw": hop(tfwd, tokx.at[2], 6, far_side * stride),
    }

    def begin(c):
        c.start()
        sends.append(c)

    def column_copy(slot, step):
        part = wob.at[tp, piece(column), lanes(slot)]
        return hop(part, part, 7 + (slot - 1) * (columns - 1) + step - 1, step, "dp")

    def column_arrival(slot, step):
        part = wob.at[tp, piece(lax.rem(column - step + columns, columns)), lanes(slot)]
        return hop(part, part, 7 + (slot - 1) * (columns - 1) + step - 1, step, "dp")

    by_distance = sorted(range(1, columns), key=lambda step: -min(step, columns - step))

    def to_columns(slot):
        for step in by_distance:
            begin(column_copy(slot, step))

    def from_columns(slot):
        for step in range(1, columns):
            column_arrival(slot, step).wait_recv()

    def share_slot(slot):
        part = wob.at[tp, :, lanes(slot)]
        return to_partner(part, part, 6 + slot)

    def forward_on():
        pre["w_up"].wait_recv()
        pre["w_dn"].wait_recv()
        begin(pre["w_fw"])
        to_columns(3)
        to_columns(1)
        pre["t_on"].wait_recv()
        begin(pre["t_fw"])

    def complete_near():
        pre["w_fw"].wait_recv()
        to_columns(2)
        for slot in (3, 1):
            from_columns(slot)
            begin(share_slot(slot))

    loads["wo"].wait()
    begin(pre["w_up"])
    begin(pre["w_dn"])
    begin(share_slot(0))

    for name in ("ngain", "wq", "wk", "wv", "wg", "wi", "wf"):
        loads[name].wait()

    gate_lanes = 2 * wib.shape[1]
    lane128 = lax.broadcasted_iota(jnp.int32, (rows, 128), 1)
    gw = jnp.concatenate(
        [wib[0].astype(F32), wib[1].astype(F32), jnp.zeros((128 - gate_lanes, 2 * half_ch), F32)], axis=0
    ).astype(BF16)
    tok_x.wait_recv()
    t = jnp.concatenate([tokb[0], tokb[1]], axis=0).astype(F32).T
    scaled = (t * ngv[...]).astype(BF16)
    main = jnp.dot(scaled, wp[...], preferred_element_type=F32)
    gates = lax.dot_general(scaled, gw, (((1,), (1,)), ((), ())), preferred_element_type=F32)
    pf[:, :, 0:proj] = main.reshape(n, seqs, proj)
    pf[:, :, proj:] = jnp.where(lane128 == gate_lanes, jnp.sum(t * t, axis=1, keepdims=True), gates).reshape(n, seqs, 128)
    tokrow[...] = t.reshape(n, seqs, 2 * half_ch)

    lane8 = lax.broadcasted_iota(jnp.int32, (seqs, 128), 1)

    def pack_gates(g):
        total = g[:, gate_lanes : gate_lanes + 1] + g[:, gate_lanes + 1 : gate_lanes + 2]
        upper = total.astype(BF16).astype(F32)
        return jnp.where(lane8 == gate_lanes, upper, jnp.where(lane8 == gate_lanes + 1, total - upper, g))

    def reduce_scatter(tree, own, emit, copies_of, before_relays=None):
        msgs = messages(tree, n)
        order = sorted(msgs, key=lambda m: (depth_below(msgs, m), -level_of(tree, m[2]), -m[2]))
        waited = set()
        for m in order:
            slot, side, k, parent = m
            mine = own(at(me - way(side) * k))
            kids = children_of(msgs, side, k)
            if kids and before_relays is not None:
                before_relays()
                before_relays = None
            for c in kids:
                if c[0] not in waited:
                    waited.add(c[0])
                    copies_of(c)[0].wait_recv()
            emit(m, mine, [(c[0], None if c[1] else far_side == side) for c in kids])
            for c in copies_of(m):
                c.start()
                sends.append(c)
        return [m for m in msgs if m[3] == 0]

    def along(m, src, dst, send_sem, recv_sem, core=None):
        slot, side, k, parent = m
        where = {"kv": at(me - way(side) * (k - parent))}
        if core is not None:
            where["tp"] = core
        return pltpu.make_async_remote_copy(
            src_ref=src, dst_ref=dst, send_sem=send_sem, recv_sem=recv_sem, device_id=where, device_id_type=MESH
        )

    def all_gather(tree, buf, send_sem, recv_sem):
        msgs = messages(tree, n)

        def copy_of(m):
            slot, side, k, parent = m
            side = way(side)
            origin = at(me - side * parent)
            return pltpu.make_async_remote_copy(
                src_ref=buf.at[origin],
                dst_ref=buf.at[origin],
                send_sem=send_sem.at[slot],
                recv_sem=recv_sem.at[slot],
                device_id={"kv": at(me + side * (k - parent))},
                device_id_type=MESH,
            )

        def arrival(m):
            slot, side, k, parent = m
            side = way(side)
            origin = at(me - side * k)
            return pltpu.make_async_remote_copy(
                src_ref=buf.at[origin],
                dst_ref=buf.at[origin],
                send_sem=send_sem.at[slot],
                recv_sem=recv_sem.at[slot],
                device_id={"kv": at(me - side * k)},
                device_id_type=MESH,
            )

        def send(m):
            c = copy_of(m)
            c.start()
            sends.append(c)

        waited = set()
        firsts = [m for m in msgs if m[3] == 0]
        for m in sorted(firsts, key=lambda m: (-depth_below(msgs, m), -m[2])):
            send(m)

        def finish():
            todo = sorted([m for m in msgs if children_of(msgs, m[1], m[2])], key=lambda m: (level_of(tree, m[2]), m[2]))
            for m in todo:
                arrival(m).wait_recv()
                waited.add(m[0])
            for c in sorted([c for c in msgs if c[3]], key=lambda c: (level_of(tree, c[2]), -c[2])):
                send(c)
            for m in msgs:
                if m[0] not in waited:
                    arrival(m).wait_recv()

        return finish

    for i, step in enumerate((stride, -stride, 2 * stride)):
        for b in range(2):
            tst[i, b] = tokrow[at(me + step + mine_offset + 2 * b)].astype(BF16)

    def own_proj(d):
        return pf[d, :, 0:proj], pf[d, :, proj:]

    def sum_proj(mine, slots):
        a, g = mine
        for s, here in slots:
            more_a, more_g = pr[s, :, 0:proj].astype(F32), pr[s, :, proj:].astype(F32)
            if here is not None:
                more_a, more_g = jnp.where(here, more_a, 0.0), jnp.where(here, more_g, 0.0)
            a = a + more_a
            g = g + more_g
        return a, g

    def emit_proj(m, mine, slots):
        slot = m[0]
        a, g = sum_proj(mine, slots)
        ps[slot, :, 0:proj] = a.astype(BF16)
        ps[slot, :, proj:] = pack_gates(g).astype(BF16)

    def proj_copies(m):
        i = m[0]
        return [along(m, ps.at[i], pr.at[i], ps_s.at[i], ps_r.at[i])]

    for name in ("t_on", "t_up", "t_dn"):
        begin(pre[name])
    last = reduce_scatter(PROJ_TREE, own_proj, emit_proj, proj_copies, forward_on)
    complete_near()

    loads["wup"].wait()
    loads["wdn"].wait()
    up_x = to_partner(wupb.at[tp], wupb.at[tp], 1)
    up_x.start()
    dn_x = to_partner(wdnb.at[tp], wdnb.at[tp], 2)
    dn_x.start()
    sends += [up_x, dn_x]
    for name in ("ib", "fb", "stab", "nrm", "mem", "mgain"):
        loads[name].wait()

    for m in last:
        proj_copies(m)[0].wait_recv()
    slots = [(m[0], None) for m in last]
    total, gate = sum_proj(own_proj(me), slots)
    sf[:, 0:proj] = total
    squares = gate[:, gate_lanes : gate_lanes + 1] + gate[:, gate_lanes + 1 : gate_lanes + 2]
    rscale = lax.rsqrt(squares / width + EPSILON)
    q = sf[:, 0:hw] * rscale
    k = sf[:, hw : 2 * hw] * rscale * qk ** (-0.5)
    v = sf[:, 2 * hw : 2 * hw + vw] * rscale
    all_heads = wib.shape[1]

    def mine_of(x, first):
        return jnp.where(tp == 0, x[:, first : first + heads], x[:, first + heads : first + 2 * heads])

    log_in = mine_of(gate, 0) * rscale + mine_of(ibb[...], 0)
    fpre = mine_of(gate, all_heads) * rscale + mine_of(fbb[...], 0)
    log_forget = jnp.minimum(fpre, 0.0) - jnp.log(1.0 + jnp.exp(-jnp.abs(fpre)))
    carried = log_forget + stabb[...].T
    snew = jnp.maximum(carried, log_in)
    take = jnp.exp(log_in - snew)
    keep = jnp.exp(carried - snew)
    stab_new[...] = snew.T

    hlane = lax.broadcasted_iota(jnp.int32, (seqs, hw), 1) // qk

    def spread(x):
        r = jnp.broadcast_to(x[:, 0:1], (seqs, hw))
        for h in range(1, heads):
            r = jnp.where(hlane == h, x[:, h : h + 1], r)
        return r

    def per_head(x):
        return [jnp.sum(jnp.where(hlane == h, x, 0.0), axis=1, keepdims=True) for h in range(heads)]

    tk = spread(take) * k
    nrm_new[...] = spread(keep) * nrmb[...] + tk
    scores = per_head(q * k)
    nqs = per_head(nrmb[...] * q)
    qt = q.T
    for s in range(seqs):
        for h in range(heads):
            col = qt[h * qk : (h + 1) * qk, s : s + 1]
            ro[s : s + 1, h * vd : (h + 1) * vd] = jnp.sum(memb[s, h] * col, axis=0, keepdims=True)
    hidden = []
    for h in range(heads):
        ts = take[:, h : h + 1] * scores[h]
        kp = keep[:, h : h + 1]
        numer = ts * v[:, h * vd : (h + 1) * vd] + kp * ro[:, h * vd : (h + 1) * vd]
        denom = ts + kp * nqs[h]
        cell = numer / jnp.maximum(jnp.abs(denom), 1.0)
        og = sf[:, 2 * hw + vw + h * vd : 2 * hw + vw + (h + 1) * vd] * rscale
        hid_own[:, h * vd : (h + 1) * vd] = ((1.0 / (1.0 + jnp.exp(-og))) * cell).astype(BF16)

    def hid_hop(i, slot, step):
        return pltpu.make_async_remote_copy(
            src_ref=hid_own,
            dst_ref=hidg.at[slot, tp],
            send_sem=hid_s.at[i],
            recv_sem=hid_r.at[2 * slot + tp],
            device_id={"kv": at(me + step), "tp": parity},
            device_id_type=MESH,
        )

    for i, (slot, step) in enumerate(((1, -2), (0, 1), (1, -1))):
        begin(hid_hop(i, slot, step))
    own_hid = pltpu.make_async_remote_copy(
        src_ref=hid_own,
        dst_ref=hidg.at[0, tp],
        send_sem=hid_s.at[3],
        recv_sem=hid_r.at[tp],
        device_id={"tp": other},
        device_id_type=MESH,
    )

    @pl.when(tp != parity)
    def _():
        own_hid.start()

    @pl.when(tp == parity)
    def _():
        hidg[0, tp] = hid_own[...]

    kt = tk.T
    for s in range(seqs):
        for h in range(heads):
            col = kt[h * qk : (h + 1) * qk, s : s + 1]
            mem_new[s, h] = keep[s : s + 1, h : h + 1] * memb[s, h] + col * v[s : s + 1, h * vd : (h + 1) * vd]

    from_columns(2)
    begin(share_slot(2))
    for name in ("t_up", "t_dn", "t_fw"):
        pre[name].wait_recv()

    def hid_arrival(slot, core):
        pltpu.make_async_remote_copy(
            src_ref=hid_own,
            dst_ref=hidg.at[slot, core],
            send_sem=hid_s.at[0],
            recv_sem=hid_r.at[2 * slot + core],
            device_id={"tp": other},
            device_id_type=MESH,
        ).wait_recv()

    for i in range(2):
        tokx[0, i] = tokrow[at(me + mine_offset + 2 * i)].astype(BF16)

    @pl.when(tp != parity)
    def _():
        own_hid.wait_send()
        hid_arrival(0, tp)

    hid_arrival(0, other)
    for core in range(2):
        hid_arrival(1, core)
    for slot in range(4):
        share_slot(slot).wait_recv()
    left_rows = jnp.concatenate(
        [jnp.concatenate([hidg[i, h].astype(F32) for h in range(2)], axis=1) for i in range(2)], axis=0
    ).astype(BF16)
    added = jnp.dot(left_rows[:, 0:vw], wob[0], preferred_element_type=F32) + jnp.dot(
        left_rows[:, vw : 2 * vw], wob[1], preferred_element_type=F32
    )
    for slot in range(4):
        cols = lax.rem(me // 4 + slot, 4)
        block = added[:, slot * 128 : (slot + 1) * 128].reshape(2, seqs, 128) + tokx[slot].astype(F32)
        midg[me, :, :, pl.ds(pl.multiple_of(cols * 128, 128), 128)] = block.astype(BF16)
    all_gather(MID_TREE, midg, mid_s, mid_r)()

    up_x.wait_recv()
    dn_x.wait_recv()
    blocks = half_rows // seqs

    def place(group, m):
        z = tp + 2 * m
        offset = lax.rem(z - group + 1 + n, 4) - 1
        return at(z - offset), lax.div(offset + 1, 2)

    sq_sum = jnp.zeros((half_rows, 512), F32)
    acc = [None, None]
    for group in range(4):
        parts = []
        for m in range(blocks):
            z, half = place(group, m)
            parts.append(midg[z, half].astype(F32))
        x = jnp.concatenate(parts, axis=0)
        sq_sum = sq_sum + x * x
        for j in range(0, 4, 2):
            chans = [group + 4 * (j + i) for i in range(2)]
            xs_in = jnp.concatenate(
                [x[:, (j + i) * 128 : (j + i + 1) * 128] * mgb[c : c + 1, :] for i, c in enumerate(chans)], axis=1
            ).astype(BF16)
            for u in range(2):
                w = jnp.concatenate([wupb[u, c * 128 : (c + 1) * 128, :] for c in chans], axis=0)
                d = jnp.dot(xs_in, w, preferred_element_type=F32)
                acc[u] = d if acc[u] is None else acc[u] + d
    rmid = lax.rsqrt(jnp.sum(sq_sum, axis=1, keepdims=True) / width + EPSILON)
    sqd = [jnp.square(jnp.maximum(a * rmid, 0.0)).astype(BF16) for a in acc]

    def own_down(d):
        cols = pl.ds(pl.multiple_of(d * 128, 128), 128)
        return jnp.dot(sqd[0], wdnb[0, :, cols], preferred_element_type=F32) + jnp.dot(
            sqd[1], wdnb[1, :, cols], preferred_element_type=F32
        )

    def sum_down(a, slots):
        for s, here in slots:
            more = dr[s].astype(F32)
            a = a + (more if here is None else jnp.where(here, more, 0.0))
        return a

    def halves(a):
        return [
            jnp.concatenate([a[0:quarter, h : h + half_ch], a[quarter : 2 * quarter, h : h + half_ch]], axis=1)
            for h in (0, half_ch)
        ]

    quarter = half_rows // 2
    msgs_n = n - 1

    def emit_down(m, mine, slots):
        a = sum_down(mine, slots)
        if m[3] == 0:
            fs[m[0], 0], fs[m[0], 1] = [x.astype(BF16) for x in halves(a)]
        else:
            ds[m[0]] = a.astype(BF16)

    def down_copies(m):
        i = m[0]
        if m[3] == 0:
            return [
                along(m, fs.at[i, c], fr.at[tp, i], fs_s.at[2 * i + c], fr_r.at[tp * msgs_n + i], c) for c in range(2)
            ]
        return [along(m, ds.at[i], dr.at[i], dn_s.at[i], dn_r.at[i])]

    last = reduce_scatter(DOWN_TREE, own_down, emit_down, down_copies)
    own_mid = []
    for m in range(blocks):
        z, half = place(lax.rem(me, 4), m)
        own_mid.append(midg[z, half, :, pl.ds(pl.multiple_of(me // 4 * 128, 128), 128)].astype(F32))
    left, right = halves(own_down(me) + jnp.concatenate(own_mid, axis=0))
    fxs[...] = jnp.where(tp == 0, right, left)
    fin_x = to_partner(fxs, fxr, 5)
    fin_x.start()
    sends.append(fin_x)
    early = len(sends)
    for c in sends[:-1]:
        c.wait_send()
    early -= 1
    fin_x.wait_recv()
    sums = [jnp.where(tp == 0, left, right), fxr[...]]
    sums = [jnp.where(tp == 0, sums[0], sums[1]), jnp.where(tp == 0, sums[1], sums[0])]
    for m in last:
        for r in range(2):
            i = m[0]
            along(m, fs.at[i, r], fr.at[r, i], fs_s.at[2 * i + r], fr_r.at[r * msgs_n + i], r).wait_recv()
            sums[r] = sums[r] + fr[r, i].astype(F32)
    flat = jnp.concatenate(
        [sums[r][m * seqs : (m + 1) * seqs] for m in range(blocks // 2) for r in range(2)], axis=0
    ).T
    out[...] = jnp.concatenate([flat[0:half_ch], flat[half_ch : 2 * half_ch]], axis=1).astype(BF16)
    for c in sends[early:]:
        c.wait_send()


def hand_over(*refs):
    count = (len(refs) - 1) // 2
    sems = refs[-1]
    copies = [pltpu.make_async_copy(refs[i], refs[count + i], sems.at[i]) for i in range(count)]
    for c in copies:
        c.start()
    for c in copies:
        c.wait()


def shards(n, columns, *args):
    (tok, ngain, wq, wk, wv, wg, wi, wf, ib, fb, mem, nrm, stab, wo, mgain, wup, wdn) = args
    rows, half_ch = tok.shape
    chans = ngain.shape[0]
    seqs, heads, qk, vd = mem.shape
    hw, vw = heads * qk, heads * vd
    proj = 2 * hw + 2 * vw
    wide = proj + 128
    width = mgain.shape[0]
    hid = wup.shape[1]
    msgs = n - 1
    any_space = pl.BlockSpec(memory_space=pl.ANY)
    vmem = pl.BlockSpec(memory_space=pltpu.VMEM)
    dma = pltpu.SemaphoreType.DMA
    out = pl.pallas_call(
        functools.partial(kernel, n, columns),
        out_shape=(
            pltpu.VMEM((half_ch, rows), BF16),
            pltpu.VMEM(mem.shape, F32),
            pltpu.VMEM(nrm.shape, F32),
            pltpu.VMEM((heads, seqs), F32),
        ),
        in_specs=[any_space] * 17,
        out_specs=(vmem,) * 4,
        scratch_shapes=[
            pltpu.VMEM((2, half_ch, rows), BF16),
            pltpu.VMEM((1, chans), F32),
            pltpu.VMEM((chans, proj), BF16),
            pltpu.VMEM((2, wi.shape[1], chans), BF16),
            pltpu.VMEM((1, ib.shape[0]), F32),
            pltpu.VMEM((1, fb.shape[0]), F32),
            pltpu.VMEM(mem.shape, F32),
            pltpu.VMEM(nrm.shape, F32),
            pltpu.VMEM((heads, seqs), F32),
            pltpu.VMEM((2, wo.shape[0], 512), BF16),
            pltpu.VMEM((width // 128, 128), F32),
            pltpu.VMEM((2, *wup.shape), BF16),
            pltpu.VMEM((2, *wdn.shape), BF16),
            pltpu.VMEM((n, seqs, wide), F32),
            pltpu.VMEM((msgs, seqs, wide), BF16),
            pltpu.VMEM((msgs, seqs, wide), BF16),
            pltpu.VMEM((seqs, proj), F32),
            pltpu.VMEM((seqs, vw), F32),
            pltpu.VMEM((n, seqs, 128), F32),
            pltpu.VMEM((3, 2, seqs, 128), BF16),
            pltpu.VMEM((4, 2, seqs, 128), BF16),
            pltpu.VMEM((2, seqs, 128), BF16),
            pltpu.VMEM((seqs, vw), BF16),
            pltpu.VMEM((2, 2, seqs, vw), BF16),
            pltpu.VMEM((n, 2, seqs, 512), BF16),
            pltpu.VMEM((msgs, rows // 2, 128), BF16),
            pltpu.VMEM((msgs, rows // 2, 128), BF16),
            pltpu.VMEM((msgs, 2, rows // 4, 128), BF16),
            pltpu.VMEM((2, msgs, rows // 4, 128), BF16),
            pltpu.VMEM((rows // 4, 128), F32),
            pltpu.VMEM((rows // 4, 128), F32),
            dma((20,)),
            dma((10,)),
            dma((10,)),
            dma((msgs,)),
            dma((msgs,)),
            dma((msgs,)),
            dma((msgs,)),
            dma((msgs,)),
            dma((msgs,)),
            dma((msgs,)),
            dma((msgs,)),
            dma((2 * msgs,)),
            dma((2 * msgs,)),
            dma((7 + 3 * (columns - 1),)),
            dma((7 + 3 * (columns - 1),)),
        ],
        compiler_params=pltpu.CompilerParams(collective_id=0, has_side_effects=True, vmem_limit_bytes=40 * 2**20),
        name="cell_step",
    )(*[pltpu.with_memory_space_constraint(x, pltpu.HBM) for x in (
        tok.T,
        ngain.reshape(1, -1),
        wq,
        wk,
        wv,
        wg,
        wi.T,
        wf.T,
        ib.reshape(1, -1),
        fb.reshape(1, -1),
        mem,
        nrm,
        stab.T,
        wo,
        mgain.reshape(-1, 128),
        wup,
        wdn,
    )])
    out = pl.pallas_call(
        hand_over,
        out_shape=tuple(jax.ShapeDtypeStruct(o.shape, o.dtype) for o in out),
        in_specs=[vmem] * 4,
        out_specs=(any_space,) * 4,
        scratch_shapes=[dma((4,))],
        name="hand_over",
    )(*[pltpu.with_memory_space_constraint(o, pltpu.VMEM) for o in out])
    return out[0].T, out[1], out[2], out[3].T


def solution(mesh):
    placed = (
        P(("grp", "dp"), ("kv", "tp")),
        P("kv"),
        P("kv", "tp"),
        P("kv", "tp"),
        P("kv", "tp"),
        P("kv", "tp"),
        P("kv", None),
        P("kv", None),
        P(),
        P(),
        P(("grp", "dp", "kv"), "tp", None, None),
        P(("grp", "dp", "kv"), "tp"),
        P(("grp", "dp", "kv"), "tp"),
        P("tp", "kv"),
        P(),
        P(None, ("kv", "tp")),
        P(("kv", "tp"), None),
    )
    return jax.shard_map(
        functools.partial(shards, mesh.shape["kv"], mesh.shape["dp"]),
        mesh=mesh,
        in_specs=placed,
        out_specs=(
            P(("grp", "dp"), ("kv", "tp")),
            P(("grp", "dp", "kv"), "tp", None, None),
            P(("grp", "dp", "kv"), "tp"),
            P(("grp", "dp", "kv"), "tp"),
        ),
        check_vma=False,
    )
```

```python
import functools

import jax
import jax.numpy as jnp
from jax import lax
from jax.experimental import pallas as pl
from jax.experimental.pallas import tpu as pltpu
from jax.sharding import PartitionSpec as P

EPSILON = 1e-06
MESH = pl.DeviceIdType.MESH
F32 = jnp.float32
BF16 = jnp.bfloat16

TWO_LEVEL = {1: 0, 2: 0, 3: 0, 4: 0, 5: 4, 6: 4, 7: 4, 8: 4}
PROJ_TREE = {1: 0, 2: 0, 3: 0, 4: 3, 5: 3, 6: 3, 7: 6, 8: 6}
REACH = 4
MID_TREE = TWO_LEVEL
DOWN_TREE = TWO_LEVEL


def messages(tree, n):
    out = []
    for side in (1, -1):
        for k in range(1, n // 2):
            out.append((len(out), side, k, tree[k]))
    out.append((len(out), 0, n // 2, tree[n // 2]))
    return out


def children_of(msgs, side, k):
    return [m for m in msgs if m[1] in (side, 0) and m[3] == k and k > 0]


def depth_below(msgs, m):
    below = children_of(msgs, m[1], m[2])
    return 1 + max(depth_below(msgs, c) for c in below) if below else 0


def level_of(tree, k):
    return 0 if k == 0 else 1 + level_of(tree, tree[k])


def kernel(
    n,
    columns,
    tok,
    ngain,
    wq,
    wk,
    wv,
    wg,
    wi,
    wf,
    ib,
    fb,
    mem,
    nrm,
    stab,
    wo,
    mgain,
    wup,
    wdn,
    out,
    mem_new,
    nrm_new,
    stab_new,
    tokb,
    ngv,
    wp,
    wib,
    ibb,
    fbb,
    memb,
    nrmb,
    stabb,
    wob,
    mgb,
    wupb,
    wdnb,
    pf,
    ps,
    pr,
    sf,
    ro,
    tokrow,
    tst,
    tokx,
    tfwd,
    hid_own,
    hidg,
    midg,
    ds,
    dr,
    fs,
    fr,
    fxs,
    fxr,
    lsem,
    xs,
    xr,
    ps_s,
    ps_r,
    hid_s,
    hid_r,
    mid_s,
    mid_r,
    dn_s,
    dn_r,
    fs_s,
    fr_r,
    pre_s,
    pre_r,
):
    me = lax.axis_index("kv")
    tp = lax.axis_index("tp")
    column = lax.axis_index("dp")
    other = 1 - tp
    half_ch, rows = tokb.shape[1:]
    seqs, heads, qk, vd = memb.shape
    hw = heads * qk
    vw = heads * vd
    proj = wp.shape[1]
    width = mgb.shape[0] * mgb.shape[1]
    half_rows = rows // 2
    wo_rows = wob.shape[1]

    def at(z):
        return lax.rem(z + 2 * n, n)

    far_side = 1 - 2 * lax.rem(me, 2)

    def way(side):
        return far_side if side == 0 else side

    barrier = pltpu.get_barrier_semaphore()
    for step in range(1, REACH + 1):
        for side in (1, -1):
            pl.semaphore_signal(barrier, inc=1, device_id={"kv": at(me + side * step)}, device_id_type=MESH)
    pl.semaphore_signal(barrier, inc=1, device_id={"tp": other}, device_id_type=MESH)
    for step in range(1, columns):
        pl.semaphore_signal(barrier, inc=1, device_id={"dp": lax.rem(column + step, columns)}, device_id_type=MESH)

    loads = {}

    def load(name, src, dst):
        c = pltpu.make_async_copy(src, dst, lsem.at[len(loads)])
        c.start()
        loads[name] = c

    load("tok", tok, tokb.at[tp])
    load("wo", wo, wob.at[tp, :, 0:128])
    load("ngain", ngain, ngv)
    load("wq", wq, wp.at[:, 0:hw])
    load("wk", wk, wp.at[:, hw : 2 * hw])
    load("wv", wv, wp.at[:, 2 * hw : 2 * hw + vw])
    load("wg", wg, wp.at[:, 2 * hw + vw : proj])
    load("wi", wi, wib.at[0])
    load("wf", wf, wib.at[1])
    load("ib", ib, ibb)
    load("fb", fb, fbb)
    load("stab", stab, stabb)
    load("nrm", nrm, nrmb)
    load("mem", mem, memb)
    load("mgain", mgain, mgb)
    load("wup", wup, wupb.at[tp])
    load("wdn", wdn, wdnb.at[tp])

    pl.semaphore_wait(barrier, 2 * REACH + columns)

    def to_partner(src, dst, i):
        return pltpu.make_async_remote_copy(
            src_ref=src, dst_ref=dst, send_sem=xs.at[i], recv_sem=xr.at[i], device_id={"tp": other}, device_id_type=MESH
        )

    loads["tok"].wait()
    tok_x = to_partner(tokb.at[tp], tokb.at[tp], 0)
    tok_x.start()
    sends = [tok_x]

    stride = n // 4
    piece_rows = wo_rows // columns
    parity = lax.rem(me, 2)
    mine_offset = jnp.where(tp == parity, 0, -1)

    def piece(x):
        return pl.ds(pl.multiple_of(x * piece_rows, piece_rows), piece_rows)

    def lanes(slot):
        return pl.ds(slot * 128 if isinstance(slot, int) else pl.multiple_of(slot * 128, 128), 128)

    def hop(src, dst, i, step, side="kv"):
        where = at(me + step) if side == "kv" else lax.rem(column + step, columns)
        return pltpu.make_async_remote_copy(
            src_ref=src, dst_ref=dst, send_sem=pre_s.at[i], recv_sem=pre_r.at[i], device_id={side: where}, device_id_type=MESH
        )

    def piece_hop(source, slot, i, step):
        return hop(wob.at[tp, piece(column), lanes(source)], wob.at[tp, piece(column), lanes(slot)], i, step)

    pre = {
        "w_up": piece_hop(0, 3, 0, stride),
        "w_dn": piece_hop(0, 1, 1, -stride),
        "t_up": hop(tst.at[0], tokx.at[3], 2, stride),
        "t_dn": hop(tst.at[1], tokx.at[1], 3, -stride),
        "t_on": hop(tst.at[2], tfwd, 4, far_side * stride),
        "w_fw": piece_hop(2 + far_side, 2, 5, far_side * stride),
        "t_fw": hop(tfwd, tokx.at[2], 6, far_side * stride),
    }

    def begin(c):
        c.start()
        sends.append(c)

    def column_copy(slot, step):
        part = wob.at[tp, piece(column), lanes(slot)]
        return hop(part, part, 7 + (slot - 1) * (columns - 1) + step - 1, step, "dp")

    def column_arrival(slot, step):
        part = wob.at[tp, piece(lax.rem(column - step + columns, columns)), lanes(slot)]
        return hop(part, part, 7 + (slot - 1) * (columns - 1) + step - 1, step, "dp")

    by_distance = sorted(range(1, columns), key=lambda step: -min(step, columns - step))

    def to_columns(slot):
        for step in by_distance:
            begin(column_copy(slot, step))

    def from_columns(slot):
        for step in range(1, columns):
            column_arrival(slot, step).wait_recv()

    def share_slot(slot):
        part = wob.at[tp, :, lanes(slot)]
        return to_partner(part, part, 6 + slot)

    up_x = to_partner(wupb.at[tp], wupb.at[tp], 1)
    dn_x = to_partner(wdnb.at[tp], wdnb.at[tp], 2)

    def forward_on():
        loads["wup"].wait()
        begin(up_x)
        loads["wdn"].wait()
        begin(dn_x)
        pre["w_up"].wait_recv()
        pre["w_dn"].wait_recv()
        begin(pre["w_fw"])
        to_columns(3)
        to_columns(1)

    def complete_near():
        pre["t_on"].wait_recv()
        begin(pre["t_fw"])
        pre["w_fw"].wait_recv()
        to_columns(2)

    loads["wo"].wait()
    begin(pre["w_up"])
    begin(pre["w_dn"])
    begin(share_slot(0))

    for name in ("ngain", "wq", "wk", "wv", "wg", "wi", "wf"):
        loads[name].wait()

    gate_lanes = 2 * wib.shape[1]
    lane128 = lax.broadcasted_iota(jnp.int32, (rows, 128), 1)
    gw = jnp.concatenate(
        [wib[0].astype(F32), wib[1].astype(F32), jnp.zeros((128 - gate_lanes, 2 * half_ch), F32)], axis=0
    ).astype(BF16)
    tok_x.wait_recv()
    t = jnp.concatenate([tokb[0], tokb[1]], axis=0).astype(F32).T
    scaled = (t * ngv[...]).astype(BF16)
    main = jnp.dot(scaled, wp[...], preferred_element_type=F32)
    gates = lax.dot_general(scaled, gw, (((1,), (1,)), ((), ())), preferred_element_type=F32)
    pf[:, :, 0:proj] = main.reshape(n, seqs, proj)
    pf[:, :, proj:] = jnp.where(lane128 == gate_lanes, jnp.sum(t * t, axis=1, keepdims=True), gates).reshape(n, seqs, 128)
    tokrow[...] = t.reshape(n, seqs, 2 * half_ch)

    lane8 = lax.broadcasted_iota(jnp.int32, (seqs, 128), 1)

    def pack_gates(g):
        total = g[:, gate_lanes : gate_lanes + 1] + g[:, gate_lanes + 1 : gate_lanes + 2]
        upper = total.astype(BF16).astype(F32)
        return jnp.where(lane8 == gate_lanes, upper, jnp.where(lane8 == gate_lanes + 1, total - upper, g))

    def reduce_scatter(tree, own, emit, copies_of, before_relays=None):
        msgs = messages(tree, n)
        order = sorted(msgs, key=lambda m: (depth_below(msgs, m), -level_of(tree, m[2]), -m[2]))
        waited = set()
        for m in order:
            slot, side, k, parent = m
            mine = own(at(me - way(side) * k))
            kids = children_of(msgs, side, k)
            if kids and before_relays is not None:
                before_relays()
                before_relays = None
            for c in kids:
                if c[0] not in waited:
                    waited.add(c[0])
                    copies_of(c)[0].wait_recv()
            emit(m, mine, [(c[0], None if c[1] else far_side == side) for c in kids])
            for c in copies_of(m):
                c.start()
                sends.append(c)
        return [m for m in msgs if m[3] == 0]

    def along(m, src, dst, send_sem, recv_sem, core=None):
        slot, side, k, parent = m
        where = {"kv": at(me - way(side) * (k - parent))}
        if core is not None:
            where["tp"] = core
        return pltpu.make_async_remote_copy(
            src_ref=src, dst_ref=dst, send_sem=send_sem, recv_sem=recv_sem, device_id=where, device_id_type=MESH
        )

    def all_gather(tree, buf, send_sem, recv_sem):
        msgs = messages(tree, n)

        def copy_of(m):
            slot, side, k, parent = m
            side = way(side)
            origin = at(me - side * parent)
            return pltpu.make_async_remote_copy(
                src_ref=buf.at[origin],
                dst_ref=buf.at[origin],
                send_sem=send_sem.at[slot],
                recv_sem=recv_sem.at[slot],
                device_id={"kv": at(me + side * (k - parent))},
                device_id_type=MESH,
            )

        def arrival(m):
            slot, side, k, parent = m
            side = way(side)
            origin = at(me - side * k)
            return pltpu.make_async_remote_copy(
                src_ref=buf.at[origin],
                dst_ref=buf.at[origin],
                send_sem=send_sem.at[slot],
                recv_sem=recv_sem.at[slot],
                device_id={"kv": at(me - side * k)},
                device_id_type=MESH,
            )

        def send(m):
            c = copy_of(m)
            c.start()
            sends.append(c)

        waited = set()
        firsts = [m for m in msgs if m[3] == 0]
        for m in sorted(firsts, key=lambda m: (-depth_below(msgs, m), -m[2])):
            send(m)

        def finish():
            todo = sorted([m for m in msgs if children_of(msgs, m[1], m[2])], key=lambda m: (level_of(tree, m[2]), m[2]))
            for m in todo:
                arrival(m).wait_recv()
                waited.add(m[0])
            for c in sorted([c for c in msgs if c[3]], key=lambda c: (level_of(tree, c[2]), -c[2])):
                send(c)
            for m in msgs:
                if m[0] not in waited:
                    arrival(m).wait_recv()

        return finish

    for i, step in enumerate((stride, -stride, 2 * stride)):
        for b in range(2):
            tst[i, b] = tokrow[at(me + step + mine_offset + 2 * b)].astype(BF16)

    def own_proj(d):
        return pf[d, :, 0:proj], pf[d, :, proj:]

    def sum_proj(mine, slots):
        a, g = mine
        for s, here in slots:
            more_a, more_g = pr[s, :, 0:proj].astype(F32), pr[s, :, proj:].astype(F32)
            if here is not None:
                more_a, more_g = jnp.where(here, more_a, 0.0), jnp.where(here, more_g, 0.0)
            a = a + more_a
            g = g + more_g
        return a, g

    def emit_proj(m, mine, slots):
        slot = m[0]
        a, g = sum_proj(mine, slots)
        ps[slot, :, 0:proj] = a.astype(BF16)
        ps[slot, :, proj:] = pack_gates(g).astype(BF16)

    def proj_copies(m):
        i = m[0]
        return [along(m, ps.at[i], pr.at[i], ps_s.at[i], ps_r.at[i])]

    for name in ("t_on", "t_up", "t_dn"):
        begin(pre[name])
    last = reduce_scatter(PROJ_TREE, own_proj, emit_proj, proj_copies, forward_on)
    complete_near()

    for name in ("ib", "fb", "stab", "nrm", "mem", "mgain"):
        loads[name].wait()

    for m in last:
        proj_copies(m)[0].wait_recv()
    slots = [(m[0], None) for m in last]
    total, gate = sum_proj(own_proj(me), slots)
    sf[:, 0:proj] = total
    squares = gate[:, gate_lanes : gate_lanes + 1] + gate[:, gate_lanes + 1 : gate_lanes + 2]
    rscale = lax.rsqrt(squares / width + EPSILON)
    q = sf[:, 0:hw] * rscale
    k = sf[:, hw : 2 * hw] * rscale * qk ** (-0.5)
    v = sf[:, 2 * hw : 2 * hw + vw] * rscale
    all_heads = wib.shape[1]

    def mine_of(x, first):
        return jnp.where(tp == 0, x[:, first : first + heads], x[:, first + heads : first + 2 * heads])

    log_in = mine_of(gate, 0) * rscale + mine_of(ibb[...], 0)
    fpre = mine_of(gate, all_heads) * rscale + mine_of(fbb[...], 0)
    log_forget = jnp.minimum(fpre, 0.0) - jnp.log(1.0 + jnp.exp(-jnp.abs(fpre)))
    carried = log_forget + stabb[...].T
    snew = jnp.maximum(carried, log_in)
    take = jnp.exp(log_in - snew)
    keep = jnp.exp(carried - snew)
    stab_new[...] = snew.T

    hlane = lax.broadcasted_iota(jnp.int32, (seqs, hw), 1) // qk

    def spread(x):
        r = jnp.broadcast_to(x[:, 0:1], (seqs, hw))
        for h in range(1, heads):
            r = jnp.where(hlane == h, x[:, h : h + 1], r)
        return r

    def per_head(x):
        return [jnp.sum(jnp.where(hlane == h, x, 0.0), axis=1, keepdims=True) for h in range(heads)]

    tk = spread(take) * k
    nrm_new[...] = spread(keep) * nrmb[...] + tk
    scores = per_head(q * k)
    nqs = per_head(nrmb[...] * q)
    qt = q.T
    for s in range(seqs):
        for h in range(heads):
            col = qt[h * qk : (h + 1) * qk, s : s + 1]
            ro[s : s + 1, h * vd : (h + 1) * vd] = jnp.sum(memb[s, h] * col, axis=0, keepdims=True)
    hidden = []
    for h in range(heads):
        ts = take[:, h : h + 1] * scores[h]
        kp = keep[:, h : h + 1]
        numer = ts * v[:, h * vd : (h + 1) * vd] + kp * ro[:, h * vd : (h + 1) * vd]
        denom = ts + kp * nqs[h]
        cell = numer / jnp.maximum(jnp.abs(denom), 1.0)
        og = sf[:, 2 * hw + vw + h * vd : 2 * hw + vw + (h + 1) * vd] * rscale
        hid_own[:, h * vd : (h + 1) * vd] = ((1.0 / (1.0 + jnp.exp(-og))) * cell).astype(BF16)

    def hid_hop(i, slot, step):
        return pltpu.make_async_remote_copy(
            src_ref=hid_own,
            dst_ref=hidg.at[slot, tp],
            send_sem=hid_s.at[i],
            recv_sem=hid_r.at[2 * slot + tp],
            device_id={"kv": at(me + step), "tp": parity},
            device_id_type=MESH,
        )

    for i, (slot, step) in enumerate(((1, -2), (0, 1), (1, -1))):
        begin(hid_hop(i, slot, step))
    own_hid = pltpu.make_async_remote_copy(
        src_ref=hid_own,
        dst_ref=hidg.at[0, tp],
        send_sem=hid_s.at[3],
        recv_sem=hid_r.at[tp],
        device_id={"tp": other},
        device_id_type=MESH,
    )

    @pl.when(tp != parity)
    def _():
        own_hid.start()

    @pl.when(tp == parity)
    def _():
        hidg[0, tp] = hid_own[...]

    for slot in (3, 1):
        from_columns(slot)
        begin(share_slot(slot))
    from_columns(2)
    begin(share_slot(2))
    for name in ("t_up", "t_dn", "t_fw"):
        pre[name].wait_recv()

    def hid_arrival(slot, core):
        pltpu.make_async_remote_copy(
            src_ref=hid_own,
            dst_ref=hidg.at[slot, core],
            send_sem=hid_s.at[0],
            recv_sem=hid_r.at[2 * slot + core],
            device_id={"tp": other},
            device_id_type=MESH,
        ).wait_recv()

    for i in range(2):
        tokx[0, i] = tokrow[at(me + mine_offset + 2 * i)].astype(BF16)

    @pl.when(tp != parity)
    def _():
        own_hid.wait_send()
        hid_arrival(0, tp)

    hid_arrival(0, other)
    for core in range(2):
        hid_arrival(1, core)
    for slot in range(4):
        share_slot(slot).wait_recv()
    left_rows = jnp.concatenate(
        [jnp.concatenate([hidg[i, h].astype(F32) for h in range(2)], axis=1) for i in range(2)], axis=0
    ).astype(BF16)
    added = jnp.dot(left_rows[:, 0:vw], wob[0], preferred_element_type=F32) + jnp.dot(
        left_rows[:, vw : 2 * vw], wob[1], preferred_element_type=F32
    )
    for slot in range(4):
        cols = lax.rem(me // 4 + slot, 4)
        block = added[:, slot * 128 : (slot + 1) * 128].reshape(2, seqs, 128) + tokx[slot].astype(F32)
        midg[me, :, :, pl.ds(pl.multiple_of(cols * 128, 128), 128)] = block.astype(BF16)
    finish = all_gather(MID_TREE, midg, mid_s, mid_r)

    kt = tk.T
    for s in range(seqs):
        for h in range(heads):
            col = kt[h * qk : (h + 1) * qk, s : s + 1]
            mem_new[s, h] = keep[s : s + 1, h : h + 1] * memb[s, h] + col * v[s : s + 1, h * vd : (h + 1) * vd]

    finish()

    up_x.wait_recv()
    dn_x.wait_recv()
    blocks = half_rows // seqs

    def place(group, m):
        z = tp + 2 * m
        offset = lax.rem(z - group + 1 + n, 4) - 1
        return at(z - offset), lax.div(offset + 1, 2)

    sq_sum = jnp.zeros((half_rows, 512), F32)
    acc = [None, None]
    for group in range(4):
        parts = []
        for m in range(blocks):
            z, half = place(group, m)
            parts.append(midg[z, half].astype(F32))
        x = jnp.concatenate(parts, axis=0)
        sq_sum = sq_sum + x * x
        for j in range(0, 4, 2):
            chans = [group + 4 * (j + i) for i in range(2)]
            xs_in = jnp.concatenate(
                [x[:, (j + i) * 128 : (j + i + 1) * 128] * mgb[c : c + 1, :] for i, c in enumerate(chans)], axis=1
            ).astype(BF16)
            for u in range(2):
                w = jnp.concatenate([wupb[u, c * 128 : (c + 1) * 128, :] for c in chans], axis=0)
                d = jnp.dot(xs_in, w, preferred_element_type=F32)
                acc[u] = d if acc[u] is None else acc[u] + d
    rmid = lax.rsqrt(jnp.sum(sq_sum, axis=1, keepdims=True) / width + EPSILON)
    sqd = [jnp.square(jnp.maximum(a * rmid, 0.0)).astype(BF16) for a in acc]

    def own_down(d):
        cols = pl.ds(pl.multiple_of(d * 128, 128), 128)
        return jnp.dot(sqd[0], wdnb[0, :, cols], preferred_element_type=F32) + jnp.dot(
            sqd[1], wdnb[1, :, cols], preferred_element_type=F32
        )

    def sum_down(a, slots):
        for s, here in slots:
            more = dr[s].astype(F32)
            a = a + (more if here is None else jnp.where(here, more, 0.0))
        return a

    def halves(a):
        return [
            jnp.concatenate([a[0:quarter, h : h + half_ch], a[quarter : 2 * quarter, h : h + half_ch]], axis=1)
            for h in (0, half_ch)
        ]

    quarter = half_rows // 2
    msgs_n = n - 1

    def emit_down(m, mine, slots):
        a = sum_down(mine, slots)
        if m[3] == 0:
            fs[m[0], 0], fs[m[0], 1] = [x.astype(BF16) for x in halves(a)]
        else:
            ds[m[0]] = a.astype(BF16)

    def down_copies(m):
        i = m[0]
        if m[3] == 0:
            return [
                along(m, fs.at[i, c], fr.at[tp, i], fs_s.at[2 * i + c], fr_r.at[tp * msgs_n + i], c) for c in range(2)
            ]
        return [along(m, ds.at[i], dr.at[i], dn_s.at[i], dn_r.at[i])]

    last = reduce_scatter(DOWN_TREE, own_down, emit_down, down_copies)
    own_mid = []
    for m in range(blocks):
        z, half = place(lax.rem(me, 4), m)
        own_mid.append(midg[z, half, :, pl.ds(pl.multiple_of(me // 4 * 128, 128), 128)].astype(F32))
    left, right = halves(own_down(me) + jnp.concatenate(own_mid, axis=0))
    fxs[...] = jnp.where(tp == 0, right, left)
    fin_x = to_partner(fxs, fxr, 5)
    fin_x.start()
    sends.append(fin_x)
    early = len(sends)
    for c in sends[:-1]:
        c.wait_send()
    early -= 1
    fin_x.wait_recv()
    sums = [jnp.where(tp == 0, left, right), fxr[...]]
    sums = [jnp.where(tp == 0, sums[0], sums[1]), jnp.where(tp == 0, sums[1], sums[0])]
    for m in last:
        for r in range(2):
            i = m[0]
            along(m, fs.at[i, r], fr.at[r, i], fs_s.at[2 * i + r], fr_r.at[r * msgs_n + i], r).wait_recv()
            sums[r] = sums[r] + fr[r, i].astype(F32)
    flat = jnp.concatenate(
        [sums[r][m * seqs : (m + 1) * seqs] for m in range(blocks // 2) for r in range(2)], axis=0
    ).T
    out[...] = jnp.concatenate([flat[0:half_ch], flat[half_ch : 2 * half_ch]], axis=1).astype(BF16)
    for c in sends[early:]:
        c.wait_send()


def hand_over(*refs):
    count = (len(refs) - 1) // 2
    sems = refs[-1]
    copies = [pltpu.make_async_copy(refs[i], refs[count + i], sems.at[i]) for i in range(count)]
    for c in copies:
        c.start()
    for c in copies:
        c.wait()


def shards(n, columns, *args):
    (tok, ngain, wq, wk, wv, wg, wi, wf, ib, fb, mem, nrm, stab, wo, mgain, wup, wdn) = args
    rows, half_ch = tok.shape
    chans = ngain.shape[0]
    seqs, heads, qk, vd = mem.shape
    hw, vw = heads * qk, heads * vd
    proj = 2 * hw + 2 * vw
    wide = proj + 128
    width = mgain.shape[0]
    hid = wup.shape[1]
    msgs = n - 1
    any_space = pl.BlockSpec(memory_space=pl.ANY)
    vmem = pl.BlockSpec(memory_space=pltpu.VMEM)
    dma = pltpu.SemaphoreType.DMA
    out = pl.pallas_call(
        functools.partial(kernel, n, columns),
        out_shape=(
            pltpu.VMEM((half_ch, rows), BF16),
            pltpu.VMEM(mem.shape, F32),
            pltpu.VMEM(nrm.shape, F32),
            pltpu.VMEM((heads, seqs), F32),
        ),
        in_specs=[any_space] * 17,
        out_specs=(vmem,) * 4,
        scratch_shapes=[
            pltpu.VMEM((2, half_ch, rows), BF16),
            pltpu.VMEM((1, chans), F32),
            pltpu.VMEM((chans, proj), BF16),
            pltpu.VMEM((2, wi.shape[1], chans), BF16),
            pltpu.VMEM((1, ib.shape[0]), F32),
            pltpu.VMEM((1, fb.shape[0]), F32),
            pltpu.VMEM(mem.shape, F32),
            pltpu.VMEM(nrm.shape, F32),
            pltpu.VMEM((heads, seqs), F32),
            pltpu.VMEM((2, wo.shape[0], 512), BF16),
            pltpu.VMEM((width // 128, 128), F32),
            pltpu.VMEM((2, *wup.shape), BF16),
            pltpu.VMEM((2, *wdn.shape), BF16),
            pltpu.VMEM((n, seqs, wide), F32),
            pltpu.VMEM((msgs, seqs, wide), BF16),
            pltpu.VMEM((msgs, seqs, wide), BF16),
            pltpu.VMEM((seqs, proj), F32),
            pltpu.VMEM((seqs, vw), F32),
            pltpu.VMEM((n, seqs, 128), F32),
            pltpu.VMEM((3, 2, seqs, 128), BF16),
            pltpu.VMEM((4, 2, seqs, 128), BF16),
            pltpu.VMEM((2, seqs, 128), BF16),
            pltpu.VMEM((seqs, vw), BF16),
            pltpu.VMEM((2, 2, seqs, vw), BF16),
            pltpu.VMEM((n, 2, seqs, 512), BF16),
            pltpu.VMEM((msgs, rows // 2, 128), BF16),
            pltpu.VMEM((msgs, rows // 2, 128), BF16),
            pltpu.VMEM((msgs, 2, rows // 4, 128), BF16),
            pltpu.VMEM((2, msgs, rows // 4, 128), BF16),
            pltpu.VMEM((rows // 4, 128), F32),
            pltpu.VMEM((rows // 4, 128), F32),
            dma((20,)),
            dma((10,)),
            dma((10,)),
            dma((msgs,)),
            dma((msgs,)),
            dma((msgs,)),
            dma((msgs,)),
            dma((msgs,)),
            dma((msgs,)),
            dma((msgs,)),
            dma((msgs,)),
            dma((2 * msgs,)),
            dma((2 * msgs,)),
            dma((7 + 3 * (columns - 1),)),
            dma((7 + 3 * (columns - 1),)),
        ],
        compiler_params=pltpu.CompilerParams(collective_id=0, has_side_effects=True, vmem_limit_bytes=40 * 2**20),
        name="cell_step",
    )(*[pltpu.with_memory_space_constraint(x, pltpu.HBM) for x in (
        tok.T,
        ngain.reshape(1, -1),
        wq,
        wk,
        wv,
        wg,
        wi.T,
        wf.T,
        ib.reshape(1, -1),
        fb.reshape(1, -1),
        mem,
        nrm,
        stab.T,
        wo,
        mgain.reshape(-1, 128),
        wup,
        wdn,
    )])
    out = pl.pallas_call(
        hand_over,
        out_shape=tuple(jax.ShapeDtypeStruct(o.shape, o.dtype) for o in out),
        in_specs=[vmem] * 4,
        out_specs=(any_space,) * 4,
        scratch_shapes=[dma((4,))],
        name="hand_over",
    )(*[pltpu.with_memory_space_constraint(o, pltpu.VMEM) for o in out])
    return out[0].T, out[1], out[2], out[3].T


def solution(mesh):
    placed = (
        P(("grp", "dp"), ("kv", "tp")),
        P("kv"),
        P("kv", "tp"),
        P("kv", "tp"),
        P("kv", "tp"),
        P("kv", "tp"),
        P("kv", None),
        P("kv", None),
        P(),
        P(),
        P(("grp", "dp", "kv"), "tp", None, None),
        P(("grp", "dp", "kv"), "tp"),
        P(("grp", "dp", "kv"), "tp"),
        P("tp", "kv"),
        P(),
        P(None, ("kv", "tp")),
        P(("kv", "tp"), None),
    )
    return jax.shard_map(
        functools.partial(shards, mesh.shape["kv"], mesh.shape["dp"]),
        mesh=mesh,
        in_specs=placed,
        out_specs=(
            P(("grp", "dp"), ("kv", "tp")),
            P(("grp", "dp", "kv"), "tp", None, None),
            P(("grp", "dp", "kv"), "tp"),
            P(("grp", "dp", "kv"), "tp"),
        ),
        check_vma=False,
    )
```

```python
import functools

import jax
import jax.numpy as jnp
from jax import lax
from jax.experimental import pallas as pl
from jax.experimental.pallas import tpu as pltpu
from jax.sharding import PartitionSpec as P

EPSILON = 1e-06
MESH = pl.DeviceIdType.MESH
F32 = jnp.float32
BF16 = jnp.bfloat16

TWO_LEVEL = {1: 0, 2: 0, 3: 0, 4: 0, 5: 4, 6: 4, 7: 4, 8: 4}
PROJ_TREE = {1: 0, 2: 0, 3: 0, 4: 3, 5: 3, 6: 3, 7: 6, 8: 6}
REACH = 4
MID_TREE = TWO_LEVEL
DOWN_TREE = TWO_LEVEL


def messages(tree, n):
    out = []
    for side in (1, -1):
        for k in range(1, n // 2):
            out.append((len(out), side, k, tree[k]))
    out.append((len(out), 0, n // 2, tree[n // 2]))
    return out


def children_of(msgs, side, k):
    return [m for m in msgs if m[1] in (side, 0) and m[3] == k and k > 0]


def depth_below(msgs, m):
    below = children_of(msgs, m[1], m[2])
    return 1 + max(depth_below(msgs, c) for c in below) if below else 0


def level_of(tree, k):
    return 0 if k == 0 else 1 + level_of(tree, tree[k])


def kernel(
    n,
    columns,
    tok,
    ngain,
    wq,
    wk,
    wv,
    wg,
    wi,
    wf,
    ib,
    fb,
    mem,
    nrm,
    stab,
    wo,
    mgain,
    wup,
    wdn,
    out,
    mem_new,
    nrm_new,
    stab_new,
    tokb,
    ngv,
    wp,
    wib,
    ibb,
    fbb,
    memb,
    nrmb,
    stabb,
    wob,
    mgb,
    wupb,
    wdnb,
    pf,
    ps,
    pr,
    sf,
    ro,
    tokrow,
    tst,
    tokx,
    tfwd,
    hid_own,
    hidg,
    midg,
    ds,
    dr,
    fs,
    fr,
    fxs,
    fxr,
    lsem,
    xs,
    xr,
    ps_s,
    ps_r,
    hid_s,
    hid_r,
    mid_s,
    mid_r,
    dn_s,
    dn_r,
    fs_s,
    fr_r,
    pre_s,
    pre_r,
):
    me = lax.axis_index("kv")
    tp = lax.axis_index("tp")
    column = lax.axis_index("dp")
    other = 1 - tp
    half_ch, rows = tokb.shape[1:]
    seqs, heads, qk, vd = memb.shape
    hw = heads * qk
    vw = heads * vd
    proj = wp.shape[1]
    width = mgb.shape[0] * mgb.shape[1]
    half_rows = rows // 2
    wo_rows = wob.shape[1]

    def at(z):
        return lax.rem(z + 2 * n, n)

    far_side = 1 - 2 * lax.rem(me, 2)

    def way(side):
        return far_side if side == 0 else side

    barrier = pltpu.get_barrier_semaphore()
    for step in range(1, REACH + 1):
        for side in (1, -1):
            pl.semaphore_signal(barrier, inc=1, device_id={"kv": at(me + side * step)}, device_id_type=MESH)
    pl.semaphore_signal(barrier, inc=1, device_id={"tp": other}, device_id_type=MESH)
    for step in range(1, columns):
        pl.semaphore_signal(barrier, inc=1, device_id={"dp": lax.rem(column + step, columns)}, device_id_type=MESH)

    loads = {}

    def load(name, src, dst):
        c = pltpu.make_async_copy(src, dst, lsem.at[len(loads)])
        c.start()
        loads[name] = c

    load("tok", tok, tokb.at[tp])
    load("wo", wo, wob.at[tp, :, 0:128])
    load("ngain", ngain, ngv)
    load("wq", wq, wp.at[:, 0:hw])
    load("wk", wk, wp.at[:, hw : 2 * hw])
    load("wv", wv, wp.at[:, 2 * hw : 2 * hw + vw])
    load("wg", wg, wp.at[:, 2 * hw + vw : proj])
    load("wi", wi, wib.at[0])
    load("wf", wf, wib.at[1])
    load("ib", ib, ibb)
    load("fb", fb, fbb)
    load("stab", stab, stabb)
    load("nrm", nrm, nrmb)
    load("mem", mem, memb)
    load("mgain", mgain, mgb)
    load("wup", wup, wupb.at[tp])
    load("wdn", wdn, wdnb.at[tp])

    pl.semaphore_wait(barrier, 2 * REACH + columns)

    def to_partner(src, dst, i):
        return pltpu.make_async_remote_copy(
            src_ref=src, dst_ref=dst, send_sem=xs.at[i], recv_sem=xr.at[i], device_id={"tp": other}, device_id_type=MESH
        )

    loads["tok"].wait()
    tok_x = to_partner(tokb.at[tp], tokb.at[tp], 0)
    tok_x.start()
    sends = [tok_x]

    stride = n // 4
    piece_rows = wo_rows // columns
    parity = lax.rem(me, 2)
    mine_offset = jnp.where(tp == parity, 0, -1)

    def piece(x):
        return pl.ds(pl.multiple_of(x * piece_rows, piece_rows), piece_rows)

    def lanes(slot):
        return pl.ds(slot * 128 if isinstance(slot, int) else pl.multiple_of(slot * 128, 128), 128)

    def hop(src, dst, i, step, side="kv"):
        where = at(me + step) if side == "kv" else lax.rem(column + step, columns)
        return pltpu.make_async_remote_copy(
            src_ref=src, dst_ref=dst, send_sem=pre_s.at[i], recv_sem=pre_r.at[i], device_id={side: where}, device_id_type=MESH
        )

    def piece_hop(source, slot, i, step):
        return hop(wob.at[tp, piece(column), lanes(source)], wob.at[tp, piece(column), lanes(slot)], i, step)

    pre = {
        "w_up": piece_hop(0, 3, 0, stride),
        "w_dn": piece_hop(0, 1, 1, -stride),
        "t_up": hop(tst.at[0], tokx.at[3], 2, stride),
        "t_dn": hop(tst.at[1], tokx.at[1], 3, -stride),
        "t_on": hop(tst.at[2], tfwd, 4, far_side * stride),
        "w_fw": piece_hop(2 + far_side, 2, 5, far_side * stride),
        "t_fw": hop(tfwd, tokx.at[2], 6, far_side * stride),
    }

    def begin(c):
        c.start()
        sends.append(c)

    def column_copy(slot, step):
        part = wob.at[tp, piece(column), lanes(slot)]
        return hop(part, part, 7 + (slot - 1) * (columns - 1) + step - 1, step, "dp")

    def column_arrival(slot, step):
        part = wob.at[tp, piece(lax.rem(column - step + columns, columns)), lanes(slot)]
        return hop(part, part, 7 + (slot - 1) * (columns - 1) + step - 1, step, "dp")

    by_distance = sorted(range(1, columns), key=lambda step: -min(step, columns - step))

    def to_columns(slot):
        for step in by_distance:
            begin(column_copy(slot, step))

    def from_columns(slot):
        for step in range(1, columns):
            column_arrival(slot, step).wait_recv()

    def share_slot(slot):
        part = wob.at[tp, :, lanes(slot)]
        return to_partner(part, part, 6 + slot)

    up_x = to_partner(wupb.at[tp], wupb.at[tp], 1)
    dn_x = to_partner(wdnb.at[tp], wdnb.at[tp], 2)

    def forward_on():
        loads["wup"].wait()
        begin(up_x)
        loads["wdn"].wait()
        begin(dn_x)
        pre["w_up"].wait_recv()
        pre["w_dn"].wait_recv()
        begin(pre["w_fw"])
        to_columns(3)
        to_columns(1)

    def complete_near():
        pre["t_on"].wait_recv()
        begin(pre["t_fw"])
        pre["w_fw"].wait_recv()
        to_columns(2)

    loads["wo"].wait()
    begin(pre["w_up"])
    begin(pre["w_dn"])
    begin(share_slot(0))

    for name in ("ngain", "wq", "wk", "wv", "wg", "wi", "wf"):
        loads[name].wait()

    gate_lanes = 2 * wib.shape[1]
    lane128 = lax.broadcasted_iota(jnp.int32, (rows, 128), 1)
    gw = jnp.concatenate(
        [wib[0].astype(F32), wib[1].astype(F32), jnp.zeros((128 - gate_lanes, 2 * half_ch), F32)], axis=0
    ).astype(BF16)
    tok_x.wait_recv()
    t = jnp.concatenate([tokb[0], tokb[1]], axis=0).astype(F32).T
    scaled = (t * ngv[...]).astype(BF16)
    main = jnp.dot(scaled, wp[...], preferred_element_type=F32)
    gates = lax.dot_general(scaled, gw, (((1,), (1,)), ((), ())), preferred_element_type=F32)
    pf[:, :, 0:proj] = main.reshape(n, seqs, proj)
    pf[:, :, proj:] = jnp.where(lane128 == gate_lanes, jnp.sum(t * t, axis=1, keepdims=True), gates).reshape(n, seqs, 128)
    tokrow[...] = t.reshape(n, seqs, 2 * half_ch)

    lane8 = lax.broadcasted_iota(jnp.int32, (seqs, 128), 1)

    def pack_gates(g):
        total = g[:, gate_lanes : gate_lanes + 1] + g[:, gate_lanes + 1 : gate_lanes + 2]
        upper = total.astype(BF16).astype(F32)
        return jnp.where(lane8 == gate_lanes, upper, jnp.where(lane8 == gate_lanes + 1, total - upper, g))

    def reduce_scatter(tree, own, add, emit, copies_of, before_relays=None):
        msgs = messages(tree, n)
        order = sorted(msgs, key=lambda m: (depth_below(msgs, m), -level_of(tree, m[2]), -m[2]))
        waited = set()
        for m in order:
            slot, side, k, parent = m
            mine = own(at(me - way(side) * k))
            kids = children_of(msgs, side, k)
            if kids and before_relays is not None:
                before_relays()
                before_relays = None
            for c in kids:
                if c[0] not in waited:
                    waited.add(c[0])
                    copies_of(c)[0].wait_recv()
                mine = add(mine, [(c[0], None if c[1] else far_side == side)])
            emit(m, mine)
            for c in copies_of(m):
                c.start()
                sends.append(c)
        return [m for m in msgs if m[3] == 0]

    def along(m, src, dst, send_sem, recv_sem, core=None):
        slot, side, k, parent = m
        where = {"kv": at(me - way(side) * (k - parent))}
        if core is not None:
            where["tp"] = core
        return pltpu.make_async_remote_copy(
            src_ref=src, dst_ref=dst, send_sem=send_sem, recv_sem=recv_sem, device_id=where, device_id_type=MESH
        )

    def all_gather(tree, buf, send_sem, recv_sem):
        msgs = messages(tree, n)

        def copy_of(m):
            slot, side, k, parent = m
            side = way(side)
            origin = at(me - side * parent)
            return pltpu.make_async_remote_copy(
                src_ref=buf.at[origin],
                dst_ref=buf.at[origin],
                send_sem=send_sem.at[slot],
                recv_sem=recv_sem.at[slot],
                device_id={"kv": at(me + side * (k - parent))},
                device_id_type=MESH,
            )

        def arrival(m):
            slot, side, k, parent = m
            side = way(side)
            origin = at(me - side * k)
            return pltpu.make_async_remote_copy(
                src_ref=buf.at[origin],
                dst_ref=buf.at[origin],
                send_sem=send_sem.at[slot],
                recv_sem=recv_sem.at[slot],
                device_id={"kv": at(me - side * k)},
                device_id_type=MESH,
            )

        def send(m):
            c = copy_of(m)
            c.start()
            sends.append(c)

        waited = set()
        firsts = [m for m in msgs if m[3] == 0]
        for m in sorted(firsts, key=lambda m: (-depth_below(msgs, m), -m[2])):
            send(m)

        def finish():
            todo = sorted([m for m in msgs if children_of(msgs, m[1], m[2])], key=lambda m: (level_of(tree, m[2]), m[2]))
            for m in todo:
                arrival(m).wait_recv()
                waited.add(m[0])
            for c in sorted([c for c in msgs if c[3]], key=lambda c: (level_of(tree, c[2]), -c[2])):
                send(c)
            for m in msgs:
                if m[0] not in waited:
                    arrival(m).wait_recv()

        return finish

    for i, step in enumerate((stride, -stride, 2 * stride)):
        for b in range(2):
            tst[i, b] = tokrow[at(me + step + mine_offset + 2 * b)].astype(BF16)

    def own_proj(d):
        return pf[d, :, 0:proj], pf[d, :, proj:]

    def sum_proj(mine, slots):
        a, g = mine
        for s, here in slots:
            more_a, more_g = pr[s, :, 0:proj].astype(F32), pr[s, :, proj:].astype(F32)
            if here is not None:
                more_a, more_g = jnp.where(here, more_a, 0.0), jnp.where(here, more_g, 0.0)
            a = a + more_a
            g = g + more_g
        return a, g

    def emit_proj(m, mine):
        slot = m[0]
        a, g = mine
        ps[slot, :, 0:proj] = a.astype(BF16)
        ps[slot, :, proj:] = pack_gates(g).astype(BF16)

    def proj_copies(m):
        i = m[0]
        return [along(m, ps.at[i], pr.at[i], ps_s.at[i], ps_r.at[i])]

    for name in ("t_on", "t_up", "t_dn"):
        begin(pre[name])
    last = reduce_scatter(PROJ_TREE, own_proj, sum_proj, emit_proj, proj_copies, forward_on)
    complete_near()

    for name in ("ib", "fb", "stab", "nrm", "mem", "mgain"):
        loads[name].wait()

    total, gate = own_proj(me)
    for m in sorted(last, key=lambda m: m[2]):
        proj_copies(m)[0].wait_recv()
        total, gate = sum_proj((total, gate), [(m[0], None)])
    sf[:, 0:proj] = total
    squares = gate[:, gate_lanes : gate_lanes + 1] + gate[:, gate_lanes + 1 : gate_lanes + 2]
    rscale = lax.rsqrt(squares / width + EPSILON)
    q = sf[:, 0:hw] * rscale
    k = sf[:, hw : 2 * hw] * rscale * qk ** (-0.5)
    v = sf[:, 2 * hw : 2 * hw + vw] * rscale
    all_heads = wib.shape[1]

    def mine_of(x, first):
        return jnp.where(tp == 0, x[:, first : first + heads], x[:, first + heads : first + 2 * heads])

    log_in = mine_of(gate, 0) * rscale + mine_of(ibb[...], 0)
    fpre = mine_of(gate, all_heads) * rscale + mine_of(fbb[...], 0)
    log_forget = jnp.minimum(fpre, 0.0) - jnp.log(1.0 + jnp.exp(-jnp.abs(fpre)))
    carried = log_forget + stabb[...].T
    snew = jnp.maximum(carried, log_in)
    take = jnp.exp(log_in - snew)
    keep = jnp.exp(carried - snew)
    stab_new[...] = snew.T

    hlane = lax.broadcasted_iota(jnp.int32, (seqs, hw), 1) // qk

    def spread(x):
        r = jnp.broadcast_to(x[:, 0:1], (seqs, hw))
        for h in range(1, heads):
            r = jnp.where(hlane == h, x[:, h : h + 1], r)
        return r

    def per_head(x):
        return [jnp.sum(jnp.where(hlane == h, x, 0.0), axis=1, keepdims=True) for h in range(heads)]

    tk = spread(take) * k
    nrm_new[...] = spread(keep) * nrmb[...] + tk
    scores = per_head(q * k)
    nqs = per_head(nrmb[...] * q)
    qt = q.T
    for s in range(seqs):
        for h in range(heads):
            col = qt[h * qk : (h + 1) * qk, s : s + 1]
            ro[s : s + 1, h * vd : (h + 1) * vd] = jnp.sum(memb[s, h] * col, axis=0, keepdims=True)
    hidden = []
    for h in range(heads):
        ts = take[:, h : h + 1] * scores[h]
        kp = keep[:, h : h + 1]
        numer = ts * v[:, h * vd : (h + 1) * vd] + kp * ro[:, h * vd : (h + 1) * vd]
        denom = ts + kp * nqs[h]
        cell = numer / jnp.maximum(jnp.abs(denom), 1.0)
        og = sf[:, 2 * hw + vw + h * vd : 2 * hw + vw + (h + 1) * vd] * rscale
        hid_own[:, h * vd : (h + 1) * vd] = ((1.0 / (1.0 + jnp.exp(-og))) * cell).astype(BF16)

    def hid_hop(i, slot, step):
        return pltpu.make_async_remote_copy(
            src_ref=hid_own,
            dst_ref=hidg.at[slot, tp],
            send_sem=hid_s.at[i],
            recv_sem=hid_r.at[2 * slot + tp],
            device_id={"kv": at(me + step), "tp": parity},
            device_id_type=MESH,
        )

    for i, (slot, step) in enumerate(((1, -2), (0, 1), (1, -1))):
        begin(hid_hop(i, slot, step))
    own_hid = pltpu.make_async_remote_copy(
        src_ref=hid_own,
        dst_ref=hidg.at[0, tp],
        send_sem=hid_s.at[3],
        recv_sem=hid_r.at[tp],
        device_id={"tp": other},
        device_id_type=MESH,
    )

    @pl.when(tp != parity)
    def _():
        own_hid.start()

    @pl.when(tp == parity)
    def _():
        hidg[0, tp] = hid_own[...]

    for slot in (3, 1):
        from_columns(slot)
        begin(share_slot(slot))
    from_columns(2)
    begin(share_slot(2))
    for name in ("t_up", "t_dn", "t_fw"):
        pre[name].wait_recv()

    def hid_arrival(slot, core):
        pltpu.make_async_remote_copy(
            src_ref=hid_own,
            dst_ref=hidg.at[slot, core],
            send_sem=hid_s.at[0],
            recv_sem=hid_r.at[2 * slot + core],
            device_id={"tp": other},
            device_id_type=MESH,
        ).wait_recv()

    for i in range(2):
        tokx[0, i] = tokrow[at(me + mine_offset + 2 * i)].astype(BF16)

    @pl.when(tp != parity)
    def _():
        own_hid.wait_send()
        hid_arrival(0, tp)

    hid_arrival(0, other)
    for core in range(2):
        hid_arrival(1, core)
    for slot in range(4):
        share_slot(slot).wait_recv()
    left_rows = jnp.concatenate(
        [jnp.concatenate([hidg[i, h].astype(F32) for h in range(2)], axis=1) for i in range(2)], axis=0
    ).astype(BF16)
    added = jnp.dot(left_rows[:, 0:vw], wob[0], preferred_element_type=F32) + jnp.dot(
        left_rows[:, vw : 2 * vw], wob[1], preferred_element_type=F32
    )
    for slot in range(4):
        cols = lax.rem(me // 4 + slot, 4)
        block = added[:, slot * 128 : (slot + 1) * 128].reshape(2, seqs, 128) + tokx[slot].astype(F32)
        midg[me, :, :, pl.ds(pl.multiple_of(cols * 128, 128), 128)] = block.astype(BF16)
    finish = all_gather(MID_TREE, midg, mid_s, mid_r)

    kt = tk.T
    for s in range(seqs):
        for h in range(heads):
            col = kt[h * qk : (h + 1) * qk, s : s + 1]
            mem_new[s, h] = keep[s : s + 1, h : h + 1] * memb[s, h] + col * v[s : s + 1, h * vd : (h + 1) * vd]

    finish()

    up_x.wait_recv()
    dn_x.wait_recv()
    blocks = half_rows // seqs

    def place(group, m):
        z = tp + 2 * m
        offset = lax.rem(z - group + 1 + n, 4) - 1
        return at(z - offset), lax.div(offset + 1, 2)

    sq_sum = jnp.zeros((half_rows, 512), F32)
    acc = [None, None]
    for group in range(4):
        parts = []
        for m in range(blocks):
            z, half = place(group, m)
            parts.append(midg[z, half].astype(F32))
        x = jnp.concatenate(parts, axis=0)
        sq_sum = sq_sum + x * x
        for j in range(0, 4, 2):
            chans = [group + 4 * (j + i) for i in range(2)]
            xs_in = jnp.concatenate(
                [x[:, (j + i) * 128 : (j + i + 1) * 128] * mgb[c : c + 1, :] for i, c in enumerate(chans)], axis=1
            ).astype(BF16)
            for u in range(2):
                w = jnp.concatenate([wupb[u, c * 128 : (c + 1) * 128, :] for c in chans], axis=0)
                d = jnp.dot(xs_in, w, preferred_element_type=F32)
                acc[u] = d if acc[u] is None else acc[u] + d
    rmid = lax.rsqrt(jnp.sum(sq_sum, axis=1, keepdims=True) / width + EPSILON)
    sqd = [jnp.square(jnp.maximum(a * rmid, 0.0)).astype(BF16) for a in acc]

    def own_down(d):
        cols = pl.ds(pl.multiple_of(d * 128, 128), 128)
        return jnp.dot(sqd[0], wdnb[0, :, cols], preferred_element_type=F32) + jnp.dot(
            sqd[1], wdnb[1, :, cols], preferred_element_type=F32
        )

    def sum_down(a, slots):
        for s, here in slots:
            more = dr[s].astype(F32)
            a = a + (more if here is None else jnp.where(here, more, 0.0))
        return a

    def halves(a):
        return [
            jnp.concatenate([a[0:quarter, h : h + half_ch], a[quarter : 2 * quarter, h : h + half_ch]], axis=1)
            for h in (0, half_ch)
        ]

    quarter = half_rows // 2
    msgs_n = n - 1

    def emit_down(m, a):
        if m[3] == 0:
            fs[m[0], 0], fs[m[0], 1] = [x.astype(BF16) for x in halves(a)]
        else:
            ds[m[0]] = a.astype(BF16)

    def down_copies(m):
        i = m[0]
        if m[3] == 0:
            return [
                along(m, fs.at[i, c], fr.at[tp, i], fs_s.at[2 * i + c], fr_r.at[tp * msgs_n + i], c) for c in range(2)
            ]
        return [along(m, ds.at[i], dr.at[i], dn_s.at[i], dn_r.at[i])]

    last = reduce_scatter(DOWN_TREE, own_down, sum_down, emit_down, down_copies)
    own_mid = []
    for m in range(blocks):
        z, half = place(lax.rem(me, 4), m)
        own_mid.append(midg[z, half, :, pl.ds(pl.multiple_of(me // 4 * 128, 128), 128)].astype(F32))
    left, right = halves(own_down(me) + jnp.concatenate(own_mid, axis=0))
    fxs[...] = jnp.where(tp == 0, right, left)
    fin_x = to_partner(fxs, fxr, 5)
    fin_x.start()
    sends.append(fin_x)
    early = len(sends)
    for c in sends[:-1]:
        c.wait_send()
    early -= 1
    fin_x.wait_recv()
    sums = [jnp.where(tp == 0, left, right), fxr[...]]
    sums = [jnp.where(tp == 0, sums[0], sums[1]), jnp.where(tp == 0, sums[1], sums[0])]
    for m in last:
        for r in range(2):
            i = m[0]
            along(m, fs.at[i, r], fr.at[r, i], fs_s.at[2 * i + r], fr_r.at[r * msgs_n + i], r).wait_recv()
            sums[r] = sums[r] + fr[r, i].astype(F32)
    flat = jnp.concatenate(
        [sums[r][m * seqs : (m + 1) * seqs] for m in range(blocks // 2) for r in range(2)], axis=0
    ).T
    out[...] = jnp.concatenate([flat[0:half_ch], flat[half_ch : 2 * half_ch]], axis=1).astype(BF16)
    for c in sends[early:]:
        c.wait_send()


def hand_over(*refs):
    count = (len(refs) - 1) // 2
    sems = refs[-1]
    copies = [pltpu.make_async_copy(refs[i], refs[count + i], sems.at[i]) for i in range(count)]
    for c in copies:
        c.start()
    for c in copies:
        c.wait()


def shards(n, columns, *args):
    (tok, ngain, wq, wk, wv, wg, wi, wf, ib, fb, mem, nrm, stab, wo, mgain, wup, wdn) = args
    rows, half_ch = tok.shape
    chans = ngain.shape[0]
    seqs, heads, qk, vd = mem.shape
    hw, vw = heads * qk, heads * vd
    proj = 2 * hw + 2 * vw
    wide = proj + 128
    width = mgain.shape[0]
    hid = wup.shape[1]
    msgs = n - 1
    any_space = pl.BlockSpec(memory_space=pl.ANY)
    vmem = pl.BlockSpec(memory_space=pltpu.VMEM)
    dma = pltpu.SemaphoreType.DMA
    out = pl.pallas_call(
        functools.partial(kernel, n, columns),
        out_shape=(
            pltpu.VMEM((half_ch, rows), BF16),
            pltpu.VMEM(mem.shape, F32),
            pltpu.VMEM(nrm.shape, F32),
            pltpu.VMEM((heads, seqs), F32),
        ),
        in_specs=[any_space] * 17,
        out_specs=(vmem,) * 4,
        scratch_shapes=[
            pltpu.VMEM((2, half_ch, rows), BF16),
            pltpu.VMEM((1, chans), F32),
            pltpu.VMEM((chans, proj), BF16),
            pltpu.VMEM((2, wi.shape[1], chans), BF16),
            pltpu.VMEM((1, ib.shape[0]), F32),
            pltpu.VMEM((1, fb.shape[0]), F32),
            pltpu.VMEM(mem.shape, F32),
            pltpu.VMEM(nrm.shape, F32),
            pltpu.VMEM((heads, seqs), F32),
            pltpu.VMEM((2, wo.shape[0], 512), BF16),
            pltpu.VMEM((width // 128, 128), F32),
            pltpu.VMEM((2, *wup.shape), BF16),
            pltpu.VMEM((2, *wdn.shape), BF16),
            pltpu.VMEM((n, seqs, wide), F32),
            pltpu.VMEM((msgs, seqs, wide), BF16),
            pltpu.VMEM((msgs, seqs, wide), BF16),
            pltpu.VMEM((seqs, proj), F32),
            pltpu.VMEM((seqs, vw), F32),
            pltpu.VMEM((n, seqs, 128), F32),
            pltpu.VMEM((3, 2, seqs, 128), BF16),
            pltpu.VMEM((4, 2, seqs, 128), BF16),
            pltpu.VMEM((2, seqs, 128), BF16),
            pltpu.VMEM((seqs, vw), BF16),
            pltpu.VMEM((2, 2, seqs, vw), BF16),
            pltpu.VMEM((n, 2, seqs, 512), BF16),
            pltpu.VMEM((msgs, rows // 2, 128), BF16),
            pltpu.VMEM((msgs, rows // 2, 128), BF16),
            pltpu.VMEM((msgs, 2, rows // 4, 128), BF16),
            pltpu.VMEM((2, msgs, rows // 4, 128), BF16),
            pltpu.VMEM((rows // 4, 128), F32),
            pltpu.VMEM((rows // 4, 128), F32),
            dma((20,)),
            dma((10,)),
            dma((10,)),
            dma((msgs,)),
            dma((msgs,)),
            dma((msgs,)),
            dma((msgs,)),
            dma((msgs,)),
            dma((msgs,)),
            dma((msgs,)),
            dma((msgs,)),
            dma((2 * msgs,)),
            dma((2 * msgs,)),
            dma((7 + 3 * (columns - 1),)),
            dma((7 + 3 * (columns - 1),)),
        ],
        compiler_params=pltpu.CompilerParams(collective_id=0, has_side_effects=True, vmem_limit_bytes=40 * 2**20),
        name="cell_step",
    )(*[pltpu.with_memory_space_constraint(x, pltpu.HBM) for x in (
        tok.T,
        ngain.reshape(1, -1),
        wq,
        wk,
        wv,
        wg,
        wi.T,
        wf.T,
        ib.reshape(1, -1),
        fb.reshape(1, -1),
        mem,
        nrm,
        stab.T,
        wo,
        mgain.reshape(-1, 128),
        wup,
        wdn,
    )])
    out = pl.pallas_call(
        hand_over,
        out_shape=tuple(jax.ShapeDtypeStruct(o.shape, o.dtype) for o in out),
        in_specs=[vmem] * 4,
        out_specs=(any_space,) * 4,
        scratch_shapes=[dma((4,))],
        name="hand_over",
    )(*[pltpu.with_memory_space_constraint(o, pltpu.VMEM) for o in out])
    return out[0].T, out[1], out[2], out[3].T


def solution(mesh):
    placed = (
        P(("grp", "dp"), ("kv", "tp")),
        P("kv"),
        P("kv", "tp"),
        P("kv", "tp"),
        P("kv", "tp"),
        P("kv", "tp"),
        P("kv", None),
        P("kv", None),
        P(),
        P(),
        P(("grp", "dp", "kv"), "tp", None, None),
        P(("grp", "dp", "kv"), "tp"),
        P(("grp", "dp", "kv"), "tp"),
        P("tp", "kv"),
        P(),
        P(None, ("kv", "tp")),
        P(("kv", "tp"), None),
    )
    return jax.shard_map(
        functools.partial(shards, mesh.shape["kv"], mesh.shape["dp"]),
        mesh=mesh,
        in_specs=placed,
        out_specs=(
            P(("grp", "dp"), ("kv", "tp")),
            P(("grp", "dp", "kv"), "tp", None, None),
            P(("grp", "dp", "kv"), "tp"),
            P(("grp", "dp", "kv"), "tp"),
        ),
        check_vma=False,
    )
```
